32 devices in a mesh: grp: 2 (over y), sp: 4 (over z), fs: 2 (over x), tp: 2 (over core).
Axes of the slice: x: 2, y: 2, z: 4, core: 2. Of those that a mesh axis runs over, the one named last changes fastest.
Arguments:
- tokens: bfloat16 [8, 256, 2048], P(('grp', 'fs'), 'sp'), parts along dimension 0, may hold values from -6 to 6
- pre_gain: float32 [2048], replicated, may hold values from 0.1 to 1.9
- query_weight: bfloat16 [2048, 1024], P(('sp', 'fs'), 'tp'), may hold values from -0.125 to 0.125
- key_weight: bfloat16 [2048, 1024], P(('sp', 'fs'), 'tp'), may hold values from -0.125 to 0.125
- value_weight: bfloat16 [2048, 1024], P(('sp', 'fs'), 'tp'), may hold values from -0.125 to 0.125
- beta_weight: bfloat16 [2048, 8], replicated, may hold values from -0.125 to 0.125
- decay_weight: bfloat16 [2048, 8], replicated, may hold values from -0.125 to 0.125
- decay_rate: float32 [8], replicated, may hold values from 0 to 1
- delta_gain: float32 [128], replicated, may hold values from 0.1 to 1.9
- query_down: bfloat16 [2048, 512], P(('sp', 'fs')), may hold values from -0.125 to 0.125
- latent_down: bfloat16 [2048, 256], P(('sp', 'fs')), may hold values from -0.125 to 0.125
- rope_weight: bfloat16 [2048, 32], replicated, may hold values from -0.125 to 0.125
- query_gain: float32 [512], replicated, may hold values from 0.1 to 1.9
- latent_gain: float32 [256], replicated, may hold values from 0.1 to 1.9
- query_up: bfloat16 [512, 1536], P(None, 'tp'), may hold values from -4 to 4
- latent_up: bfloat16 [256, 2048], P(None, 'tp'), may hold values from -4 to 4
- delta_out: bfloat16 [1024, 2048], P('tp', ('sp', 'fs')), may hold values from -8 to 8
- latent_out: bfloat16 [1024, 2048], P('tp', ('sp', 'fs')), may hold values from -8 to 8
- post_gain: float32 [2048], P('tp'), may hold values from 0.1 to 1.9
Outputs:
- mixed_out: bfloat16 [8, 256, 2048], P(('grp', 'fs'), 'sp', 'tp'), parts along dimension 0
The draws below stay inside these ranges and needn't reach their ends.
There are 2 independent parts, one for each index of `grp`. The reference program is written for one: setup_inputs(seed, part) draws one part's arguments, and reference() takes and returns one part's arrays. A program takes and returns all parts, laid end to end along the dimension named above; an argument that names none is the same for every part. Nothing has to cross between parts.
All inputs are finite; a program needn't handle non-finite values.
Results may differ from the reference program's by a relative error of at most 0.018.
The reference program's roundings to bfloat16 on the way count: a program that leaves them out, or rounds other values in their place, can miss the bound.
Values may be sent and summed in bfloat16 or wider, within the bound.
A program may use at most 128 MiB of HBM per device.

```python
import math
import jax
import jax.numpy as jnp
from jax import lax

D = 2048
DELTA_HEADS = 8
HEAD = 128
LATENT_HEADS = 16
NOPE = 64
ROPE = 32
VDIM = 64
QRANK = 512
KVRANK = 256
BLOCK = 64
SEQS = 4
LENGTH = 256


def draw_decay_rate(key, part):
    slow_key, fast_key, order_key = jax.random.split(key, 3)
    slow_rate = jnp.exp(jax.random.uniform(slow_key, (DELTA_HEADS,), jnp.float32, math.log(0.3), math.log(1.5))) / LENGTH
    fast_rate = jnp.exp(jax.random.uniform(fast_key, (DELTA_HEADS,), jnp.float32, math.log(0.025), math.log(0.06)))
    head_order = jax.random.permutation(order_key, DELTA_HEADS)
    return jnp.where(head_order < DELTA_HEADS // 2, fast_rate, slow_rate)


def column_scaled(key, row_count):
    entry_key, jitter_key = jax.random.split(key)
    entries = jnp.clip(jax.random.normal(entry_key, (row_count, D), jnp.float32), -6.0, 6.0)
    jitter = jax.random.uniform(jitter_key, (D,), jnp.float32, -0.5, 0.5)
    column_tilt = 2.2 * (jnp.arange(D, dtype=jnp.float32) / D - 0.5)
    fan_scale = (DELTA_HEADS * HEAD + LATENT_HEADS * VDIM) ** (-0.5)
    return entries * jnp.exp(column_tilt + jitter)[None, :] * fan_scale


def draw_delta_out(key, part):
    return column_scaled(jax.random.fold_in(key, 11), DELTA_HEADS * HEAD).astype(jnp.bfloat16)


def draw_latent_out(key, part):
    return column_scaled(jax.random.fold_in(key, 23), LATENT_HEADS * VDIM).astype(jnp.bfloat16)


def expansion_base(key, rank, head_width):
    entries = jnp.clip(jax.random.normal(key, (rank, LATENT_HEADS, head_width), jnp.float32), -6.0, 6.0)
    return entries / math.sqrt(rank)


def draw_query_up(key, part):
    entries = expansion_base(jax.random.fold_in(key, 31), QRANK, NOPE + ROPE)
    return entries.reshape(QRANK, LATENT_HEADS * (NOPE + ROPE)).astype(jnp.bfloat16)


def draw_latent_up(key, part):
    entries = expansion_base(jax.random.fold_in(key, 53), KVRANK, NOPE + VDIM)
    return entries.reshape(KVRANK, LATENT_HEADS * (NOPE + VDIM)).astype(jnp.bfloat16)


def shard_levels(stream_key, extent, cuts, low, largest):
    def one(axis_at, parts):
        heights = jax.random.uniform(jax.random.fold_in(jax.random.fold_in(stream_key, 6), axis_at), (parts,), jnp.float32, low / len(cuts), largest / len(cuts))
        return jnp.repeat(jnp.exp(heights), extent[axis_at] // parts).reshape((-1,) + (1,) * (len(extent) - axis_at - 1))

    factor_of = one(*cuts[0])
    for cut in cuts[1:]:
        factor_of = factor_of * one(*cut)
    return factor_of


def gaussian(stream_key, dims, scale, limit, cuts=(), held_as=jnp.bfloat16):
    result = scale * jax.random.normal(stream_key, dims, jnp.float32)
    if cuts:
        result = result * shard_levels(stream_key, dims, cuts, -0.22, 0.18)
    return jnp.clip(result, -limit, limit).astype(held_as)


def setup_inputs(seed: int = 0, part: int = 0) -> dict:
    key_of = jax.random.split(jax.random.key(seed), 20)
    own_keys = jax.random.split(jax.random.fold_in(key_of[19], part), 20)
    tokens = gaussian(own_keys[0], (SEQS, LENGTH, D), 1.0, 6.0, ((0, 2), (1, 4)))
    pre_gain = jnp.clip(1.0 + 0.18 * jax.random.normal(key_of[1], (D,), jnp.float32), 0.1, 1.9)
    query_weight = gaussian(key_of[2], (D, DELTA_HEADS * HEAD), D ** -0.5, 0.125, ((0, 8), (1, 2)))
    key_weight = gaussian(key_of[3], (D, DELTA_HEADS * HEAD), D ** -0.5, 0.125, ((0, 8), (1, 2)))
    value_weight = gaussian(key_of[4], (D, DELTA_HEADS * HEAD), D ** -0.5, 0.125, ((0, 8), (1, 2)))
    beta_weight = gaussian(key_of[5], (D, DELTA_HEADS), D ** -0.5, 0.125)
    decay_weight = gaussian(key_of[6], (D, DELTA_HEADS), D ** -0.5, 0.125)
    decay_rate = draw_decay_rate(jax.random.fold_in(key_of[19], 71), part)
    delta_gain = jnp.clip(1.0 + 0.18 * jax.random.normal(key_of[8], (HEAD,), jnp.float32), 0.1, 1.9)
    query_down = gaussian(key_of[9], (D, QRANK), D ** -0.5, 0.125, ((0, 8),))
    latent_down = gaussian(key_of[10], (D, KVRANK), D ** -0.5, 0.125, ((0, 8),))
    rope_weight = gaussian(key_of[11], (D, ROPE), D ** -0.5, 0.125)
    query_gain = jnp.clip(1.0 + 0.18 * jax.random.normal(key_of[12], (QRANK,), jnp.float32), 0.1, 1.9)
    latent_gain = jnp.clip(1.0 + 0.18 * jax.random.normal(key_of[13], (KVRANK,), jnp.float32), 0.1, 1.9)
    query_up = draw_query_up(jax.random.fold_in(key_of[19], 71), part)
    latent_up = draw_latent_up(jax.random.fold_in(key_of[19], 71), part)
    delta_out = draw_delta_out(jax.random.fold_in(key_of[19], 71), part)
    latent_out = draw_latent_out(jax.random.fold_in(key_of[19], 71), part)
    post_gain = jnp.clip(1.0 + 0.18 * jax.random.normal(key_of[18], (D,), jnp.float32), 0.1, 1.9)
    return dict(tokens=tokens, pre_gain=pre_gain, query_weight=query_weight, key_weight=key_weight, value_weight=value_weight, beta_weight=beta_weight, decay_weight=decay_weight, decay_rate=decay_rate, delta_gain=delta_gain, query_down=query_down, latent_down=latent_down, rope_weight=rope_weight, query_gain=query_gain, latent_gain=latent_gain, query_up=query_up, latent_up=latent_up, delta_out=delta_out, latent_out=latent_out, post_gain=post_gain)


NORM_EPS = 1e-06
ROPE_THETA = 10000.0
HIGHEST = lax.Precision.HIGHEST

def stored(values):
    return lax.optimization_barrier(values.astype(jnp.bfloat16))

def rms_scale(values):
    return lax.rsqrt(lax.optimization_barrier(jnp.mean(values * values, axis=-1, keepdims=True)) + NORM_EPS)

def unit_rows(values):
    return values * lax.rsqrt(lax.optimization_barrier(jnp.sum(values * values, axis=-1, keepdims=True)) + NORM_EPS)

def rope_tables(positions, rope_width):
    frequency = ROPE_THETA ** (-jnp.arange(0, rope_width, 2, dtype=jnp.float32) / rope_width)
    angles = positions.astype(jnp.float32)[:, None] * frequency[None, :]
    return (jnp.cos(angles), jnp.sin(angles))

def rotate(values, cosine_table, sine_table):
    lower_half, upper_half = jnp.split(values, 2, axis=-1)
    return jnp.concatenate([lower_half * cosine_table - upper_half * sine_table, upper_half * cosine_table + lower_half * sine_table], axis=-1)

def delta_terms(query_vectors, key_vectors, value_vectors, beta_gate, log_decay):
    length, head_count, head_width = query_vectors.shape
    nblocks = length // BLOCK

    def split_blocks(tensor):
        return jnp.moveaxis(tensor.reshape((nblocks, BLOCK, head_count) + tensor.shape[2:]), 2, 0)
    query_vectors = split_blocks(query_vectors)
    key_vectors = split_blocks(key_vectors)
    value_vectors = split_blocks(value_vectors)
    beta_gate = split_blocks(beta_gate)
    gate_sum = jnp.cumsum(split_blocks(log_decay), axis=-1)
    position = jnp.arange(BLOCK)
    strict = position[:, None] > position[None, :]
    causal = position[:, None] >= position[None, :]
    gate_gap = gate_sum[..., :, None] - gate_sum[..., None, :]
    strict_decay = jnp.where(strict, jnp.exp(jnp.where(strict, gate_gap, 0.0)), 0.0)
    causal_decay = jnp.where(causal, jnp.exp(jnp.where(causal, gate_gap, 0.0)), 0.0)
    keys_scaled = key_vectors * beta_gate[..., None]
    lower_mat = jnp.einsum('hnid,hnjd->hnij', keys_scaled, key_vectors, precision=HIGHEST) * strict_decay
    identity = jnp.eye(BLOCK, dtype=jnp.float32)
    inverse = jax.scipy.linalg.solve_triangular(identity + lower_mat, jnp.broadcast_to(identity, lower_mat.shape), lower=True)
    new_values = jnp.einsum('hnij,hnjd->hnid', inverse, value_vectors * beta_gate[..., None], precision=HIGHEST)
    key_weights = jnp.einsum('hnij,hnjd->hnid', inverse, keys_scaled * jnp.exp(gate_sum)[..., None], precision=HIGHEST)
    scores = jnp.einsum('hnid,hnjd->hnij', query_vectors, key_vectors, precision=HIGHEST) * causal_decay
    last_gate = gate_sum[..., -1]
    query_decay = query_vectors * jnp.exp(gate_sum)[..., None]
    key_decay = key_vectors * jnp.exp(last_gate[..., None] - gate_sum)[..., None]
    return (query_decay, key_decay, new_values, key_weights, scores, last_gate)

def delta_rule(query_vectors, key_vectors, value_vectors, beta_gate, log_decay):
    head_count, head_width = (query_vectors.shape[1], query_vectors.shape[2])
    block_terms = delta_terms(query_vectors, key_vectors, value_vectors, beta_gate, log_decay)
    inputs = tuple((jnp.moveaxis(tensor, 1, 0) for tensor in block_terms))

    def advance(carried, block_in):
        query_decay, key_decay, new_values, key_weights, scores, last_gate = block_in
        corrected = new_values - jnp.einsum('hcd,hde->hce', key_weights, carried, precision=HIGHEST)
        output = jnp.einsum('hcd,hde->hce', query_decay, carried, precision=HIGHEST) + jnp.einsum('hij,hje->hie', scores, corrected, precision=HIGHEST)
        carried = carried * jnp.exp(last_gate)[:, None, None] + jnp.einsum('hcd,hce->hde', key_decay, corrected, precision=HIGHEST)
        return (carried, output)
    zero_state = jnp.zeros((head_count, head_width, head_width), jnp.float32)
    _, outputs = lax.scan(advance, zero_state, inputs)
    return jnp.transpose(outputs, (0, 2, 1, 3)).reshape(-1, head_count, head_width)

def reference(tokens, pre_gain, query_weight, key_weight, value_weight, beta_weight, decay_weight, decay_rate, delta_gain, query_down, latent_down, rope_weight, query_gain, latent_gain, query_up, latent_up, delta_out, latent_out, post_gain):
    f32 = jnp.float32

    def one_sequence(sequence):
        length = sequence.shape[0]
        positions = jnp.arange(length)
        seq_float = sequence.astype(f32)
        normed = stored(seq_float * rms_scale(seq_float) * pre_gain)
        raw_query = stored(jnp.dot(normed, query_weight, preferred_element_type=f32))
        raw_key = stored(jnp.dot(normed, key_weight, preferred_element_type=f32))
        raw_value = stored(jnp.dot(normed, value_weight, preferred_element_type=f32))
        q_latent = stored(jnp.dot(normed, query_down, preferred_element_type=f32))
        kv_latent = stored(jnp.dot(normed, latent_down, preferred_element_type=f32))
        rope_raw = stored(jnp.dot(normed, rope_weight, preferred_element_type=f32))
        beta_gate = jax.nn.sigmoid(jnp.dot(normed, beta_weight, preferred_element_type=f32))
        log_decay = -decay_rate[None, :] * jax.nn.softplus(jnp.dot(normed, decay_weight, preferred_element_type=f32))
        query_vectors = unit_rows(jax.nn.silu(raw_query.astype(f32)).reshape(length, DELTA_HEADS, HEAD)) * HEAD ** (-0.5)
        key_vectors = unit_rows(jax.nn.silu(raw_key.astype(f32)).reshape(length, DELTA_HEADS, HEAD))
        value_vectors = jax.nn.silu(raw_value.astype(f32)).reshape(length, DELTA_HEADS, HEAD)
        delta_raw = delta_rule(query_vectors, key_vectors, value_vectors, beta_gate, log_decay)
        delta_heads = stored(delta_raw * rms_scale(delta_raw) * delta_gain).reshape(length, DELTA_HEADS * HEAD)
        q_lat32 = q_latent.astype(f32)
        kv_lat32 = kv_latent.astype(f32)
        q_normed = stored(q_lat32 * rms_scale(q_lat32) * query_gain)
        kv_normed = stored(kv_lat32 * rms_scale(kv_lat32) * latent_gain)
        cosine_table, sine_table = rope_tables(positions, ROPE)
        rope_keys = stored(rotate(rope_raw.astype(f32), cosine_table, sine_table)).astype(f32)
        query_all = stored(jnp.dot(q_normed, query_up, preferred_element_type=f32)).reshape(length, LATENT_HEADS, NOPE + ROPE)
        kv_all = stored(jnp.dot(kv_normed, latent_up, preferred_element_type=f32)).reshape(length, LATENT_HEADS, NOPE + VDIM)
        query_plain = query_all[..., :NOPE].astype(f32)
        query_turned = stored(rotate(query_all[..., NOPE:].astype(f32), cosine_table[:, None, :], sine_table[:, None, :])).astype(f32)
        key_plain = kv_all[..., :NOPE].astype(f32)
        value_rows = kv_all[..., NOPE:].astype(f32)
        score_scale = (NOPE + ROPE) ** (-0.5)
        query_span = math.gcd(length, 512)
        key_block = positions // BLOCK

        def attend(block_index):
            row_start = block_index * query_span
            plain_rows = lax.dynamic_slice_in_dim(query_plain, row_start, query_span, 0)
            turned_rows = lax.dynamic_slice_in_dim(query_turned, row_start, query_span, 0)
            logits = (jnp.einsum('qhd,khd->hqk', plain_rows, key_plain) + jnp.einsum('qhd,kd->hqk', turned_rows, rope_keys)) * score_scale
            query_block = (row_start + jnp.arange(query_span)) // BLOCK
            allowed = key_block[None, :] <= query_block[:, None]
            logits = jnp.where(allowed[None], logits, -jnp.inf)
            peak = lax.optimization_barrier(jnp.max(logits, axis=-1, keepdims=True))
            weights = jnp.where(allowed[None], jnp.exp(logits - peak), 0.0)
            row_sum = lax.optimization_barrier(jnp.sum(weights, axis=-1))
            weights_b = stored(weights).astype(f32)
            weighted = jnp.einsum('hqk,khd->qhd', weights_b, value_rows)
            return stored(weighted / jnp.transpose(row_sum)[:, :, None]).reshape(query_span, LATENT_HEADS * VDIM)
        latent_heads = lax.map(attend, jnp.arange(length // query_span)).reshape(length, LATENT_HEADS * VDIM)
        half_delta = DELTA_HEADS * HEAD // 2
        half_latent = LATENT_HEADS * VDIM // 2
        mixed = jnp.zeros((length, D), f32)
        for group_index in range(2):
            group_heads = jnp.concatenate([delta_heads[:, group_index * half_delta:(group_index + 1) * half_delta], latent_heads[:, group_index * half_latent:(group_index + 1) * half_latent]], axis=1)
            group_rows = jnp.concatenate([delta_out[group_index * half_delta:(group_index + 1) * half_delta], latent_out[group_index * half_latent:(group_index + 1) * half_latent]], axis=0)
            group_term = jnp.dot(group_heads, group_rows, preferred_element_type=f32)
            mixed = mixed + stored(group_term).astype(f32)
        return (mixed * rms_scale(mixed) * post_gain).astype(jnp.bfloat16)
    return lax.map(one_sequence, tokens)
```

```python
import functools
import math

import jax
import jax.numpy as jnp
from jax import lax
from jax.experimental import pallas as pl
from jax.experimental.pallas import tpu as pltpu
from jax.sharding import PartitionSpec as P

HEAD = 128
NOPE = 64
ROPE = 32
VDIM = 64
BLOCK = 64
NORM_EPS = 1e-06
ROPE_THETA = 10000.0
HIGHEST = lax.Precision.HIGHEST
MESH = pl.DeviceIdType.MESH
F32 = jnp.float32
BF16 = jnp.bfloat16


def dot(a, b, precision=None):
    return jnp.dot(a, b, preferred_element_type=F32, precision=precision)


def dot_t(a, b, precision=None):
    return lax.dot_general(
        a, b, (((1,), (1,)), ((), ())), preferred_element_type=F32, precision=precision
    )


def t_dot(a, b, precision=None):
    return lax.dot_general(
        a, b, (((0,), (0,)), ((), ())), preferred_element_type=F32, precision=precision
    )


def when(cond, fn):
    if cond is True:
        fn()
    elif cond is not False:
        pl.when(cond)(fn)


def both(a, b):
    if a is True:
        return b
    if b is True:
        return a
    return jnp.logical_and(a, b)


class Place:
    def __init__(self, sizes):
        self.Y, self.Z, self.X, self.C = sizes
        self.y = lax.axis_index("grp")
        self.z = lax.axis_index("sp")
        self.x = lax.axis_index("fs")
        self.c = lax.axis_index("tp")


def greet(place, plane=True, later=False):
    barrier = pltpu.get_barrier_semaphore()

    def signal(cond, dev):
        when(
            cond,
            lambda: pl.semaphore_signal(barrier, inc=1, device_id=dev, device_id_type=MESH),
        )

    count = jnp.int32(0)
    if later:
        for k in range(1, place.Z):
            signal(place.z + k < place.Z, {"sp": place.z + k})
            signal(place.z - k >= 0, {"sp": place.z - k})
        count += place.Z - 1
    else:
        signal(place.z + 1 < place.Z, {"sp": place.z + 1})
        signal(place.z > 0, {"sp": place.z - 1})
        count += (place.z + 1 < place.Z).astype(jnp.int32) + (place.z > 0).astype(jnp.int32)
    if plane:
        for d in range(1, place.X):
            signal(True, {"fs": lax.rem(place.x + d, place.X)})
        count += place.X - 1
        if place.Y == 2:
            signal(True, {"grp": 1 - place.y})
            count += 1
    signal(True, {"tp": 1 - place.c})
    count += 1
    pl.semaphore_wait(barrier, count)


class Gather:
    def __init__(self, place, own, buf, send, recv, lsem):
        self.pl, self.own, self.buf = place, own, buf
        self.send, self.recv, self.lsem = send, recv, lsem
        self.sends = []
        self.ev = 0

    def active(self, p):
        return True if p == 2 else self.pl.y == p

    def push(self, cond, src, p, slot, dev, ev, way):
        index = len(self.sends)

        def make():
            return pltpu.make_async_remote_copy(
                src_ref=src,
                dst_ref=self.buf(p, slot),
                send_sem=self.send.at[index],
                recv_sem=self.recv.at[slot, p],
                device_id=dev,
                device_id_type=MESH,
            )

        when(cond, lambda: make().start())
        self.sends.append((cond, make))

    def arrived(self, cond, p, slot):
        def wait():
            ref = self.buf(p, slot)
            pltpu.make_async_remote_copy(
                src_ref=ref,
                dst_ref=ref,
                send_sem=self.lsem.at[p],
                recv_sem=self.recv.at[slot, p],
                device_id={"tp": self.pl.c},
                device_id_type=MESH,
            ).wait_recv()

        when(cond, wait)

    def across(self, cond, src, p, slot, ev):
        q = self.pl
        for d in range(1, q.X):
            self.push(cond, src, p, slot, {"fs": lax.rem(q.x + d, q.X)}, ev, 1 + d)

    def to_y(self, cond, src, p, slot, ev):
        if p < 2:
            self.push(cond, src, p, slot, {"grp": 1 - self.pl.y}, ev, 0)

    def kinds(self):
        return (0, 1, 2)

    def start_along(self):
        q = self.pl
        me = q.z * q.X + q.x
        for p in self.kinds():
            a = self.active(p)
            src = self.own(p)
            self.push(both(a, q.z + 1 < q.Z), src, p, me, {"sp": q.z + 1}, 0, 0)
            self.push(both(a, q.z > 0), src, p, me, {"sp": q.z - 1}, 0, 1)

    def start_across(self):
        q = self.pl
        me = q.z * q.X + q.x
        for p in self.kinds():
            self.across(self.active(p), self.own(p), p, me, 0)
        for p in self.kinds():
            pltpu.make_async_copy(self.own(p), self.buf(p, me), self.lsem.at[p]).start()

    def step(self, k):
        q = self.pl
        for p in self.kinds():
            a = self.active(p)
            for sign in (1, -1):
                zz = q.z - sign * k
                ok = both(a, jnp.logical_and(zz >= 0, zz < q.Z))
                slot = zz * q.X + q.x
                nxt = q.z + sign
                ev = 2 * k - (sign == 1)
                self.arrived(ok, p, slot)
                ref = self.buf(p, slot)
                self.push(
                    both(ok, jnp.logical_and(nxt >= 0, nxt < q.Z)),
                    ref, p, slot, {"sp": nxt}, ev, 1,
                )
                self.across(ok, ref, p, slot, ev)
                self.to_y(ok, ref, p, slot, ev)

    def cross_step(self, k):
        q = self.pl
        base = 2 * q.Z
        for p in self.kinds():
            a = self.active(p)
            for sign in (1, -1) if k else (1,):
                zz = q.z - sign * k
                ok = both(a, jnp.logical_and(zz >= 0, zz < q.Z))
                for d in range(1, q.X):
                    slot = zz * q.X + lax.rem(q.x + d, q.X)
                    ev = base + (2 * k - (sign == 1) + 1) * (q.X - 1) + d - 1
                    self.arrived(ok, p, slot)
                    self.to_y(ok, self.buf(p, slot), p, slot, ev)

    def finish(self):
        q = self.pl
        self.cross_step(q.Z - 1)
        me = q.z * q.X + q.x
        for p in (0, 1):
            for s in range(q.Z * q.X):
                self.arrived(jnp.logical_and(q.y != p, me != s), p, s)
        for p in self.kinds():
            pltpu.make_async_copy(self.own(p), self.buf(p, me), self.lsem.at[p]).wait()

    def drain(self):
        for cond, make in self.sends:
            when(cond, lambda make=make: make().wait_send())

    @staticmethod
    def scratch(Z, X):
        n = Z * X
        sends = 3 * (X + 1) + 2 * (Z - 1) * (3 * X + 2) + (2 * Z - 1) * (X - 1) * 2
        return [
            pltpu.SemaphoreType.DMA((sends,)),
            pltpu.SemaphoreType.DMA((n, 3)),
            pltpu.SemaphoreType.DMA((3,)),
        ]


def spread(copies, parts, target, bounds):
    at = 0
    for ref, offset, width in parts:
        done = 0
        while done < width:
            p, col = divmod(at + done, bounds)
            size = min(width - done, bounds - col)
            start = offset + done
            if not isinstance(start, int):
                start = pl.multiple_of(start, 128)
            copies.append((ref.at[:, pl.ds(start, size)], target.at[p, :, pl.ds(col, size)]))
            done += size
        at += width


def back_kernel(
    sizes, seqs, heads, cuts, tokens, pre_gain, small, w_query, w_key, w_value, w_qdown, w_kdown,
    w_delta, w_latent, qgain, kgain, w_qup, w_lup, rate_in, gain, post,
    out, qup, lup, raw, lat, rate, own1, own, buf1, kvr, kbuf, sin, sout, hbuf, buf, pbuf, rbuf, sq,
    asem, ksem, ssem, send1, recv1, lsem1, send, recv, lsem, tsem,
):
    place = Place(sizes)
    Z, z, c = place.Z, place.z, place.c
    C = sizes[3]
    rows = tokens.shape[0]
    third = own1.shape[2]
    qcols, kcols = w_qdown.shape[1] // C, w_kdown.shape[1] // C
    pairs = []
    spread(
        pairs,
        [(w, 0, w.shape[1]) for w in (w_query, w_key, w_value)]
        + [(w_qdown, c * qcols, qcols), (w_kdown, c * kcols, kcols)],
        own1, third,
    )
    upper = w_delta.shape[0]
    pairs.append((w_delta, own.at[pl.ds(0, upper)]))
    pairs.append((w_latent, own.at[pl.ds(upper, w_latent.shape[0])]))
    loads = [pltpu.make_async_copy(a, b, asem.at[i]) for i, (a, b) in enumerate(pairs)]
    for load in loads:
        load.start()
    greet(place, later=True)
    for load in loads:
        load.wait()
    g1 = Gather(
        place, lambda p: own1.at[p], lambda p, s: buf1.at[p, s], send1, recv1, lsem1
    )
    g = Gather(
        place,
        lambda p: own.at[pl.ds(cuts[p], cuts[p + 1] - cuts[p])],
        lambda p, s: buf.at[s, pl.ds(cuts[p], cuts[p + 1] - cuts[p])],
        send, recv, lsem,
    )
    g1.start_along()
    g1.start_across()
    x = tokens[...].astype(F32)
    xscale = lax.rsqrt(jnp.mean(x * x, axis=-1, keepdims=True) + NORM_EPS)
    normed = (x * xscale * pre_gain[...]).astype(BF16)
    sm_all = dot_t(normed, small[...])
    qcol = w_qup.shape[1]
    lh = qcol // (NOPE + ROPE)
    turn_w = ROPE // 2
    kinds = ((NOPE, 0, qup, w_qup, NOPE + ROPE), (turn_w, NOPE, qup, w_qup, NOPE + ROPE),
             (turn_w, NOPE + turn_w, qup, w_qup, NOPE + ROPE),
             (NOPE, 0, lup, w_lup, NOPE + VDIM), (VDIM, NOPE, lup, w_lup, NOPE + VDIM))
    fill_at = {}
    for w, off, to, frm, per in kinds:
        size = lh * w
        dst_i = lax.broadcasted_iota(jnp.int32, (frm.shape[1], size), 1)
        src_i = lax.broadcasted_iota(jnp.int32, (frm.shape[1], size), 0)
        perm = jnp.where(src_i == dst_i // w * per + off + dst_i % w, 1.0, 0.0).astype(BF16)
        lo = fill_at.get(per, 0)
        to[:, lo : lo + size] = dot(frm[...], perm).astype(BF16)
        fill_at[per] = lo + size
    for k in range(1, Z):
        g1.step(k)
        g1.cross_step(k - 1)
        if k == max(1, Z - 2):
            g.start_along()
    g.start_across()
    if Z > 1:
        g.step(1)
    g1.finish()
    depth1 = buf1.shape[1] * buf1.shape[2]
    part2 = dot(normed, buf1[2].reshape(depth1, third)).astype(BF16)
    lat[c] = part2[:, third - qcols - kcols :]
    trade = pltpu.make_async_remote_copy(
        src_ref=lat.at[c], dst_ref=lat.at[c], send_sem=tsem.at[4], recv_sem=tsem.at[5],
        device_id={"tp": 1 - c}, device_id_type=MESH,
    )
    trade.start()
    raw[:, 2 * third : 3 * third] = part2
    for p in range(2):
        raw[:, p * third : (p + 1) * third] = dot(
            normed, buf1[p].reshape(depth1, third)
        ).astype(BF16)
    trade.wait()
    qw = qup.shape[0] // sizes[3]
    kw_lat = lup.shape[0] // sizes[3]
    tile = 128
    lane = lax.broadcasted_iota(jnp.int32, (rows, tile), 1)
    half_turn = ROPE // 2
    step = (lane % half_turn).astype(F32)
    row = lax.broadcasted_iota(jnp.int32, (rows, tile), 0)
    pos = (z * BLOCK + row % BLOCK).astype(F32)
    angle = pos * jnp.exp(step * (-2.0 * math.log(ROPE_THETA) / ROPE))
    cos, sin_t = jnp.cos(angle), jnp.sin(angle)

    def normed_parts(lo, w, g):
        parts = [lat[i, :, lo : lo + w].astype(F32) for i in range(sizes[3])]
        squares = sum(jnp.sum(p * p, axis=-1, keepdims=True) for p in parts)
        scale = lax.rsqrt(squares / (w * sizes[3]) + NORM_EPS)
        return [
            (p * scale * g[:, i * w : (i + 1) * w]).astype(BF16) for i, p in enumerate(parts)
        ]

    kparts = normed_parts(qw, kw_lat, kgain)
    krank = kw_lat * sizes[3]
    for i, p in enumerate(kparts):
        kvr[:, i * kw_lat : (i + 1) * kw_lat] = p
    allheads = heads * C
    src = lax.broadcasted_iota(jnp.int32, (tile, tile), 0)
    dst = lax.broadcasted_iota(jnp.int32, (tile, tile), 1)
    rope_raw = sm_all.astype(BF16)
    base = 2 * allheads + dst % half_turn

    def pick(cond, kind):
        return jnp.where(cond, 1.0, 0.0).astype(kind)

    rlo = dot(rope_raw, pick(src == base, BF16))
    rhi = dot(rope_raw, pick(src == base + half_turn, BF16))
    left = lane < tile // 2
    kvr[:, krank : krank + tile] = jnp.where(
        left, rlo * cos - rhi * sin_t, rhi * cos + rlo * sin_t
    ).astype(BF16)

    def kv_copy(k):
        return pltpu.make_async_remote_copy(
            src_ref=kvr,
            dst_ref=kbuf.at[z],
            send_sem=ksem.at[0, k],
            recv_sem=ksem.at[1, z],
            device_id={"sp": z + k},
            device_id_type=MESH,
        )

    for k in range(1, Z):
        when(z + k < Z, lambda k=k: kv_copy(k).start())
    ri = lax.broadcasted_iota(jnp.int32, (rows, rows), 0)
    ci = lax.broadcasted_iota(jnp.int32, (rows, rows), 1)
    tri = jnp.where((ri >= ci) & (ri // BLOCK == ci // BLOCK), 1.0, 0.0).astype(F32)
    rate[...] = jnp.zeros(rate.shape, F32)
    rate[:, allheads : 2 * allheads] = rate_in[...]
    first_head = c * heads
    own_beta = pick((dst < heads) & (src == first_head + dst), F32)
    own_rate = pick(
        (dst >= heads) & (dst < 2 * heads) & (src == allheads + first_head + dst - heads), F32
    )
    pre = dot(sm_all, own_beta + own_rate, HIGHEST)
    rates = dot(jnp.broadcast_to(rate[...], (8, tile)), own_rate, HIGHEST)[:1]
    beta_all = jax.nn.sigmoid(pre)
    log_a = -rates * (jnp.maximum(pre, 0.0) + jnp.log1p(jnp.exp(-jnp.abs(pre))))
    gates = dot(tri, log_a, HIGHEST)
    gates_t = gates.T
    r = lax.broadcasted_iota(jnp.int32, (BLOCK, BLOCK), 0)
    cc = lax.broadcasted_iota(jnp.int32, (BLOCK, BLOCK), 1)
    strict = r > cc
    causal = r >= cc
    eye = jnp.where(r == cc, 1.0, 0.0).astype(F32)
    lanes = [(b, h) for b in range(seqs) for h in range(heads)]
    width = heads * HEAD
    terms = []
    for b, h in lanes:
        t = slice(b * BLOCK, (b + 1) * BLOCK)

        def act(i):
            v = raw[t, i * width + h * HEAD : i * width + (h + 1) * HEAD].astype(F32)
            return v * jax.nn.sigmoid(v)

        def unit(u):
            return u * lax.rsqrt(jnp.sum(u * u, axis=-1, keepdims=True) + NORM_EPS)

        q = unit(act(0)) * HEAD ** (-0.5)
        k = unit(act(1))
        v = act(2)
        beta = beta_all[t, h : h + 1]
        gcol = gates[t, heads + h : heads + h + 1]
        grow = gates_t[heads + h : heads + h + 1, t]
        glast = gates[(b + 1) * BLOCK - 1 : (b + 1) * BLOCK, heads + h : heads + h + 1]
        gap = gcol - grow
        decay = jnp.where(causal, jnp.exp(jnp.where(causal, gap, 0.0)), 0.0)
        ks = k * beta
        low = jnp.where(strict, dot_t(ks, k, HIGHEST) * decay, 0.0)
        scores = dot_t(q.astype(BF16), k.astype(BF16)) * decay
        eg = jnp.exp(gcol)
        terms.append([low, scores, v * beta, ks * eg, q * eg, k * jnp.exp(glast - gcol),
                      jnp.exp(glast)])
    every = range(len(lanes))
    inv = [eye - jnp.where((r // 2 == cc // 2), terms[i][0], 0.0) for i in every]
    size = 2
    while size < BLOCK:
        joint = (r // (2 * size) == cc // (2 * size)) & (r // size != cc // size)
        mids = [dot(jnp.where(joint, terms[i][0], 0.0), inv[i], HIGHEST) for i in every]
        inv = [inv[i] - dot(inv[i], mids[i], HIGHEST) for i in every]
        size *= 2
    inv = [m.astype(BF16) for m in inv]
    nv = [dot(inv[i], terms[i][2].astype(BF16)) for i in every]
    kw = [dot(inv[i], terms[i][3].astype(BF16)) for i in every]

    def state_copy(i):
        return pltpu.make_async_remote_copy(
            src_ref=sout.at[i],
            dst_ref=sin.at[i],
            send_sem=ssem.at[0, i],
            recv_sem=ssem.at[1, i],
            device_id={"sp": z + 1},
            device_id_type=MESH,
        )

    g.cross_step(0)
    if Z > 2:
        g.step(2)
    for i, (b, h) in enumerate(lanes):
        low, scores, vb, ke, qd, kd, factor = terms[i]

        def clear(i=i):
            sin[i] = jnp.zeros((HEAD, HEAD), BF16)

        when(z == 0, clear)
        when(z > 0, lambda i=i: state_copy(i).wait_recv())
        s_in = sin[i]
        corrected = nv[i] - dot(kw[i].astype(BF16), s_in)
        sout[i] = (
            s_in.astype(F32) * factor + t_dot(kd.astype(BF16), corrected.astype(BF16))
        ).astype(BF16)
        when(z + 1 < Z, lambda i=i: state_copy(i).start())
        o = dot(qd.astype(BF16), s_in) + dot(scores.astype(BF16), corrected.astype(BF16))
        o = o * lax.rsqrt(jnp.mean(o * o, axis=-1, keepdims=True) + NORM_EPS) * gain[...]
        hbuf[b * BLOCK : (b + 1) * BLOCK, h * HEAD : (h + 1) * HEAD] = o.astype(BF16)
    g.cross_step(1)
    for k in range(3, Z):
        g.step(k)
        if k < Z - 1:
            g.cross_step(k - 1)

    for k in range(1, Z):
        def take(k=k):
            pltpu.make_async_remote_copy(
                src_ref=kvr, dst_ref=kbuf.at[z - k], send_sem=ksem.at[0, k],
                recv_sem=ksem.at[1, z - k], device_id={"sp": z}, device_id_type=MESH,
            ).wait_recv()

        when(z - k >= 0, take)
    for s in range(Z):
        def fill(s=s):
            kbuf[s] = kvr[...]

        def none(s=s):
            kbuf[s] = jnp.zeros(kbuf.shape[1:], BF16)

        when(z == s, fill)
        when(z < s, none)
    qparts = normed_parts(0, qw, qgain)
    qa = sum(dot(p, qup[i * qw : (i + 1) * qw, :]) for i, p in enumerate(qparts)).astype(BF16)
    plain_width = qa.shape[1] - 2 * tile
    qlo_raw = qa[:, plain_width : plain_width + tile].astype(F32)
    qhi_raw = qa[:, plain_width + tile :].astype(F32)
    qlo = (qlo_raw * cos - qhi_raw * sin_t).astype(BF16)
    qhi = (qhi_raw * cos + qlo_raw * sin_t).astype(BF16)
    lane1 = lax.broadcasted_iota(jnp.int32, (1, tile), 1)

    def keep(cond):
        return jnp.where(cond, 1.0, 0.0).astype(BF16)

    keys = Z * BLOCK
    allowed = lax.broadcasted_iota(jnp.int32, (2 * BLOCK, keys), 1) // BLOCK <= z
    left_half = lax.broadcasted_iota(jnp.int32, (BLOCK, tile), 1) < tile // 2
    for b in range(seqs):
        t = slice(b * BLOCK, (b + 1) * BLOCK)
        kv = jnp.concatenate([kbuf[s, t, :] for s in range(Z)], axis=0)
        up = dot(kv[:, :krank], lup[...]).astype(BF16)
        turn = kv[:, krank : krank + tile].astype(F32)
        rolled = pltpu.roll(turn, tile // 2, 1)
        sel = lax.broadcasted_iota(jnp.int32, (keys, tile), 1) < tile // 2
        klo = jnp.where(sel, turn, rolled).astype(BF16)
        khi = jnp.where(sel, rolled, turn).astype(BF16)
        for j in range(plain_width // tile):
            at = slice(j * tile, (j + 1) * tile)
            qp = qa[t, at]
            first, second = keep(lane1 < tile // 2), keep(lane1 >= tile // 2)
            m0, m1 = keep(lane1 // half_turn == 2 * j), keep(lane1 // half_turn == 2 * j + 1)
            s = (
                dot_t(jnp.concatenate([qp * first, qp * second], axis=0), up[:, at])
                + dot_t(jnp.concatenate([qlo[t] * m0, qlo[t] * m1], axis=0), klo)
                + dot_t(jnp.concatenate([qhi[t] * m0, qhi[t] * m1], axis=0), khi)
            ) * (NOPE + ROPE) ** (-0.5)
            s = jnp.where(allowed, s, -jnp.inf)
            w = jnp.exp(s - jnp.max(s, axis=-1, keepdims=True))
            o = dot(w.astype(BF16), up[:, plain_width + j * tile : plain_width + (j + 1) * tile])
            o = o / jnp.sum(w, axis=-1, keepdims=True)
            hbuf[t, width + j * tile : width + (j + 1) * tile] = jnp.where(
                left_half, o[:BLOCK], o[BLOCK:]
            ).astype(BF16)
    if Z > 3:
        g.cross_step(Z - 2)
    g.finish()
    n = buf.shape[0]
    half = n // 2
    hv = hbuf[...]

    def part(s, carry):
        pbuf[s] = dot(hv, buf[s]).astype(BF16)
        return carry

    lax.fori_loop(0, n, part, 0)
    peer = 1 - c
    copy = pltpu.make_async_remote_copy(
        src_ref=pbuf.at[pl.ds(peer * half, half)],
        dst_ref=rbuf,
        send_sem=tsem.at[0],
        recv_sem=tsem.at[1],
        device_id={"tp": peer},
        device_id_type=MESH,
    )
    copy.start()
    g1.drain()
    g.drain()
    for k in range(1, Z):
        when(z + k < Z, lambda k=k: kv_copy(k).wait_send())
    for i in every:
        when(z + 1 < Z, lambda i=i: state_copy(i).wait_send())
    copy.wait()
    total = jnp.zeros((rows, 1), F32)
    mixed = []
    for s in range(half):
        m = pbuf[c * half + s].astype(F32) + rbuf[s].astype(F32)
        mixed.append(m)
        total = total + jnp.sum(m * m, axis=-1, keepdims=True)
    sq[0] = jnp.broadcast_to(total, sq.shape[1:])
    squares = pltpu.make_async_remote_copy(
        src_ref=sq.at[0],
        dst_ref=sq.at[1],
        send_sem=tsem.at[2],
        recv_sem=tsem.at[3],
        device_id={"tp": peer},
        device_id_type=MESH,
    )
    squares.start()
    squares.wait()
    total = total + sq[1][:, :1]
    cb = buf.shape[2]
    scale = lax.rsqrt(total / (n * cb) + NORM_EPS)
    for s in range(half):
        out[:, s * cb : (s + 1) * cb] = (mixed[s] * scale * post[s]).astype(BF16)


def vmem():
    return pl.BlockSpec(memory_space=pltpu.VMEM)


def anywhere():
    return pl.BlockSpec(memory_space=pl.ANY)


def local(
    sizes,
    tokens, pre_gain, query_weight, key_weight, value_weight, beta_weight, decay_weight,
    decay_rate, delta_gain, query_down, latent_down, rope_weight, query_gain, latent_gain,
    query_up, latent_up, delta_out, latent_out, post_gain,
):
    Y, Z, X, C = sizes
    n = Z * X
    seqs, count, width = tokens.shape
    if splits_by_heads(sizes, seqs, count, query_weight.shape, query_down.shape,
                       latent_down.shape, query_up.shape, latent_up.shape):
        return by_heads(
            sizes, tokens, pre_gain, query_weight, key_weight, value_weight, beta_weight,
            decay_weight, decay_rate, delta_gain, query_down, latent_down, rope_weight,
            query_gain, latent_gain, query_up, latent_up, delta_out, latent_out, post_gain,
        )
    rows = seqs * count
    qw = query_down.shape[1] // C
    kw = latent_down.shape[1] // C
    heads = query_weight.shape[1] // HEAD
    shard = query_weight.shape[0]
    third = (3 * query_weight.shape[1] + qw + kw) // 3
    small = [beta_weight.T, decay_weight.T, rope_weight.T]
    used = sum(w.shape[0] for w in small)
    small = jnp.concatenate(small + [jnp.zeros((128 - used, width), BF16)], axis=0)
    lanes = seqs * heads
    cb = delta_out.shape[1]
    depth = delta_out.shape[0] + latent_out.shape[0]
    cuts = (0, depth * 3 // 8, depth * 6 // 8, depth)
    half = n // 2
    kv_width = latent_down.shape[1] + 128
    args = (
        tokens.reshape(rows, width), pre_gain.reshape(1, width), small,
        query_weight, key_weight, value_weight, query_down, latent_down, delta_out, latent_out,
        query_gain.reshape(1, -1), latent_gain.reshape(1, -1), query_up, latent_up,
        decay_rate.reshape(1, -1), delta_gain.reshape(1, HEAD), post_gain.reshape(half, 1, cb),
    )
    result = pl.pallas_call(
        functools.partial(back_kernel, sizes, seqs, heads, cuts),
        name="layer",
        out_shape=jax.ShapeDtypeStruct((rows, half * cb), BF16),
        in_specs=[anywhere() if 3 <= i < 10 else vmem() for i in range(len(args))],
        out_specs=vmem(),
        scratch_shapes=[
            pltpu.VMEM(query_up.shape, BF16),
            pltpu.VMEM(latent_up.shape, BF16),
            pltpu.VMEM((rows, 3 * third), BF16),
            pltpu.VMEM((C, rows, qw + kw), BF16),
            pltpu.VMEM((1, 128), F32),
            pltpu.VMEM((3, shard, third), BF16),
            pltpu.VMEM((depth, cb), BF16),
            pltpu.VMEM((3, n, shard, third), BF16),
            pltpu.VMEM((rows, kv_width), BF16),
            pltpu.VMEM((Z, rows, kv_width), BF16),
            pltpu.VMEM((lanes, HEAD, HEAD), BF16),
            pltpu.VMEM((lanes, HEAD, HEAD), BF16),
            pltpu.VMEM((rows, depth), BF16),
            pltpu.VMEM((n, depth, cb), BF16),
            pltpu.VMEM((n, rows, cb), BF16),
            pltpu.VMEM((half, rows, cb), BF16),
            pltpu.VMEM((2, rows, 128), F32),
            pltpu.SemaphoreType.DMA((16,)),
            pltpu.SemaphoreType.DMA((2, Z)),
            pltpu.SemaphoreType.DMA((2, lanes)),
        ]
        + Gather.scratch(Z, X) + Gather.scratch(Z, X) + [pltpu.SemaphoreType.DMA((6,))],
        compiler_params=pltpu.CompilerParams(
            collective_id=0, has_side_effects=True, vmem_limit_bytes=60 * 1024 * 1024
        ),
    )(*args)
    return result.reshape(seqs, count, half * cb)


class Puts:
    def __init__(self, sems):
        self.sems, self.sent = sems, []

    def put(self, cond, src, dst, recv, dev):
        index = len(self.sent)

        def make():
            return pltpu.make_async_remote_copy(
                src_ref=src, dst_ref=dst, send_sem=self.sems.at[index], recv_sem=recv,
                device_id=dev, device_id_type=MESH,
            )

        when(cond, lambda: make().start())
        self.sent.append((cond, make))

    def drain(self):
        for cond, make in self.sent:
            when(cond, lambda make=make: make().wait_send())


def landed(cond, ref, dummy, recv, c):
    def wait():
        pltpu.make_async_remote_copy(
            src_ref=ref, dst_ref=ref, send_sem=dummy, recv_sem=recv,
            device_id={"tp": c}, device_id_type=MESH,
        ).wait_recv()

    when(cond, wait)


def heads_kernel(
    sizes, seqs, cuts, tokens, pre_gain, w_beta, w_decay, w_rope, w_query, w_key, w_value,
    w_qdown, w_kdown, w_delta, w_latent, qgain, kgain, w_qup, w_lup, rate_in, gain, post,
    out, tok, beta_v, decay_v, rope_v, qup_v, lup_v, wown, wbuf, nbuf, ssel, qsel, turn_a, turn_b,
    raw, sm, lat, hsrc, hbuf, own, buf, pbuf, rbuf, sq,
    asem, wsend, wrecv, nsend, nrecv, lsend, lrecv, hsend, hrecv, osem, dummy,
    send, recv, lsem, tsem,
):
    place = Place(sizes)
    Z, X = place.Z, place.X
    y, z, x, c = place.y, place.z, place.x, place.c
    tile = 128
    shard = wown.shape[1]
    part = shard // 2
    me = z * X + x
    nk = w_kdown.shape[1] // tile
    kblock = lax.rem(z, nk)
    length = Z * BLOCK
    count = seqs * length
    width = nbuf.shape[3]
    ncol = wown.shape[2]
    loads = []

    def load(src, dst, cond=True):
        index = len(loads)

        def make():
            return pltpu.make_async_copy(src, dst, asem.at[index])

        when(cond, lambda: make().start())
        loads.append(make)
        return index

    first = []
    for d in range(Z):
        for i, w in enumerate((w_query, w_key, w_value)):
            at = wown.at[d, :, pl.ds(i * tile, tile)]
            first.append(load(w.at[:, pl.ds(d * tile, tile)], at))
        at = wown.at[d, :, pl.ds(3 * tile, tile)]
        index = load(w_qdown.at[:, pl.ds(d * tile, tile)], at, c == 0)
        first.append(index)
        kd = d % nk

        def other(kd=kd, at=at, index=index):
            pltpu.make_async_copy(
                w_kdown.at[:, pl.ds(kd * tile, tile)], at, asem.at[index]
            ).start()

        when(c == 1, other)
    tok_at = load(tokens, tok)
    rest = [load(a, b) for a, b in (
        (w_beta, beta_v), (w_decay, decay_v), (w_rope, rope_v), (w_qup, qup_v), (w_lup, lup_v),
    )]
    upper = w_delta.shape[0]
    outs = [load(w_delta, own.at[pl.ds(0, upper)]),
            load(w_latent, own.at[pl.ds(upper, w_latent.shape[0])])]

    barrier = pltpu.get_barrier_semaphore()
    peers = [{"sp": lax.rem(z + k, Z)} for k in range(1, Z)]
    peers += [{"fs": 1 - x}, {"grp": 1 - y}, {"fs": 1 - x, "grp": 1 - y}, {"tp": 1 - c}]
    for dev in peers:
        pl.semaphore_signal(barrier, inc=1, device_id=dev, device_id_type=MESH)
    pl.semaphore_wait(barrier, len(peers))

    for index in first:
        loads[index]().wait()
    W, N, L, H = Puts(wsend), Puts(nsend), Puts(lsend), Puts(hsend)
    mine = pl.ds(pl.multiple_of(y * part, part), part)
    yours = pl.ds(pl.multiple_of((1 - y) * part, part), part)
    for k in range(1, Z):
        to = lax.rem(z + k, Z)
        W.put(True, wown.at[to, mine], wbuf.at[me, mine], wrecv.at[me, y], {"sp": to})
    W.put(True, wown.at[z], wbuf.at[me], wrecv.at[me, 0], {"fs": 1 - x})
    keep_own = pltpu.make_async_copy(wown.at[z], wbuf.at[me], osem.at[0])
    keep_own.start()
    loads[tok_at]().wait()
    for b in range(seqs):
        t = tok[b * BLOCK : (b + 1) * BLOCK].astype(F32)
        scale = lax.rsqrt(jnp.mean(t * t, axis=-1, keepdims=True) + NORM_EPS)
        nbuf[b, z] = (t * scale * pre_gain[...]).astype(BF16)
    for sign in (1, -1):
        nxt = z + sign
        N.put(jnp.logical_and(nxt >= 0, nxt < Z), nbuf.at[c, z], nbuf.at[c, z],
              nrecv.at[c, z], {"sp": nxt})

    for index in rest:
        loads[index]().wait()
    lane = lax.broadcasted_iota(jnp.int32, (length, tile), 1)
    row = lax.broadcasted_iota(jnp.int32, (length, tile), 0)
    half_turn = ROPE // 2
    step = (lane % half_turn).astype(F32)
    angle = row.astype(F32) * jnp.exp(step * (-2.0 * math.log(ROPE_THETA) / ROPE))
    turning = (lane >= NOPE) & (lane < NOPE + ROPE)
    turn_a[...] = jnp.where(lane < NOPE, 1.0, jnp.where(turning, jnp.cos(angle), 0.0))
    sin_t = jnp.sin(angle)
    turn_b[...] = jnp.where(turning, jnp.where(lane < NOPE + half_turn, -sin_t, sin_t), 0.0)

    def pick(cond):
        return jnp.where(cond, 1.0, 0.0).astype(BF16)

    head = c * w_query.shape[1] // HEAD + z
    nb = w_beta.shape[1]
    r8 = lax.broadcasted_iota(jnp.int32, (nb, 2 * tile), 0)
    l8 = lax.broadcasted_iota(jnp.int32, (nb, 2 * tile), 1)
    r32 = lax.broadcasted_iota(jnp.int32, (ROPE, 2 * tile), 0)
    l32 = lax.broadcasted_iota(jnp.int32, (ROPE, 2 * tile), 1)
    turned_lane = jnp.where(l32 < tile, r32 + NOPE, (r32 + half_turn) % ROPE + NOPE + tile)
    ssel[...] = (
        dot(beta_v[...], pick((r8 == head) & (l8 == 0)))
        + dot(decay_v[...], pick((r8 == head) & (l8 == 1)))
        + dot(rope_v[...], pick(l32 == turned_lane))
    ).astype(BF16)
    per = NOPE + ROPE
    lh = w_qup.shape[1] // per // Z
    qd = lax.broadcasted_iota(jnp.int32, (w_qup.shape[1], tile), 1)
    qs = lax.broadcasted_iota(jnp.int32, (w_qup.shape[1], tile), 0)
    swapped = jnp.where(qd < NOPE, qd, NOPE + (qd - NOPE + half_turn) % ROPE)
    for j in range(lh):
        base = (z * lh + j) * per
        qsel[:, j * tile : (j + 1) * tile] = dot(
            qup_v[...], pick((qd < per) & (qs == base + qd))
        ).astype(BF16)
        qsel[:, (lh + j) * tile : (lh + j + 1) * tile] = dot(
            qup_v[...], pick((qd >= NOPE) & (qd < per) & (qs == base + swapped))
        ).astype(BF16)

    for index in outs:
        loads[index]().wait()
    g = Gather(
        place,
        lambda p: own.at[pl.ds(cuts[p], cuts[p + 1] - cuts[p])],
        lambda p, s: buf.at[s, pl.ds(cuts[p], cuts[p + 1] - cuts[p])],
        send, recv, lsem,
    )

    def wait_w(zz, xx, yy, rows):
        slot = zz * X + xx
        landed(True, wbuf.at[slot, rows], dummy.at[0], wrecv.at[slot, yy], c)

    for k in range(1, Z):
        zz = lax.rem(z - k + Z, Z)
        slot = zz * X + x
        wait_w(zz, x, y, mine)
        for dev in ({"fs": 1 - x}, {"grp": 1 - y}, {"fs": 1 - x, "grp": 1 - y}):
            ref = wbuf.at[slot, mine]
            W.put(True, ref, ref, wrecv.at[slot, y], dev)
        for sign in (1, -1):
            zz = z - sign * k
            ok = jnp.logical_and(zz >= 0, zz < Z)
            nxt = z + sign
            ref = nbuf.at[c, zz]
            landed(ok, ref, dummy.at[1], nrecv.at[c, zz], c)
            N.put(both(ok, jnp.logical_and(nxt >= 0, nxt < Z)), ref, ref, nrecv.at[c, zz],
                  {"sp": nxt})
            N.put(ok, ref, ref, nrecv.at[c, zz], {"tp": 1 - c})
        if k == max(1, Z - 2):
            g.start_along()
    g.start_across()
    for k in range(1, Z):
        zz = lax.rem(z - k + Z, Z)
        wait_w(zz, x, 1 - y, yours)
        wait_w(zz, 1 - x, y, mine)
        wait_w(zz, 1 - x, 1 - y, yours)
    slot = z * X + 1 - x
    landed(True, wbuf.at[slot], dummy.at[0], wrecv.at[slot, 0], c)
    keep_own.wait()
    for k in range(1, Z):
        zz = lax.rem(z - k + Z, Z)
        landed(True, nbuf.at[1 - c, zz], dummy.at[1], nrecv.at[1 - c, zz], c)

    lslot = (1 - c) * z + c * (Z + kblock)
    for b in range(seqs):
        at = slice(b * length, (b + 1) * length)
        normed = nbuf[b].reshape(length, width)
        pr = dot(normed, wbuf[...].reshape(width, ncol)).astype(BF16)
        lat[lslot, at] = pr[:, 3 * tile :]
        raw[at] = pr[:, : 3 * tile]
        sm[at] = dot(normed, ssel[...])

    def latput(cond, slot, dev):
        L.put(cond, lat.at[slot], lat.at[slot], lrecv.at[slot], dev)

    for k in range(1, Z):
        latput(c == 0, z, {"sp": lax.rem(z + k, Z)})
    pair = z - kblock
    for k in range(1, nk):
        latput(c == 1, Z + kblock, {"sp": pair + lax.rem(kblock + k, nk)})
    latput(True, lslot, {"tp": 1 - c})
    g.step(1)

    ri = lax.broadcasted_iota(jnp.int32, (BLOCK, BLOCK), 0)
    ci = lax.broadcasted_iota(jnp.int32, (BLOCK, BLOCK), 1)
    strict = ri > ci
    causal = ri >= ci
    eye = jnp.where(ri == ci, 1.0, 0.0).astype(F32)
    tri = jnp.where(causal, 1.0, 0.0).astype(F32)
    units = [(b, n) for b in range(seqs) for n in range(Z)]
    lane1 = lax.broadcasted_iota(jnp.int32, (1, nb), 1)
    rate = jnp.sum(jnp.where(lane1 == head, rate_in[...], 0.0), axis=-1, keepdims=True)
    pre_b = sm[:, 0:1]
    pre_d = sm[:, 1:2]
    beta_all = jax.nn.sigmoid(pre_b)
    log_a = -rate * (jnp.maximum(pre_d, 0.0) + jnp.log1p(jnp.exp(-jnp.abs(pre_d))))
    blane = lax.broadcasted_iota(jnp.int32, (BLOCK, tile), 1)
    spread_a = jnp.zeros((BLOCK, tile), F32)
    for u in range(len(units)):
        spread_a = jnp.where(blane == u, log_a[u * BLOCK : (u + 1) * BLOCK], spread_a)
    gates = dot(tri, spread_a, HIGHEST)
    gates_t = gates.T
    terms = []
    for u in range(len(units)):
        at = slice(u * BLOCK, (u + 1) * BLOCK)

        def act(i):
            v = raw[at, i * tile : (i + 1) * tile].astype(F32)
            return v * jax.nn.sigmoid(v)

        def unit(v):
            return v * lax.rsqrt(jnp.sum(v * v, axis=-1, keepdims=True) + NORM_EPS)

        q = unit(act(0)) * HEAD ** (-0.5)
        k = unit(act(1))
        v = act(2)
        beta = beta_all[at]
        gcol = gates[:, u : u + 1]
        grow = gates_t[u : u + 1, :]
        glast = gates[BLOCK - 1 : BLOCK, u : u + 1]
        gap = gcol - grow
        decay = jnp.where(causal, jnp.exp(jnp.where(causal, gap, 0.0)), 0.0)
        ks = k * beta
        low = jnp.where(strict, dot_t(ks, k, HIGHEST) * decay, 0.0)
        scores = dot_t(q.astype(BF16), k.astype(BF16)) * decay
        eg = jnp.exp(gcol)
        terms.append([low, scores, v * beta, ks * eg, q * eg, k * jnp.exp(glast - gcol),
                      jnp.exp(glast)])
    every = range(len(units))
    inv = [eye - jnp.where((ri // 2 == ci // 2), terms[i][0], 0.0) for i in every]
    size = 2
    while size < BLOCK:
        joint = (ri // (2 * size) == ci // (2 * size)) & (ri // size != ci // size)
        mids = [dot(jnp.where(joint, terms[i][0], 0.0), inv[i], HIGHEST) for i in every]
        inv = [inv[i] - dot(inv[i], mids[i], HIGHEST) for i in every]
        size *= 2
    inv = [m.astype(BF16) for m in inv]
    nv = [dot(inv[i], terms[i][2].astype(BF16)) for i in every]
    kw = [dot(inv[i], terms[i][3].astype(BF16)).astype(BF16) for i in every]
    g.cross_step(0)
    if Z > 2:
        g.step(2)
    state = [None] * seqs
    for n in range(Z):
        for b in range(seqs):
            i = b * Z + n
            _, scores, _, _, qd_, kd_, factor = terms[i]
            corrected = nv[i]
            if n:
                s_in = state[b].astype(BF16)
                corrected = corrected - dot(kw[i], s_in)
            o = dot(scores.astype(BF16), corrected.astype(BF16))
            if n:
                o = o + dot(qd_.astype(BF16), s_in)
            grown = t_dot(kd_.astype(BF16), corrected.astype(BF16))
            state[b] = state[b] * factor + grown if n else grown
            o = o * lax.rsqrt(jnp.mean(o * o, axis=-1, keepdims=True) + NORM_EPS) * gain[...]
            hsrc[0, n, b * BLOCK : (b + 1) * BLOCK] = o.astype(BF16)

    def give(kind):
        hbuf[kind, z] = hsrc[kind, z]
        for k in range(1, Z):
            to = lax.rem(z + k, Z)
            H.put(True, hsrc.at[kind, to], hbuf.at[kind, z], hrecv.at[kind, z], {"sp": to})

    give(0)
    for k in range(1, Z):
        zz = lax.rem(z - k + Z, Z)
        landed(c == 0, lat.at[zz], dummy.at[2], lrecv.at[zz], c)
        latput(c == 0, zz, {"tp": 1 - c})
    for k in range(1, nk):
        slot = Z + lax.rem(kblock + k, nk)
        landed(c == 1, lat.at[slot], dummy.at[2], lrecv.at[slot], c)
        latput(c == 1, slot, {"tp": 1 - c})
    g.cross_step(1)
    for k in range(3, Z):
        g.step(k)
        if k < Z - 1:
            g.cross_step(k - 1)
    for s in range(Z):
        landed(c == 1, lat.at[s], dummy.at[2], lrecv.at[s], c)
    for s in range(Z, Z + nk):
        landed(c == 0, lat.at[s], dummy.at[2], lrecv.at[s], c)

    scale = per ** (-0.5)
    la = lax.broadcasted_iota(jnp.int32, (length, length), 1) // BLOCK
    lb = lax.broadcasted_iota(jnp.int32, (length, length), 0) // BLOCK
    allowed = la <= lb
    lcol = pl.ds(pl.multiple_of(z * lh * tile, lh * tile), lh * tile)

    def normed_parts(slots, at, g_):
        parts = [lat[s, at].astype(F32) for s in slots]
        squares = sum(jnp.sum(p * p, axis=-1, keepdims=True) for p in parts)
        factor = lax.rsqrt(squares / (len(parts) * tile) + NORM_EPS)
        return jnp.concatenate(
            [(p * factor * g_[:, i * tile : (i + 1) * tile]).astype(BF16)
             for i, p in enumerate(parts)], axis=1
        )

    for b in range(seqs):
        at = slice(b * length, (b + 1) * length)
        ta, tb = turn_a[...], turn_b[...]
        qn = normed_parts(range(Z), at, qgain)
        kn = normed_parts(range(Z, Z + nk), at, kgain)
        qa = dot(qn, qsel[...]).astype(BF16).astype(F32)
        ka = dot(kn, lup_v[:, lcol]).astype(BF16)
        rope = sm[at].astype(BF16).astype(F32)
        turned = (rope[:, :tile] * ta + rope[:, tile:] * tb).astype(BF16)
        outs_ = []
        for j in range(lh):
            qf = (qa[:, j * tile : (j + 1) * tile] * ta
                  + qa[:, (lh + j) * tile : (lh + j + 1) * tile] * tb).astype(BF16)
            kj = ka[:, j * tile : (j + 1) * tile]
            kf = jnp.where(lane < NOPE, kj, turned)
            s = jnp.where(allowed, dot_t(qf, kf) * scale, -jnp.inf)
            w = jnp.exp(s - jnp.max(s, axis=-1, keepdims=True))
            o = dot(w.astype(BF16), kj) / jnp.sum(w, axis=-1, keepdims=True)
            outs_.append(o)
        both_ = jnp.where(lane < VDIM, pltpu.roll(outs_[0], VDIM, 1), outs_[1]).astype(BF16)
        for n in range(Z):
            hsrc[1, n, b * BLOCK : (b + 1) * BLOCK] = both_[n * BLOCK : (n + 1) * BLOCK]
    give(1)
    if Z > 3:
        g.cross_step(Z - 2)
    g.finish()
    for kind in range(2):
        for k in range(1, Z):
            zz = lax.rem(z - k + Z, Z)
            landed(True, hbuf.at[kind, zz], dummy.at[2], hrecv.at[kind, zz], c)
    hv = jnp.concatenate([hbuf[kind, s] for kind in range(2) for s in range(Z)], axis=1)
    n = buf.shape[0]
    half = n // 2
    rows = hv.shape[0]

    def piece(s, carry):
        pbuf[s] = dot(hv, buf[s]).astype(BF16)
        return carry

    lax.fori_loop(0, n, piece, 0)
    peer = 1 - c
    copy = pltpu.make_async_remote_copy(
        src_ref=pbuf.at[pl.ds(peer * half, half)], dst_ref=rbuf, send_sem=tsem.at[0],
        recv_sem=tsem.at[1], device_id={"tp": peer}, device_id_type=MESH,
    )
    copy.start()
    for p in (W, N, L, H, g):
        p.drain()
    copy.wait()
    total = jnp.zeros((rows, 1), F32)
    mixed = []
    for s in range(half):
        m = pbuf[c * half + s].astype(F32) + rbuf[s].astype(F32)
        mixed.append(m)
        total = total + jnp.sum(m * m, axis=-1, keepdims=True)
    sq[0] = jnp.broadcast_to(total, sq.shape[1:])
    squares = pltpu.make_async_remote_copy(
        src_ref=sq.at[0], dst_ref=sq.at[1], send_sem=tsem.at[2], recv_sem=tsem.at[3],
        device_id={"tp": peer}, device_id_type=MESH,
    )
    squares.start()
    squares.wait()
    total = total + sq[1][:, :1]
    cb = buf.shape[2]
    norm = lax.rsqrt(total / (n * cb) + NORM_EPS)
    for s in range(half):
        out[:, s * cb : (s + 1) * cb] = (mixed[s] * norm * post[s]).astype(BF16)


def splits_by_heads(sizes, seqs, count, qw, qd, kd, qup, lup):
    Y, Z, X, C = sizes
    nk = kd[1] // 128
    return (
        Y == 2 and X == 2 and C == 2 and seqs == C and count == BLOCK and qw[1] == Z * HEAD
        and qd[1] == Z * 128 and kd[1] == nk * 128 and Z % nk == 0
        and qup[1] == Z * 2 * (NOPE + ROPE) and lup[1] == Z * 2 * (NOPE + VDIM)
    )


def by_heads(sizes, *arrays):
    (tokens, pre_gain, query_weight, key_weight, value_weight, beta_weight, decay_weight,
     decay_rate, delta_gain, query_down, latent_down, rope_weight, query_gain, latent_gain,
     query_up, latent_up, delta_out, latent_out, post_gain) = arrays
    Y, Z, X, C = sizes
    n = Z * X
    seqs, count, width = tokens.shape
    rows = seqs * count
    shard = query_weight.shape[0]
    nk = latent_down.shape[1] // 128
    cb = delta_out.shape[1]
    depth = delta_out.shape[0] + latent_out.shape[0]
    cuts = (0, depth * 7 // 16, depth * 14 // 16, depth)
    half = n // 2
    lh = query_up.shape[1] // (NOPE + ROPE) // Z
    total = rows * Z
    ncol = 4 * 128
    args = (
        tokens.reshape(rows, width), pre_gain.reshape(1, width),
        beta_weight, decay_weight, rope_weight,
        query_weight, key_weight, value_weight, query_down, latent_down, delta_out, latent_out,
        query_gain.reshape(1, -1), latent_gain.reshape(1, -1), query_up, latent_up,
        decay_rate.reshape(1, -1), delta_gain.reshape(1, HEAD), post_gain.reshape(half, 1, cb),
    )
    hbm = (0, 2, 3, 4, 5, 6, 7, 8, 9, 10, 11, 14, 15)
    DMA = pltpu.SemaphoreType.DMA
    result = pl.pallas_call(
        functools.partial(heads_kernel, sizes, seqs, cuts),
        name="layer",
        out_shape=jax.ShapeDtypeStruct((rows, half * cb), BF16),
        in_specs=[anywhere() if i in hbm else vmem() for i in range(len(args))],
        out_specs=vmem(),
        scratch_shapes=[
            pltpu.VMEM((rows, width), BF16),
            pltpu.VMEM(beta_weight.shape, BF16),
            pltpu.VMEM(decay_weight.shape, BF16),
            pltpu.VMEM(rope_weight.shape, BF16),
            pltpu.VMEM(query_up.shape, BF16),
            pltpu.VMEM(latent_up.shape, BF16),
            pltpu.VMEM((Z, shard, ncol), BF16),
            pltpu.VMEM((n, shard, ncol), BF16),
            pltpu.VMEM((seqs, Z, BLOCK, width), BF16),
            pltpu.VMEM((width, 256), BF16),
            pltpu.VMEM((query_up.shape[0], 2 * lh * 128), BF16),
            pltpu.VMEM((Z * BLOCK, 128), F32),
            pltpu.VMEM((Z * BLOCK, 128), F32),
            pltpu.VMEM((total, 384), BF16),
            pltpu.VMEM((total, 256), F32),
            pltpu.VMEM((Z + nk, total, 128), BF16),
            pltpu.VMEM((2, Z, rows, 128), BF16),
            pltpu.VMEM((2, Z, rows, 128), BF16),
            pltpu.VMEM((depth, cb), BF16),
            pltpu.VMEM((n, depth, cb), BF16),
            pltpu.VMEM((n, rows, cb), BF16),
            pltpu.VMEM((half, rows, cb), BF16),
            pltpu.VMEM((2, rows, 128), F32),
            DMA((4 * Z + 8,)),
            DMA((4 * Z,)),
            DMA((n, 2)),
            DMA((2 + 4 * Z,)),
            DMA((seqs, Z)),
            DMA((2 * Z + 2 * nk,)),
            DMA((Z + nk,)),
            DMA((2 * Z,)),
            DMA((2, Z)),
            DMA((1,)),
            DMA((3,)),
        ]
        + Gather.scratch(Z, X) + [DMA((6,))],
        compiler_params=pltpu.CompilerParams(
            collective_id=0, has_side_effects=True, vmem_limit_bytes=60 * 1024 * 1024
        ),
    )(*args)
    return result.reshape(seqs, count, half * cb)


def solution(mesh):
    sizes = tuple(mesh.shape[a] for a in ("grp", "sp", "fs", "tp"))
    return jax.shard_map(
        functools.partial(local, sizes),
        mesh=mesh,
        in_specs=(
            P(("grp", "fs"), "sp", None),
            P(),
            P(("sp", "fs"), "tp"),
            P(("sp", "fs"), "tp"),
            P(("sp", "fs"), "tp"),
            P(),
            P(),
            P(),
            P(),
            P(("sp", "fs"), None),
            P(("sp", "fs"), None),
            P(),
            P(),
            P(),
            P(None, "tp"),
            P(None, "tp"),
            P("tp", ("sp", "fs")),
            P("tp", ("sp", "fs")),
            P("tp"),
        ),
        out_specs=P(("grp", "fs"), "sp", "tp"),
        check_vma=False,
    )
```

```python
import functools
import math

import jax
import jax.numpy as jnp
from jax import lax
from jax.experimental import pallas as pl
from jax.experimental.pallas import tpu as pltpu
from jax.sharding import PartitionSpec as P

HEAD = 128
NOPE = 64
ROPE = 32
VDIM = 64
BLOCK = 64
NORM_EPS = 1e-06
ROPE_THETA = 10000.0
HIGHEST = lax.Precision.HIGHEST
MESH = pl.DeviceIdType.MESH
F32 = jnp.float32
BF16 = jnp.bfloat16


def dot(a, b, precision=None):
    return jnp.dot(a, b, preferred_element_type=F32, precision=precision)


def dot_t(a, b, precision=None):
    return lax.dot_general(
        a, b, (((1,), (1,)), ((), ())), preferred_element_type=F32, precision=precision
    )


def t_dot(a, b, precision=None):
    return lax.dot_general(
        a, b, (((0,), (0,)), ((), ())), preferred_element_type=F32, precision=precision
    )


def when(cond, fn):
    if cond is True:
        fn()
    elif cond is not False:
        pl.when(cond)(fn)


def both(a, b):
    if a is True:
        return b
    if b is True:
        return a
    return jnp.logical_and(a, b)


class Place:
    def __init__(self, sizes):
        self.Y, self.Z, self.X, self.C = sizes
        self.y = lax.axis_index("grp")
        self.z = lax.axis_index("sp")
        self.x = lax.axis_index("fs")
        self.c = lax.axis_index("tp")


def greet(place, plane=True, later=False):
    barrier = pltpu.get_barrier_semaphore()

    def signal(cond, dev):
        when(
            cond,
            lambda: pl.semaphore_signal(barrier, inc=1, device_id=dev, device_id_type=MESH),
        )

    count = jnp.int32(0)
    if later:
        for k in range(1, place.Z):
            signal(place.z + k < place.Z, {"sp": place.z + k})
            signal(place.z - k >= 0, {"sp": place.z - k})
        count += place.Z - 1
    else:
        signal(place.z + 1 < place.Z, {"sp": place.z + 1})
        signal(place.z > 0, {"sp": place.z - 1})
        count += (place.z + 1 < place.Z).astype(jnp.int32) + (place.z > 0).astype(jnp.int32)
    if plane:
        for d in range(1, place.X):
            signal(True, {"fs": lax.rem(place.x + d, place.X)})
        count += place.X - 1
        if place.Y == 2:
            signal(True, {"grp": 1 - place.y})
            count += 1
    signal(True, {"tp": 1 - place.c})
    count += 1
    pl.semaphore_wait(barrier, count)


class Gather:
    def __init__(self, place, own, buf, send, recv, lsem):
        self.pl, self.own, self.buf = place, own, buf
        self.send, self.recv, self.lsem = send, recv, lsem
        self.sends = []
        self.ev = 0

    def active(self, p):
        return True if p == 2 else self.pl.y == p

    def push(self, cond, src, p, slot, dev, ev, way):
        index = len(self.sends)

        def make():
            return pltpu.make_async_remote_copy(
                src_ref=src,
                dst_ref=self.buf(p, slot),
                send_sem=self.send.at[index],
                recv_sem=self.recv.at[slot, p],
                device_id=dev,
                device_id_type=MESH,
            )

        when(cond, lambda: make().start())
        self.sends.append((cond, make))

    def arrived(self, cond, p, slot):
        def wait():
            ref = self.buf(p, slot)
            pltpu.make_async_remote_copy(
                src_ref=ref,
                dst_ref=ref,
                send_sem=self.lsem.at[p],
                recv_sem=self.recv.at[slot, p],
                device_id={"tp": self.pl.c},
                device_id_type=MESH,
            ).wait_recv()

        when(cond, wait)

    def across(self, cond, src, p, slot, ev):
        q = self.pl
        for d in range(1, q.X):
            self.push(cond, src, p, slot, {"fs": lax.rem(q.x + d, q.X)}, ev, 1 + d)

    def to_y(self, cond, src, p, slot, ev):
        if p < 2:
            self.push(cond, src, p, slot, {"grp": 1 - self.pl.y}, ev, 0)

    def kinds(self):
        return (0, 1, 2)

    def start_along(self):
        q = self.pl
        me = q.z * q.X + q.x
        for p in self.kinds():
            a = self.active(p)
            src = self.own(p)
            self.push(both(a, q.z + 1 < q.Z), src, p, me, {"sp": q.z + 1}, 0, 0)
            self.push(both(a, q.z > 0), src, p, me, {"sp": q.z - 1}, 0, 1)

    def start_across(self):
        q = self.pl
        me = q.z * q.X + q.x
        for p in self.kinds():
            self.across(self.active(p), self.own(p), p, me, 0)
        for p in self.kinds():
            pltpu.make_async_copy(self.own(p), self.buf(p, me), self.lsem.at[p]).start()

    def step(self, k):
        q = self.pl
        for p in self.kinds():
            a = self.active(p)
            for sign in (1, -1):
                zz = q.z - sign * k
                ok = both(a, jnp.logical_and(zz >= 0, zz < q.Z))
                slot = zz * q.X + q.x
                nxt = q.z + sign
                ev = 2 * k - (sign == 1)
                self.arrived(ok, p, slot)
                ref = self.buf(p, slot)
                self.push(
                    both(ok, jnp.logical_and(nxt >= 0, nxt < q.Z)),
                    ref, p, slot, {"sp": nxt}, ev, 1,
                )
                self.across(ok, ref, p, slot, ev)
                self.to_y(ok, ref, p, slot, ev)

    def cross_step(self, k):
        q = self.pl
        base = 2 * q.Z
        for p in self.kinds():
            a = self.active(p)
            for sign in (1, -1) if k else (1,):
                zz = q.z - sign * k
                ok = both(a, jnp.logical_and(zz >= 0, zz < q.Z))
                for d in range(1, q.X):
                    slot = zz * q.X + lax.rem(q.x + d, q.X)
                    ev = base + (2 * k - (sign == 1) + 1) * (q.X - 1) + d - 1
                    self.arrived(ok, p, slot)
                    self.to_y(ok, self.buf(p, slot), p, slot, ev)

    def finish(self):
        q = self.pl
        self.cross_step(q.Z - 1)
        me = q.z * q.X + q.x
        for p in (0, 1):
            for s in range(q.Z * q.X):
                self.arrived(jnp.logical_and(q.y != p, me != s), p, s)
        for p in self.kinds():
            pltpu.make_async_copy(self.own(p), self.buf(p, me), self.lsem.at[p]).wait()

    def drain(self):
        for cond, make in self.sends:
            when(cond, lambda make=make: make().wait_send())

    @staticmethod
    def scratch(Z, X):
        n = Z * X
        sends = 3 * (X + 1) + 2 * (Z - 1) * (3 * X + 2) + (2 * Z - 1) * (X - 1) * 2
        return [
            pltpu.SemaphoreType.DMA((sends,)),
            pltpu.SemaphoreType.DMA((n, 3)),
            pltpu.SemaphoreType.DMA((3,)),
        ]


def spread(copies, parts, target, bounds):
    at = 0
    for ref, offset, width in parts:
        done = 0
        while done < width:
            p, col = divmod(at + done, bounds)
            size = min(width - done, bounds - col)
            start = offset + done
            if not isinstance(start, int):
                start = pl.multiple_of(start, 128)
            copies.append((ref.at[:, pl.ds(start, size)], target.at[p, :, pl.ds(col, size)]))
            done += size
        at += width


def back_kernel(
    sizes, seqs, heads, cuts, tokens, pre_gain, small, w_query, w_key, w_value, w_qdown, w_kdown,
    w_delta, w_latent, qgain, kgain, w_qup, w_lup, rate_in, gain, post,
    out, qup, lup, raw, lat, rate, own1, own, buf1, kvr, kbuf, sin, sout, hbuf, buf, pbuf, rbuf, sq,
    asem, ksem, ssem, send1, recv1, lsem1, send, recv, lsem, tsem,
):
    place = Place(sizes)
    Z, z, c = place.Z, place.z, place.c
    C = sizes[3]
    rows = tokens.shape[0]
    third = own1.shape[2]
    qcols, kcols = w_qdown.shape[1] // C, w_kdown.shape[1] // C
    pairs = []
    spread(
        pairs,
        [(w, 0, w.shape[1]) for w in (w_query, w_key, w_value)]
        + [(w_qdown, c * qcols, qcols), (w_kdown, c * kcols, kcols)],
        own1, third,
    )
    upper = w_delta.shape[0]
    pairs.append((w_delta, own.at[pl.ds(0, upper)]))
    pairs.append((w_latent, own.at[pl.ds(upper, w_latent.shape[0])]))
    loads = [pltpu.make_async_copy(a, b, asem.at[i]) for i, (a, b) in enumerate(pairs)]
    for load in loads:
        load.start()
    greet(place, later=True)
    for load in loads:
        load.wait()
    g1 = Gather(
        place, lambda p: own1.at[p], lambda p, s: buf1.at[p, s], send1, recv1, lsem1
    )
    g = Gather(
        place,
        lambda p: own.at[pl.ds(cuts[p], cuts[p + 1] - cuts[p])],
        lambda p, s: buf.at[s, pl.ds(cuts[p], cuts[p + 1] - cuts[p])],
        send, recv, lsem,
    )
    g1.start_along()
    g1.start_across()
    x = tokens[...].astype(F32)
    xscale = lax.rsqrt(jnp.mean(x * x, axis=-1, keepdims=True) + NORM_EPS)
    normed = (x * xscale * pre_gain[...]).astype(BF16)
    sm_all = dot_t(normed, small[...])
    qcol = w_qup.shape[1]
    lh = qcol // (NOPE + ROPE)
    turn_w = ROPE // 2
    kinds = ((NOPE, 0, qup, w_qup, NOPE + ROPE), (turn_w, NOPE, qup, w_qup, NOPE + ROPE),
             (turn_w, NOPE + turn_w, qup, w_qup, NOPE + ROPE),
             (NOPE, 0, lup, w_lup, NOPE + VDIM), (VDIM, NOPE, lup, w_lup, NOPE + VDIM))
    fill_at = {}
    for w, off, to, frm, per in kinds:
        size = lh * w
        dst_i = lax.broadcasted_iota(jnp.int32, (frm.shape[1], size), 1)
        src_i = lax.broadcasted_iota(jnp.int32, (frm.shape[1], size), 0)
        perm = jnp.where(src_i == dst_i // w * per + off + dst_i % w, 1.0, 0.0).astype(BF16)
        lo = fill_at.get(per, 0)
        to[:, lo : lo + size] = dot(frm[...], perm).astype(BF16)
        fill_at[per] = lo + size
    for k in range(1, Z):
        g1.step(k)
        g1.cross_step(k - 1)
        if k == max(1, Z - 2):
            g.start_along()
    g.start_across()
    if Z > 1:
        g.step(1)
    g1.finish()
    depth1 = buf1.shape[1] * buf1.shape[2]
    part2 = dot(normed, buf1[2].reshape(depth1, third)).astype(BF16)
    lat[c] = part2[:, third - qcols - kcols :]
    trade = pltpu.make_async_remote_copy(
        src_ref=lat.at[c], dst_ref=lat.at[c], send_sem=tsem.at[4], recv_sem=tsem.at[5],
        device_id={"tp": 1 - c}, device_id_type=MESH,
    )
    trade.start()
    raw[:, 2 * third : 3 * third] = part2
    for p in range(2):
        raw[:, p * third : (p + 1) * third] = dot(
            normed, buf1[p].reshape(depth1, third)
        ).astype(BF16)
    trade.wait()
    qw = qup.shape[0] // sizes[3]
    kw_lat = lup.shape[0] // sizes[3]
    tile = 128
    lane = lax.broadcasted_iota(jnp.int32, (rows, tile), 1)
    half_turn = ROPE // 2
    step = (lane % half_turn).astype(F32)
    row = lax.broadcasted_iota(jnp.int32, (rows, tile), 0)
    pos = (z * BLOCK + row % BLOCK).astype(F32)
    angle = pos * jnp.exp(step * (-2.0 * math.log(ROPE_THETA) / ROPE))
    cos, sin_t = jnp.cos(angle), jnp.sin(angle)

    def normed_parts(lo, w, g):
        parts = [lat[i, :, lo : lo + w].astype(F32) for i in range(sizes[3])]
        squares = sum(jnp.sum(p * p, axis=-1, keepdims=True) for p in parts)
        scale = lax.rsqrt(squares / (w * sizes[3]) + NORM_EPS)
        return [
            (p * scale * g[:, i * w : (i + 1) * w]).astype(BF16) for i, p in enumerate(parts)
        ]

    kparts = normed_parts(qw, kw_lat, kgain)
    krank = kw_lat * sizes[3]
    for i, p in enumerate(kparts):
        kvr[:, i * kw_lat : (i + 1) * kw_lat] = p
    allheads = heads * C
    src = lax.broadcasted_iota(jnp.int32, (tile, tile), 0)
    dst = lax.broadcasted_iota(jnp.int32, (tile, tile), 1)
    rope_raw = sm_all.astype(BF16)
    base = 2 * allheads + dst % half_turn

    def pick(cond, kind):
        return jnp.where(cond, 1.0, 0.0).astype(kind)

    rlo = dot(rope_raw, pick(src == base, BF16))
    rhi = dot(rope_raw, pick(src == base + half_turn, BF16))
    left = lane < tile // 2
    kvr[:, krank : krank + tile] = jnp.where(
        left, rlo * cos - rhi * sin_t, rhi * cos + rlo * sin_t
    ).astype(BF16)

    def kv_copy(k):
        return pltpu.make_async_remote_copy(
            src_ref=kvr,
            dst_ref=kbuf.at[z],
            send_sem=ksem.at[0, k],
            recv_sem=ksem.at[1, z],
            device_id={"sp": z + k},
            device_id_type=MESH,
        )

    for k in range(1, Z):
        when(z + k < Z, lambda k=k: kv_copy(k).start())
    ri = lax.broadcasted_iota(jnp.int32, (rows, rows), 0)
    ci = lax.broadcasted_iota(jnp.int32, (rows, rows), 1)
    tri = jnp.where((ri >= ci) & (ri // BLOCK == ci // BLOCK), 1.0, 0.0).astype(F32)
    rate[...] = jnp.zeros(rate.shape, F32)
    rate[:, allheads : 2 * allheads] = rate_in[...]
    first_head = c * heads
    own_beta = pick((dst < heads) & (src == first_head + dst), F32)
    own_rate = pick(
        (dst >= heads) & (dst < 2 * heads) & (src == allheads + first_head + dst - heads), F32
    )
    pre = dot(sm_all, own_beta + own_rate, HIGHEST)
    rates = dot(jnp.broadcast_to(rate[...], (8, tile)), own_rate, HIGHEST)[:1]
    beta_all = jax.nn.sigmoid(pre)
    log_a = -rates * (jnp.maximum(pre, 0.0) + jnp.log1p(jnp.exp(-jnp.abs(pre))))
    gates = dot(tri, log_a, HIGHEST)
    gates_t = gates.T
    r = lax.broadcasted_iota(jnp.int32, (BLOCK, BLOCK), 0)
    cc = lax.broadcasted_iota(jnp.int32, (BLOCK, BLOCK), 1)
    strict = r > cc
    causal = r >= cc
    eye = jnp.where(r == cc, 1.0, 0.0).astype(F32)
    lanes = [(b, h) for b in range(seqs) for h in range(heads)]
    width = heads * HEAD
    terms = []
    for b, h in lanes:
        t = slice(b * BLOCK, (b + 1) * BLOCK)

        def act(i):
            v = raw[t, i * width + h * HEAD : i * width + (h + 1) * HEAD].astype(F32)
            return v * jax.nn.sigmoid(v)

        def unit(u):
            return u * lax.rsqrt(jnp.sum(u * u, axis=-1, keepdims=True) + NORM_EPS)

        q = unit(act(0)) * HEAD ** (-0.5)
        k = unit(act(1))
        v = act(2)
        beta = beta_all[t, h : h + 1]
        gcol = gates[t, heads + h : heads + h + 1]
        grow = gates_t[heads + h : heads + h + 1, t]
        glast = gates[(b + 1) * BLOCK - 1 : (b + 1) * BLOCK, heads + h : heads + h + 1]
        gap = gcol - grow
        decay = jnp.where(causal, jnp.exp(jnp.where(causal, gap, 0.0)), 0.0)
        ks = k * beta
        low = jnp.where(strict, dot_t(ks, k, HIGHEST) * decay, 0.0)
        scores = dot_t(q.astype(BF16), k.astype(BF16)) * decay
        eg = jnp.exp(gcol)
        terms.append([low, scores, v * beta, ks * eg, q * eg, k * jnp.exp(glast - gcol),
                      jnp.exp(glast)])
    every = range(len(lanes))
    inv = [eye - jnp.where((r // 2 == cc // 2), terms[i][0], 0.0) for i in every]
    size = 2
    while size < BLOCK:
        joint = (r // (2 * size) == cc // (2 * size)) & (r // size != cc // size)
        mids = [dot(jnp.where(joint, terms[i][0], 0.0), inv[i], HIGHEST) for i in every]
        inv = [inv[i] - dot(inv[i], mids[i], HIGHEST) for i in every]
        size *= 2
    inv = [m.astype(BF16) for m in inv]
    nv = [dot(inv[i], terms[i][2].astype(BF16)) for i in every]
    kw = [dot(inv[i], terms[i][3].astype(BF16)) for i in every]

    def state_copy(i):
        return pltpu.make_async_remote_copy(
            src_ref=sout.at[i],
            dst_ref=sin.at[i],
            send_sem=ssem.at[0, i],
            recv_sem=ssem.at[1, i],
            device_id={"sp": z + 1},
            device_id_type=MESH,
        )

    g.cross_step(0)
    if Z > 2:
        g.step(2)
    for i, (b, h) in enumerate(lanes):
        low, scores, vb, ke, qd, kd, factor = terms[i]

        def clear(i=i):
            sin[i] = jnp.zeros((HEAD, HEAD), BF16)

        when(z == 0, clear)
        when(z > 0, lambda i=i: state_copy(i).wait_recv())
        s_in = sin[i]
        corrected = nv[i] - dot(kw[i].astype(BF16), s_in)
        sout[i] = (
            s_in.astype(F32) * factor + t_dot(kd.astype(BF16), corrected.astype(BF16))
        ).astype(BF16)
        when(z + 1 < Z, lambda i=i: state_copy(i).start())
        o = dot(qd.astype(BF16), s_in) + dot(scores.astype(BF16), corrected.astype(BF16))
        o = o * lax.rsqrt(jnp.mean(o * o, axis=-1, keepdims=True) + NORM_EPS) * gain[...]
        hbuf[b * BLOCK : (b + 1) * BLOCK, h * HEAD : (h + 1) * HEAD] = o.astype(BF16)
    g.cross_step(1)
    for k in range(3, Z):
        g.step(k)
        if k < Z - 1:
            g.cross_step(k - 1)

    for k in range(1, Z):
        def take(k=k):
            pltpu.make_async_remote_copy(
                src_ref=kvr, dst_ref=kbuf.at[z - k], send_sem=ksem.at[0, k],
                recv_sem=ksem.at[1, z - k], device_id={"sp": z}, device_id_type=MESH,
            ).wait_recv()

        when(z - k >= 0, take)
    for s in range(Z):
        def fill(s=s):
            kbuf[s] = kvr[...]

        def none(s=s):
            kbuf[s] = jnp.zeros(kbuf.shape[1:], BF16)

        when(z == s, fill)
        when(z < s, none)
    qparts = normed_parts(0, qw, qgain)
    qa = sum(dot(p, qup[i * qw : (i + 1) * qw, :]) for i, p in enumerate(qparts)).astype(BF16)
    plain_width = qa.shape[1] - 2 * tile
    qlo_raw = qa[:, plain_width : plain_width + tile].astype(F32)
    qhi_raw = qa[:, plain_width + tile :].astype(F32)
    qlo = (qlo_raw * cos - qhi_raw * sin_t).astype(BF16)
    qhi = (qhi_raw * cos + qlo_raw * sin_t).astype(BF16)
    lane1 = lax.broadcasted_iota(jnp.int32, (1, tile), 1)

    def keep(cond):
        return jnp.where(cond, 1.0, 0.0).astype(BF16)

    keys = Z * BLOCK
    allowed = lax.broadcasted_iota(jnp.int32, (2 * BLOCK, keys), 1) // BLOCK <= z
    left_half = lax.broadcasted_iota(jnp.int32, (BLOCK, tile), 1) < tile // 2
    for b in range(seqs):
        t = slice(b * BLOCK, (b + 1) * BLOCK)
        kv = jnp.concatenate([kbuf[s, t, :] for s in range(Z)], axis=0)
        up = dot(kv[:, :krank], lup[...]).astype(BF16)
        turn = kv[:, krank : krank + tile].astype(F32)
        rolled = pltpu.roll(turn, tile // 2, 1)
        sel = lax.broadcasted_iota(jnp.int32, (keys, tile), 1) < tile // 2
        klo = jnp.where(sel, turn, rolled).astype(BF16)
        khi = jnp.where(sel, rolled, turn).astype(BF16)
        for j in range(plain_width // tile):
            at = slice(j * tile, (j + 1) * tile)
            qp = qa[t, at]
            first, second = keep(lane1 < tile // 2), keep(lane1 >= tile // 2)
            m0, m1 = keep(lane1 // half_turn == 2 * j), keep(lane1 // half_turn == 2 * j + 1)
            s = (
                dot_t(jnp.concatenate([qp * first, qp * second], axis=0), up[:, at])
                + dot_t(jnp.concatenate([qlo[t] * m0, qlo[t] * m1], axis=0), klo)
                + dot_t(jnp.concatenate([qhi[t] * m0, qhi[t] * m1], axis=0), khi)
            ) * (NOPE + ROPE) ** (-0.5)
            s = jnp.where(allowed, s, -jnp.inf)
            w = jnp.exp(s - jnp.max(s, axis=-1, keepdims=True))
            o = dot(w.astype(BF16), up[:, plain_width + j * tile : plain_width + (j + 1) * tile])
            o = o / jnp.sum(w, axis=-1, keepdims=True)
            hbuf[t, width + j * tile : width + (j + 1) * tile] = jnp.where(
                left_half, o[:BLOCK], o[BLOCK:]
            ).astype(BF16)
    if Z > 3:
        g.cross_step(Z - 2)
    g.finish()
    n = buf.shape[0]
    half = n // 2
    hv = hbuf[...]

    def part(s, carry):
        pbuf[s] = dot(hv, buf[s]).astype(BF16)
        return carry

    lax.fori_loop(0, n, part, 0)
    peer = 1 - c
    copy = pltpu.make_async_remote_copy(
        src_ref=pbuf.at[pl.ds(peer * half, half)],
        dst_ref=rbuf,
        send_sem=tsem.at[0],
        recv_sem=tsem.at[1],
        device_id={"tp": peer},
        device_id_type=MESH,
    )
    copy.start()
    g1.drain()
    g.drain()
    for k in range(1, Z):
        when(z + k < Z, lambda k=k: kv_copy(k).wait_send())
    for i in every:
        when(z + 1 < Z, lambda i=i: state_copy(i).wait_send())
    copy.wait()
    total = jnp.zeros((rows, 1), F32)
    mixed = []
    for s in range(half):
        m = pbuf[c * half + s].astype(F32) + rbuf[s].astype(F32)
        mixed.append(m)
        total = total + jnp.sum(m * m, axis=-1, keepdims=True)
    sq[0] = jnp.broadcast_to(total, sq.shape[1:])
    squares = pltpu.make_async_remote_copy(
        src_ref=sq.at[0],
        dst_ref=sq.at[1],
        send_sem=tsem.at[2],
        recv_sem=tsem.at[3],
        device_id={"tp": peer},
        device_id_type=MESH,
    )
    squares.start()
    squares.wait()
    total = total + sq[1][:, :1]
    cb = buf.shape[2]
    scale = lax.rsqrt(total / (n * cb) + NORM_EPS)
    for s in range(half):
        out[:, s * cb : (s + 1) * cb] = (mixed[s] * scale * post[s]).astype(BF16)


def vmem():
    return pl.BlockSpec(memory_space=pltpu.VMEM)


def anywhere():
    return pl.BlockSpec(memory_space=pl.ANY)


def local(
    sizes,
    tokens, pre_gain, query_weight, key_weight, value_weight, beta_weight, decay_weight,
    decay_rate, delta_gain, query_down, latent_down, rope_weight, query_gain, latent_gain,
    query_up, latent_up, delta_out, latent_out, post_gain,
):
    Y, Z, X, C = sizes
    n = Z * X
    seqs, count, width = tokens.shape
    if splits_by_heads(sizes, seqs, count, query_weight.shape, query_down.shape,
                       latent_down.shape, query_up.shape, latent_up.shape, delta_out.shape,
                       latent_out.shape):
        return by_heads(
            sizes, tokens, pre_gain, query_weight, key_weight, value_weight, beta_weight,
            decay_weight, decay_rate, delta_gain, query_down, latent_down, rope_weight,
            query_gain, latent_gain, query_up, latent_up, delta_out, latent_out, post_gain,
        )
    rows = seqs * count
    qw = query_down.shape[1] // C
    kw = latent_down.shape[1] // C
    heads = query_weight.shape[1] // HEAD
    shard = query_weight.shape[0]
    third = (3 * query_weight.shape[1] + qw + kw) // 3
    small = [beta_weight.T, decay_weight.T, rope_weight.T]
    used = sum(w.shape[0] for w in small)
    small = jnp.concatenate(small + [jnp.zeros((128 - used, width), BF16)], axis=0)
    lanes = seqs * heads
    cb = delta_out.shape[1]
    depth = delta_out.shape[0] + latent_out.shape[0]
    cuts = (0, depth * 3 // 8, depth * 6 // 8, depth)
    half = n // 2
    kv_width = latent_down.shape[1] + 128
    args = (
        tokens.reshape(rows, width), pre_gain.reshape(1, width), small,
        query_weight, key_weight, value_weight, query_down, latent_down, delta_out, latent_out,
        query_gain.reshape(1, -1), latent_gain.reshape(1, -1), query_up, latent_up,
        decay_rate.reshape(1, -1), delta_gain.reshape(1, HEAD), post_gain.reshape(half, 1, cb),
    )
    result = pl.pallas_call(
        functools.partial(back_kernel, sizes, seqs, heads, cuts),
        name="layer",
        out_shape=jax.ShapeDtypeStruct((rows, half * cb), BF16),
        in_specs=[anywhere() if 3 <= i < 10 else vmem() for i in range(len(args))],
        out_specs=vmem(),
        scratch_shapes=[
            pltpu.VMEM(query_up.shape, BF16),
            pltpu.VMEM(latent_up.shape, BF16),
            pltpu.VMEM((rows, 3 * third), BF16),
            pltpu.VMEM((C, rows, qw + kw), BF16),
            pltpu.VMEM((1, 128), F32),
            pltpu.VMEM((3, shard, third), BF16),
            pltpu.VMEM((depth, cb), BF16),
            pltpu.VMEM((3, n, shard, third), BF16),
            pltpu.VMEM((rows, kv_width), BF16),
            pltpu.VMEM((Z, rows, kv_width), BF16),
            pltpu.VMEM((lanes, HEAD, HEAD), BF16),
            pltpu.VMEM((lanes, HEAD, HEAD), BF16),
            pltpu.VMEM((rows, depth), BF16),
            pltpu.VMEM((n, depth, cb), BF16),
            pltpu.VMEM((n, rows, cb), BF16),
            pltpu.VMEM((half, rows, cb), BF16),
            pltpu.VMEM((2, rows, 128), F32),
            pltpu.SemaphoreType.DMA((16,)),
            pltpu.SemaphoreType.DMA((2, Z)),
            pltpu.SemaphoreType.DMA((2, lanes)),
        ]
        + Gather.scratch(Z, X) + Gather.scratch(Z, X) + [pltpu.SemaphoreType.DMA((6,))],
        compiler_params=pltpu.CompilerParams(
            collective_id=0, has_side_effects=True, vmem_limit_bytes=60 * 1024 * 1024
        ),
    )(*args)
    return result.reshape(seqs, count, half * cb)


class Puts:
    def __init__(self, sems):
        self.sems, self.sent = sems, []

    def put(self, cond, src, dst, recv, dev):
        index = len(self.sent)

        def make():
            return pltpu.make_async_remote_copy(
                src_ref=src, dst_ref=dst, send_sem=self.sems.at[index], recv_sem=recv,
                device_id=dev, device_id_type=MESH,
            )

        when(cond, lambda: make().start())
        self.sent.append((cond, make))

    def drain(self):
        for cond, make in self.sent:
            when(cond, lambda make=make: make().wait_send())


def landed(cond, ref, dummy, recv, c):
    def wait():
        pltpu.make_async_remote_copy(
            src_ref=ref, dst_ref=ref, send_sem=dummy, recv_sem=recv,
            device_id={"tp": c}, device_id_type=MESH,
        ).wait_recv()

    when(cond, wait)


def heads_kernel(
    sizes, seqs, tokens, pre_gain, w_beta, w_decay, w_rope, w_query, w_key, w_value,
    w_qdown, w_kdown, w_delta, w_latent, qgain, kgain, w_qup, w_lup, rate_in, gain, post,
    out, tok, beta_v, decay_v, rope_v, qup_v, lup_v, wown, wbuf, nbuf, ssel, qsel, turn_a, turn_b,
    raw, sm, lat, hsrc, hbuf, obuf, pbuf, rbuf, sq,
    asem, wsend, wrecv, nsend, nrecv, lsend, lrecv, hsend, hrecv, osend, orecv, psend, precv,
    ksem, dummy, tsem,
):
    place = Place(sizes)
    Z, X = place.Z, place.X
    y, z, x, c = place.y, place.z, place.x, place.c
    tile = 128
    shard = wown.shape[1]
    part = shard // 2
    me = z * X + x
    nk = w_kdown.shape[1] // tile
    kblock = lax.rem(z, nk)
    length = Z * BLOCK
    count = seqs * length
    width = nbuf.shape[3]
    ncol = wown.shape[2]
    barrier = pltpu.get_barrier_semaphore()
    peers = [{"sp": lax.rem(z + k, Z)} for k in range(1, Z)]
    peers += [{"fs": 1 - x}, {"grp": 1 - y}, {"fs": 1 - x, "grp": 1 - y}, {"tp": 1 - c},
              {"fs": 1 - x, "tp": 1 - c}]
    for dev in peers:
        pl.semaphore_signal(barrier, inc=1, device_id=dev, device_id_type=MESH)
    loads = []

    def load(src, dst, cond=True):
        index = len(loads)

        def make():
            return pltpu.make_async_copy(src, dst, asem.at[index])

        when(cond, lambda: make().start())
        loads.append(make)
        return index

    first = []
    for d in range(Z):
        for i, w in enumerate((w_query, w_key, w_value)):
            at = wown.at[d, :, pl.ds(i * tile, tile)]
            first.append(load(w.at[:, pl.ds(d * tile, tile)], at))
        at = wown.at[d, :, pl.ds(3 * tile, tile)]
        index = load(w_qdown.at[:, pl.ds(d * tile, tile)], at, c == 0)
        first.append(index)
        kd = d % nk

        def other(kd=kd, at=at, index=index):
            pltpu.make_async_copy(
                w_kdown.at[:, pl.ds(kd * tile, tile)], at, asem.at[index]
            ).start()

        when(c == 1, other)
    tok_at = load(tokens, tok)
    rest = [load(a, b) for a, b in (
        (w_beta, beta_v), (w_decay, decay_v), (w_rope, rope_v), (w_qup, qup_v), (w_lup, lup_v),
    )]
    upper = w_delta.shape[0]
    outs = [load(w_delta, obuf.at[z, pl.ds(0, upper)]),
            load(w_latent, obuf.at[z, pl.ds(upper, w_latent.shape[0])])]

    pl.semaphore_wait(barrier, len(peers))

    for index in first:
        loads[index]().wait()
    W, N, L, H = Puts(wsend), Puts(nsend), Puts(lsend), Puts(hsend)
    O, R = Puts(osend), Puts(psend)
    mine = pl.ds(pl.multiple_of(y * part, part), part)
    yours = pl.ds(pl.multiple_of((1 - y) * part, part), part)
    for k in range(1, Z):
        to = lax.rem(z + k, Z)
        W.put(True, wown.at[to, mine], wbuf.at[me, mine], wrecv.at[me, y], {"sp": to})
    W.put(True, wown.at[z], wbuf.at[me], wrecv.at[me, 0], {"fs": 1 - x})
    keep_own = pltpu.make_async_copy(wown.at[z], wbuf.at[me], ksem.at[0])
    keep_own.start()
    loads[tok_at]().wait()
    for b in range(seqs):
        t = tok[b * BLOCK : (b + 1) * BLOCK].astype(F32)
        scale = lax.rsqrt(jnp.mean(t * t, axis=-1, keepdims=True) + NORM_EPS)
        nbuf[b, z] = (t * scale * pre_gain[...]).astype(BF16)
    for sign in (1, -1):
        nxt = z + sign
        N.put(jnp.logical_and(nxt >= 0, nxt < Z), nbuf.at[c, z], nbuf.at[c, z],
              nrecv.at[c, z], {"sp": nxt})

    for index in rest:
        loads[index]().wait()
    lane = lax.broadcasted_iota(jnp.int32, (length, tile), 1)
    row = lax.broadcasted_iota(jnp.int32, (length, tile), 0)
    half_turn = ROPE // 2
    step = (lane % half_turn).astype(F32)
    angle = row.astype(F32) * jnp.exp(step * (-2.0 * math.log(ROPE_THETA) / ROPE))
    turning = (lane >= NOPE) & (lane < NOPE + ROPE)
    turn_a[...] = jnp.where(lane < NOPE, 1.0, jnp.where(turning, jnp.cos(angle), 0.0))
    sin_t = jnp.sin(angle)
    turn_b[...] = jnp.where(turning, jnp.where(lane < NOPE + half_turn, -sin_t, sin_t), 0.0)

    def pick(cond):
        return jnp.where(cond, 1.0, 0.0).astype(BF16)

    head = c * w_query.shape[1] // HEAD + z
    nb = w_beta.shape[0]
    r8 = lax.broadcasted_iota(jnp.int32, (2 * tile, nb), 1)
    l8 = lax.broadcasted_iota(jnp.int32, (2 * tile, nb), 0)
    r32 = lax.broadcasted_iota(jnp.int32, (2 * tile, ROPE), 1)
    l32 = lax.broadcasted_iota(jnp.int32, (2 * tile, ROPE), 0)
    turned_lane = jnp.where(l32 < tile, r32 + NOPE, (r32 + half_turn) % ROPE + NOPE + tile)
    ssel[...] = (
        dot(pick((r8 == head) & (l8 == 0)), beta_v[...])
        + dot(pick((r8 == head) & (l8 == 1)), decay_v[...])
        + dot(pick(l32 == turned_lane), rope_v[...])
    ).astype(BF16)
    per = NOPE + ROPE
    lh = w_qup.shape[1] // per // Z
    qd = lax.broadcasted_iota(jnp.int32, (w_qup.shape[1], tile), 1)
    qs = lax.broadcasted_iota(jnp.int32, (w_qup.shape[1], tile), 0)
    swapped = jnp.where(qd < NOPE, qd, NOPE + (qd - NOPE + half_turn) % ROPE)
    for j in range(lh):
        base = (z * lh + j) * per
        qsel[:, j * tile : (j + 1) * tile] = dot(
            qup_v[...], pick((qd < per) & (qs == base + qd))
        ).astype(BF16)
        qsel[:, (lh + j) * tile : (lh + j + 1) * tile] = dot(
            qup_v[...], pick((qd >= NOPE) & (qd < per) & (qs == base + swapped))
        ).astype(BF16)

    for index in outs:
        loads[index]().wait()
    obl = upper
    omine = pl.ds(pl.multiple_of(y * obl, obl), obl)
    oyours = pl.ds(pl.multiple_of((1 - y) * obl, obl), obl)

    def out_send(dist):
        for sign in (1, -1):
            to = z + sign * dist
            ref = obuf.at[z, omine]
            O.put(jnp.logical_and(to >= 0, to < Z), ref, ref, orecv.at[z, y], {"sp": to})

    def out_pass(dist):
        for sign in (1, -1):
            zz = z - sign * dist
            ok = jnp.logical_and(zz >= 0, zz < Z)
            nxt = z + sign
            ref = obuf.at[zz, omine]
            landed(ok, ref, dummy.at[0], orecv.at[zz, y], c)
            if dist >= 2:
                O.put(both(ok, jnp.logical_and(nxt >= 0, nxt < Z)), ref, ref,
                      orecv.at[zz, y], {"sp": nxt})
            O.put(ok, ref, ref, orecv.at[zz, y], {"grp": 1 - y})

    def wait_w(zz, xx, yy, rows):
        slot = zz * X + xx
        landed(True, wbuf.at[slot, rows], dummy.at[0], wrecv.at[slot, yy], c)

    for k in range(1, Z):
        zz = lax.rem(z - k + Z, Z)
        slot = zz * X + x
        wait_w(zz, x, y, mine)
        for dev in ({"fs": 1 - x}, {"grp": 1 - y}, {"fs": 1 - x, "grp": 1 - y}):
            ref = wbuf.at[slot, mine]
            W.put(True, ref, ref, wrecv.at[slot, y], dev)
        for sign in (1, -1):
            zz = z - sign * k
            ok = jnp.logical_and(zz >= 0, zz < Z)
            nxt = z + sign
            ref = nbuf.at[c, zz]
            landed(ok, ref, dummy.at[1], nrecv.at[c, zz], c)
            N.put(both(ok, jnp.logical_and(nxt >= 0, nxt < Z)), ref, ref, nrecv.at[c, zz],
                  {"sp": nxt})
            N.put(ok, ref, ref, nrecv.at[c, zz], {"tp": 1 - c})
        if k == max(1, Z - 2):
            out_send(1)
    for k in range(1, Z):
        zz = lax.rem(z - k + Z, Z)
        wait_w(zz, x, 1 - y, yours)
        wait_w(zz, 1 - x, y, mine)
        wait_w(zz, 1 - x, 1 - y, yours)
    slot = z * X + 1 - x
    landed(True, wbuf.at[slot], dummy.at[0], wrecv.at[slot, 0], c)
    keep_own.wait()
    for k in range(1, Z):
        zz = lax.rem(z - k + Z, Z)
        landed(True, nbuf.at[1 - c, zz], dummy.at[1], nrecv.at[1 - c, zz], c)

    lslot = (1 - c) * z + c * (Z + kblock)
    for b in range(seqs):
        at = slice(b * length, (b + 1) * length)
        normed = nbuf[b].reshape(length, width)
        pr = dot(normed, wbuf[...].reshape(width, ncol)).astype(BF16)
        lat[lslot, at] = pr[:, 3 * tile :]
        raw[at] = pr[:, : 3 * tile]
        sm[at] = dot_t(normed, ssel[...])

    def latput(cond, slot, dev):
        L.put(cond, lat.at[slot], lat.at[slot], lrecv.at[slot], dev)

    for k in range(1, Z):
        latput(c == 0, z, {"sp": lax.rem(z + k, Z)})
    pair = z - kblock
    for k in range(1, nk):
        latput(c == 1, Z + kblock, {"sp": pair + lax.rem(kblock + k, nk)})
    latput(True, lslot, {"tp": 1 - c})
    out_send(2)

    ri = lax.broadcasted_iota(jnp.int32, (BLOCK, BLOCK), 0)
    ci = lax.broadcasted_iota(jnp.int32, (BLOCK, BLOCK), 1)
    strict = ri > ci
    causal = ri >= ci
    eye = jnp.where(ri == ci, 1.0, 0.0).astype(F32)
    tri = jnp.where(causal, 1.0, 0.0).astype(F32)
    units = [(b, n) for b in range(seqs) for n in range(Z)]
    lane1 = lax.broadcasted_iota(jnp.int32, (1, nb), 1)
    rate = jnp.sum(jnp.where(lane1 == head, rate_in[...], 0.0), axis=-1, keepdims=True)
    pre_b = sm[:, 0:1]
    pre_d = sm[:, 1:2]
    beta_all = jax.nn.sigmoid(pre_b)
    log_a = -rate * (jnp.maximum(pre_d, 0.0) + jnp.log1p(jnp.exp(-jnp.abs(pre_d))))
    blane = lax.broadcasted_iota(jnp.int32, (BLOCK, tile), 1)
    spread_a = jnp.zeros((BLOCK, tile), F32)
    for u in range(len(units)):
        spread_a = jnp.where(blane == u, log_a[u * BLOCK : (u + 1) * BLOCK], spread_a)
    gates = dot(tri, spread_a, HIGHEST)
    gates_t = gates.T
    terms = []
    for u in range(len(units)):
        at = slice(u * BLOCK, (u + 1) * BLOCK)

        def act(i):
            v = raw[at, i * tile : (i + 1) * tile].astype(F32)
            return v * jax.nn.sigmoid(v)

        def unit(v):
            return v * lax.rsqrt(jnp.sum(v * v, axis=-1, keepdims=True) + NORM_EPS)

        q = unit(act(0)) * HEAD ** (-0.5)
        k = unit(act(1))
        v = act(2)
        beta = beta_all[at]
        gcol = gates[:, u : u + 1]
        grow = gates_t[u : u + 1, :]
        glast = gates[BLOCK - 1 : BLOCK, u : u + 1]
        gap = gcol - grow
        decay = jnp.where(causal, jnp.exp(jnp.where(causal, gap, 0.0)), 0.0)
        ks = k * beta
        low = jnp.where(strict, dot_t(ks, k, HIGHEST) * decay, 0.0)
        scores = dot_t(q.astype(BF16), k.astype(BF16)) * decay
        eg = jnp.exp(gcol)
        terms.append([low, scores, v * beta, ks * eg, q * eg, k * jnp.exp(glast - gcol),
                      jnp.exp(glast)])
    every = range(len(units))
    inv = [eye - jnp.where((ri // 2 == ci // 2), terms[i][0], 0.0) for i in every]
    size = 2
    while size < BLOCK:
        joint = (ri // (2 * size) == ci // (2 * size)) & (ri // size != ci // size)
        mids = [dot(jnp.where(joint, terms[i][0], 0.0), inv[i], HIGHEST) for i in every]
        inv = [inv[i] - dot(inv[i], mids[i], HIGHEST) for i in every]
        size *= 2
    inv = [m.astype(BF16) for m in inv]
    nv = [dot(inv[i], terms[i][2].astype(BF16)) for i in every]
    kw = [dot(inv[i], terms[i][3].astype(BF16)).astype(BF16) for i in every]
    state = [None] * seqs
    for n in range(Z):
        for b in range(seqs):
            i = b * Z + n
            _, scores, _, _, qd_, kd_, factor = terms[i]
            corrected = nv[i]
            if n:
                s_in = state[b].astype(BF16)
                corrected = corrected - dot(kw[i], s_in)
            o = dot(scores.astype(BF16), corrected.astype(BF16))
            if n:
                o = o + dot(qd_.astype(BF16), s_in)
            grown = t_dot(kd_.astype(BF16), corrected.astype(BF16))
            state[b] = state[b] * factor + grown if n else grown
            o = o * lax.rsqrt(jnp.mean(o * o, axis=-1, keepdims=True) + NORM_EPS) * gain[...]
            hsrc[0, n, b * BLOCK : (b + 1) * BLOCK] = o.astype(BF16)

    def give(kind):
        for k in range(1, Z):
            to = lax.rem(z + k, Z)
            H.put(True, hsrc.at[kind, to], hbuf.at[x, kind, z], hrecv.at[x, kind, z], {"sp": to})
        hbuf[x, kind, z] = hsrc[kind, z]
        H.put(True, hsrc.at[kind, z], hbuf.at[x, kind, z], hrecv.at[x, kind, z], {"fs": 1 - x})

    def pass_heads(kind):
        for k in range(1, Z):
            zz = lax.rem(z - k + Z, Z)
            ref = hbuf.at[x, kind, zz]
            landed(True, ref, dummy.at[2], hrecv.at[x, kind, zz], c)
            H.put(True, ref, ref, hrecv.at[x, kind, zz], {"fs": 1 - x})

    give(0)
    for k in range(1, Z):
        zz = lax.rem(z - k + Z, Z)
        landed(c == 0, lat.at[zz], dummy.at[2], lrecv.at[zz], c)
        latput(c == 0, zz, {"tp": 1 - c})
    for k in range(1, nk):
        slot = Z + lax.rem(kblock + k, nk)
        landed(c == 1, lat.at[slot], dummy.at[2], lrecv.at[slot], c)
        latput(c == 1, slot, {"tp": 1 - c})
    for s in range(Z):
        landed(c == 1, lat.at[s], dummy.at[2], lrecv.at[s], c)
    for s in range(Z, Z + nk):
        landed(c == 0, lat.at[s], dummy.at[2], lrecv.at[s], c)

    scale = per ** (-0.5)
    la = lax.broadcasted_iota(jnp.int32, (length, length), 1) // BLOCK
    lb = lax.broadcasted_iota(jnp.int32, (length, length), 0) // BLOCK
    allowed = la <= lb
    lcol = pl.ds(pl.multiple_of(z * lh * tile, lh * tile), lh * tile)

    def normed_parts(slots, at, g_):
        parts = [lat[s, at].astype(F32) for s in slots]
        squares = sum(jnp.sum(p * p, axis=-1, keepdims=True) for p in parts)
        factor = lax.rsqrt(squares / (len(parts) * tile) + NORM_EPS)
        return jnp.concatenate(
            [(p * factor * g_[:, i * tile : (i + 1) * tile]).astype(BF16)
             for i, p in enumerate(parts)], axis=1
        )

    for b in range(seqs):
        at = slice(b * length, (b + 1) * length)
        ta, tb = turn_a[...], turn_b[...]
        qn = normed_parts(range(Z), at, qgain)
        kn = normed_parts(range(Z, Z + nk), at, kgain)
        qa = dot(qn, qsel[...]).astype(BF16).astype(F32)
        ka = dot(kn, lup_v[:, lcol]).astype(BF16)
        rope = sm[at].astype(BF16).astype(F32)
        turned = (rope[:, :tile] * ta + rope[:, tile:] * tb).astype(BF16)
        outs_ = []
        for j in range(lh):
            qf = (qa[:, j * tile : (j + 1) * tile] * ta
                  + qa[:, (lh + j) * tile : (lh + j + 1) * tile] * tb).astype(BF16)
            kj = ka[:, j * tile : (j + 1) * tile]
            kf = jnp.where(lane < NOPE, kj, turned)
            s = jnp.where(allowed, dot_t(qf, kf) * scale, -jnp.inf)
            w = jnp.exp(s - jnp.max(s, axis=-1, keepdims=True))
            o = dot(w.astype(BF16), kj) / jnp.sum(w, axis=-1, keepdims=True)
            outs_.append(o)
        both_ = jnp.where(lane < VDIM, pltpu.roll(outs_[0], VDIM, 1), outs_[1]).astype(BF16)
        for n in range(Z):
            hsrc[1, n, b * BLOCK : (b + 1) * BLOCK] = both_[n * BLOCK : (n + 1) * BLOCK]
    give(1)
    pass_heads(0)
    out_pass(1)
    pass_heads(1)
    for dist in range(2, Z):
        out_pass(dist)
    for kind in range(2):
        for zz in range(Z):
            landed(True, hbuf.at[1 - x, kind, zz], dummy.at[2], hrecv.at[1 - x, kind, zz], c)
    hv = jnp.concatenate(
        [jnp.concatenate([hbuf[xx, kind, s] for kind in range(2) for s in range(Z)], axis=1)
         for xx in range(X)], axis=0
    )
    rows = hbuf.shape[3]
    cb = obuf.shape[2]
    zh = Z // 2
    for i in range(Z):
        zz = lax.rem(z + i, Z)
        if i:
            landed(True, obuf.at[zz, oyours], dummy.at[0], orecv.at[zz, 1 - y], c)
        res = dot(hv, obuf[zz]).astype(BF16)
        owner, at = zz // zh, lax.rem(zz, zh)
        for xx in range(X):
            pbuf[zz, xx] = res[xx * rows : (xx + 1) * rows]
        for to in range(2):
            R.put(owner == to, pbuf.at[zz, 1 - x], rbuf.at[c, 1, at], precv.at[c, 1, at],
                  {"fs": 1 - x, "tp": to})
        R.put(owner != c, pbuf.at[zz, x], rbuf.at[1 - c, 0, at], precv.at[1 - c, 0, at],
              {"tp": 1 - c})
    for p in (W, N, L, H, O):
        p.drain()
    total = jnp.zeros((rows, 1), F32)
    mixed = []
    for at in range(zh):
        landed(True, rbuf.at[c, 0, at], dummy.at[2], precv.at[c, 0, at], c)
        m = pbuf[c * zh + at, x].astype(F32) + rbuf[c, 0, at].astype(F32)
        mixed.append((at * X + x, m))
        total = total + jnp.sum(m * m, axis=-1, keepdims=True)
    for at in range(zh):
        for cc in range(2):
            landed(True, rbuf.at[cc, 1, at], dummy.at[2], precv.at[cc, 1, at], c)
        m = rbuf[0, 1, at].astype(F32) + rbuf[1, 1, at].astype(F32)
        mixed.append((at * X + 1 - x, m))
        total = total + jnp.sum(m * m, axis=-1, keepdims=True)
    sq[0] = jnp.broadcast_to(total, sq.shape[1:])
    squares = pltpu.make_async_remote_copy(
        src_ref=sq.at[0], dst_ref=sq.at[1], send_sem=tsem.at[0], recv_sem=tsem.at[1],
        device_id={"tp": 1 - c}, device_id_type=MESH,
    )
    squares.start()
    R.drain()
    squares.wait()
    total = total + sq[1][:, :1]
    norm = lax.rsqrt(total / (Z * X * cb) + NORM_EPS)
    for s, m in mixed:
        at = pl.ds(pl.multiple_of(s * cb, cb), cb)
        out[:, at] = (m * norm * post[s]).astype(BF16)


def splits_by_heads(sizes, seqs, count, qw, qd, kd, qup, lup, do, lo):
    Y, Z, X, C = sizes
    nk = kd[1] // 128
    return (
        Y == 2 and X == 2 and C == 2 and seqs == C and count == BLOCK and qw[1] == Z * HEAD
        and qd[1] == Z * 128 and kd[1] == nk * 128 and Z % nk == 0 and Z % 2 == 0
        and do[0] == lo[0]
        and qup[1] == Z * 2 * (NOPE + ROPE) and lup[1] == Z * 2 * (NOPE + VDIM)
    )


def by_heads(sizes, *arrays):
    (tokens, pre_gain, query_weight, key_weight, value_weight, beta_weight, decay_weight,
     decay_rate, delta_gain, query_down, latent_down, rope_weight, query_gain, latent_gain,
     query_up, latent_up, delta_out, latent_out, post_gain) = arrays
    Y, Z, X, C = sizes
    n = Z * X
    seqs, count, width = tokens.shape
    rows = seqs * count
    shard = query_weight.shape[0]
    nk = latent_down.shape[1] // 128
    cb = delta_out.shape[1]
    depth = delta_out.shape[0] + latent_out.shape[0]
    half = n // 2
    lh = query_up.shape[1] // (NOPE + ROPE) // Z
    total = rows * Z
    ncol = 4 * 128
    small = [w.T for w in (beta_weight, decay_weight, rope_weight)]
    args = (
        tokens.reshape(rows, width), pre_gain.reshape(1, width),
        small[0], small[1], small[2],
        query_weight, key_weight, value_weight, query_down, latent_down, delta_out, latent_out,
        query_gain.reshape(1, -1), latent_gain.reshape(1, -1), query_up, latent_up,
        decay_rate.reshape(1, -1), delta_gain.reshape(1, HEAD), post_gain.reshape(half, 1, cb),
    )
    hbm = (0, 2, 3, 4, 5, 6, 7, 8, 9, 10, 11, 14, 15)
    DMA = pltpu.SemaphoreType.DMA
    result = pl.pallas_call(
        functools.partial(heads_kernel, sizes, seqs),
        name="layer",
        out_shape=jax.ShapeDtypeStruct((rows, half * cb), BF16),
        in_specs=[anywhere() if i in hbm else vmem() for i in range(len(args))],
        out_specs=vmem(),
        scratch_shapes=[
            pltpu.VMEM((rows, width), BF16),
            pltpu.VMEM(small[0].shape, BF16),
            pltpu.VMEM(small[1].shape, BF16),
            pltpu.VMEM(small[2].shape, BF16),
            pltpu.VMEM(query_up.shape, BF16),
            pltpu.VMEM(latent_up.shape, BF16),
            pltpu.VMEM((Z, shard, ncol), BF16),
            pltpu.VMEM((n, shard, ncol), BF16),
            pltpu.VMEM((seqs, Z, BLOCK, width), BF16),
            pltpu.VMEM((256, width), BF16),
            pltpu.VMEM((query_up.shape[0], 2 * lh * 128), BF16),
            pltpu.VMEM((Z * BLOCK, 128), F32),
            pltpu.VMEM((Z * BLOCK, 128), F32),
            pltpu.VMEM((total, 384), BF16),
            pltpu.VMEM((total, 256), F32),
            pltpu.VMEM((Z + nk, total, 128), BF16),
            pltpu.VMEM((2, Z, rows, 128), BF16),
            pltpu.VMEM((X, 2, Z, rows, 128), BF16),
            pltpu.VMEM((Z, depth, cb), BF16),
            pltpu.VMEM((Z, X, rows, cb), BF16),
            pltpu.VMEM((2, 2, Z // 2, rows, cb), BF16),
            pltpu.VMEM((2, rows, 128), F32),
            DMA((4 * Z + 8,)),
            DMA((4 * Z,)),
            DMA((n, 2)),
            DMA((2 + 4 * Z,)),
            DMA((seqs, Z)),
            DMA((2 * Z + 2 * nk,)),
            DMA((Z + nk,)),
            DMA((4 * Z,)),
            DMA((X, 2, Z)),
            DMA((4 + 6 * Z,)),
            DMA((Z, 2)),
            DMA((3 * Z,)),
            DMA((2, 2, Z // 2)),
            DMA((1,)),
            DMA((3,)),
            DMA((2,)),
        ],
        compiler_params=pltpu.CompilerParams(
            collective_id=0, has_side_effects=True, vmem_limit_bytes=60 * 1024 * 1024
        ),
    )(*args)
    return result.reshape(seqs, count, half * cb)


def solution(mesh):
    sizes = tuple(mesh.shape[a] for a in ("grp", "sp", "fs", "tp"))
    return jax.shard_map(
        functools.partial(local, sizes),
        mesh=mesh,
        in_specs=(
            P(("grp", "fs"), "sp", None),
            P(),
            P(("sp", "fs"), "tp"),
            P(("sp", "fs"), "tp"),
            P(("sp", "fs"), "tp"),
            P(),
            P(),
            P(),
            P(),
            P(("sp", "fs"), None),
            P(("sp", "fs"), None),
            P(),
            P(),
            P(),
            P(None, "tp"),
            P(None, "tp"),
            P("tp", ("sp", "fs")),
            P("tp", ("sp", "fs")),
            P("tp"),
        ),
        out_specs=P(("grp", "fs"), "sp", "tp"),
        check_vma=False,
    )
```

```python
import functools
import math

import jax
import jax.numpy as jnp
from jax import lax
from jax.experimental import pallas as pl
from jax.experimental.pallas import tpu as pltpu
from jax.sharding import PartitionSpec as P

HEAD = 128
NOPE = 64
ROPE = 32
VDIM = 64
BLOCK = 64
NORM_EPS = 1e-06
ROPE_THETA = 10000.0
HIGHEST = lax.Precision.HIGHEST
MESH = pl.DeviceIdType.MESH
F32 = jnp.float32
BF16 = jnp.bfloat16


def dot(a, b, precision=None):
    return jnp.dot(a, b, preferred_element_type=F32, precision=precision)


def dot_t(a, b, precision=None):
    return lax.dot_general(
        a, b, (((1,), (1,)), ((), ())), preferred_element_type=F32, precision=precision
    )


def t_dot(a, b, precision=None):
    return lax.dot_general(
        a, b, (((0,), (0,)), ((), ())), preferred_element_type=F32, precision=precision
    )


def when(cond, fn):
    if cond is True:
        fn()
    elif cond is not False:
        pl.when(cond)(fn)


def both(a, b):
    if a is True:
        return b
    if b is True:
        return a
    return jnp.logical_and(a, b)


class Place:
    def __init__(self, sizes):
        self.Y, self.Z, self.X, self.C = sizes
        self.y = lax.axis_index("grp")
        self.z = lax.axis_index("sp")
        self.x = lax.axis_index("fs")
        self.c = lax.axis_index("tp")


def greet(place, plane=True, later=False):
    barrier = pltpu.get_barrier_semaphore()

    def signal(cond, dev):
        when(
            cond,
            lambda: pl.semaphore_signal(barrier, inc=1, device_id=dev, device_id_type=MESH),
        )

    count = jnp.int32(0)
    if later:
        for k in range(1, place.Z):
            signal(place.z + k < place.Z, {"sp": place.z + k})
            signal(place.z - k >= 0, {"sp": place.z - k})
        count += place.Z - 1
    else:
        signal(place.z + 1 < place.Z, {"sp": place.z + 1})
        signal(place.z > 0, {"sp": place.z - 1})
        count += (place.z + 1 < place.Z).astype(jnp.int32) + (place.z > 0).astype(jnp.int32)
    if plane:
        for d in range(1, place.X):
            signal(True, {"fs": lax.rem(place.x + d, place.X)})
        count += place.X - 1
        if place.Y == 2:
            signal(True, {"grp": 1 - place.y})
            count += 1
    signal(True, {"tp": 1 - place.c})
    count += 1
    pl.semaphore_wait(barrier, count)


class Gather:
    def __init__(self, place, own, buf, send, recv, lsem):
        self.pl, self.own, self.buf = place, own, buf
        self.send, self.recv, self.lsem = send, recv, lsem
        self.sends = []
        self.ev = 0

    def active(self, p):
        return True if p == 2 else self.pl.y == p

    def push(self, cond, src, p, slot, dev, ev, way):
        index = len(self.sends)

        def make():
            return pltpu.make_async_remote_copy(
                src_ref=src,
                dst_ref=self.buf(p, slot),
                send_sem=self.send.at[index],
                recv_sem=self.recv.at[slot, p],
                device_id=dev,
                device_id_type=MESH,
            )

        when(cond, lambda: make().start())
        self.sends.append((cond, make))

    def arrived(self, cond, p, slot):
        def wait():
            ref = self.buf(p, slot)
            pltpu.make_async_remote_copy(
                src_ref=ref,
                dst_ref=ref,
                send_sem=self.lsem.at[p],
                recv_sem=self.recv.at[slot, p],
                device_id={"tp": self.pl.c},
                device_id_type=MESH,
            ).wait_recv()

        when(cond, wait)

    def across(self, cond, src, p, slot, ev):
        q = self.pl
        for d in range(1, q.X):
            self.push(cond, src, p, slot, {"fs": lax.rem(q.x + d, q.X)}, ev, 1 + d)

    def to_y(self, cond, src, p, slot, ev):
        if p < 2:
            self.push(cond, src, p, slot, {"grp": 1 - self.pl.y}, ev, 0)

    def kinds(self):
        return (0, 1, 2)

    def start_along(self):
        q = self.pl
        me = q.z * q.X + q.x
        for p in self.kinds():
            a = self.active(p)
            src = self.own(p)
            self.push(both(a, q.z + 1 < q.Z), src, p, me, {"sp": q.z + 1}, 0, 0)
            self.push(both(a, q.z > 0), src, p, me, {"sp": q.z - 1}, 0, 1)

    def start_across(self):
        q = self.pl
        me = q.z * q.X + q.x
        for p in self.kinds():
            self.across(self.active(p), self.own(p), p, me, 0)
        for p in self.kinds():
            pltpu.make_async_copy(self.own(p), self.buf(p, me), self.lsem.at[p]).start()

    def step(self, k):
        q = self.pl
        for p in self.kinds():
            a = self.active(p)
            for sign in (1, -1):
                zz = q.z - sign * k
                ok = both(a, jnp.logical_and(zz >= 0, zz < q.Z))
                slot = zz * q.X + q.x
                nxt = q.z + sign
                ev = 2 * k - (sign == 1)
                self.arrived(ok, p, slot)
                ref = self.buf(p, slot)
                self.push(
                    both(ok, jnp.logical_and(nxt >= 0, nxt < q.Z)),
                    ref, p, slot, {"sp": nxt}, ev, 1,
                )
                self.across(ok, ref, p, slot, ev)
                self.to_y(ok, ref, p, slot, ev)

    def cross_step(self, k):
        q = self.pl
        base = 2 * q.Z
        for p in self.kinds():
            a = self.active(p)
            for sign in (1, -1) if k else (1,):
                zz = q.z - sign * k
                ok = both(a, jnp.logical_and(zz >= 0, zz < q.Z))
                for d in range(1, q.X):
                    slot = zz * q.X + lax.rem(q.x + d, q.X)
                    ev = base + (2 * k - (sign == 1) + 1) * (q.X - 1) + d - 1
                    self.arrived(ok, p, slot)
                    self.to_y(ok, self.buf(p, slot), p, slot, ev)

    def finish(self):
        q = self.pl
        self.cross_step(q.Z - 1)
        me = q.z * q.X + q.x
        for p in (0, 1):
            for s in range(q.Z * q.X):
                self.arrived(jnp.logical_and(q.y != p, me != s), p, s)
        for p in self.kinds():
            pltpu.make_async_copy(self.own(p), self.buf(p, me), self.lsem.at[p]).wait()

    def drain(self):
        for cond, make in self.sends:
            when(cond, lambda make=make: make().wait_send())

    @staticmethod
    def scratch(Z, X):
        n = Z * X
        sends = 3 * (X + 1) + 2 * (Z - 1) * (3 * X + 2) + (2 * Z - 1) * (X - 1) * 2
        return [
            pltpu.SemaphoreType.DMA((sends,)),
            pltpu.SemaphoreType.DMA((n, 3)),
            pltpu.SemaphoreType.DMA((3,)),
        ]


def spread(copies, parts, target, bounds):
    at = 0
    for ref, offset, width in parts:
        done = 0
        while done < width:
            p, col = divmod(at + done, bounds)
            size = min(width - done, bounds - col)
            start = offset + done
            if not isinstance(start, int):
                start = pl.multiple_of(start, 128)
            copies.append((ref.at[:, pl.ds(start, size)], target.at[p, :, pl.ds(col, size)]))
            done += size
        at += width


def back_kernel(
    sizes, seqs, heads, cuts, tokens, pre_gain, small, w_query, w_key, w_value, w_qdown, w_kdown,
    w_delta, w_latent, qgain, kgain, w_qup, w_lup, rate_in, gain, post,
    out, qup, lup, raw, lat, rate, own1, own, buf1, kvr, kbuf, sin, sout, hbuf, buf, pbuf, rbuf, sq,
    asem, ksem, ssem, send1, recv1, lsem1, send, recv, lsem, tsem,
):
    place = Place(sizes)
    Z, z, c = place.Z, place.z, place.c
    C = sizes[3]
    rows = tokens.shape[0]
    third = own1.shape[2]
    qcols, kcols = w_qdown.shape[1] // C, w_kdown.shape[1] // C
    pairs = []
    spread(
        pairs,
        [(w, 0, w.shape[1]) for w in (w_query, w_key, w_value)]
        + [(w_qdown, c * qcols, qcols), (w_kdown, c * kcols, kcols)],
        own1, third,
    )
    upper = w_delta.shape[0]
    pairs.append((w_delta, own.at[pl.ds(0, upper)]))
    pairs.append((w_latent, own.at[pl.ds(upper, w_latent.shape[0])]))
    loads = [pltpu.make_async_copy(a, b, asem.at[i]) for i, (a, b) in enumerate(pairs)]
    for load in loads:
        load.start()
    greet(place, later=True)
    for load in loads:
        load.wait()
    g1 = Gather(
        place, lambda p: own1.at[p], lambda p, s: buf1.at[p, s], send1, recv1, lsem1
    )
    g = Gather(
        place,
        lambda p: own.at[pl.ds(cuts[p], cuts[p + 1] - cuts[p])],
        lambda p, s: buf.at[s, pl.ds(cuts[p], cuts[p + 1] - cuts[p])],
        send, recv, lsem,
    )
    g1.start_along()
    g1.start_across()
    x = tokens[...].astype(F32)
    xscale = lax.rsqrt(jnp.mean(x * x, axis=-1, keepdims=True) + NORM_EPS)
    normed = (x * xscale * pre_gain[...]).astype(BF16)
    sm_all = dot_t(normed, small[...])
    qcol = w_qup.shape[1]
    lh = qcol // (NOPE + ROPE)
    turn_w = ROPE // 2
    kinds = ((NOPE, 0, qup, w_qup, NOPE + ROPE), (turn_w, NOPE, qup, w_qup, NOPE + ROPE),
             (turn_w, NOPE + turn_w, qup, w_qup, NOPE + ROPE),
             (NOPE, 0, lup, w_lup, NOPE + VDIM), (VDIM, NOPE, lup, w_lup, NOPE + VDIM))
    fill_at = {}
    for w, off, to, frm, per in kinds:
        size = lh * w
        dst_i = lax.broadcasted_iota(jnp.int32, (frm.shape[1], size), 1)
        src_i = lax.broadcasted_iota(jnp.int32, (frm.shape[1], size), 0)
        perm = jnp.where(src_i == dst_i // w * per + off + dst_i % w, 1.0, 0.0).astype(BF16)
        lo = fill_at.get(per, 0)
        to[:, lo : lo + size] = dot(frm[...], perm).astype(BF16)
        fill_at[per] = lo + size
    for k in range(1, Z):
        g1.step(k)
        g1.cross_step(k - 1)
        if k == max(1, Z - 2):
            g.start_along()
    g.start_across()
    if Z > 1:
        g.step(1)
    g1.finish()
    depth1 = buf1.shape[1] * buf1.shape[2]
    part2 = dot(normed, buf1[2].reshape(depth1, third)).astype(BF16)
    lat[c] = part2[:, third - qcols - kcols :]
    trade = pltpu.make_async_remote_copy(
        src_ref=lat.at[c], dst_ref=lat.at[c], send_sem=tsem.at[4], recv_sem=tsem.at[5],
        device_id={"tp": 1 - c}, device_id_type=MESH,
    )
    trade.start()
    raw[:, 2 * third : 3 * third] = part2
    for p in range(2):
        raw[:, p * third : (p + 1) * third] = dot(
            normed, buf1[p].reshape(depth1, third)
        ).astype(BF16)
    trade.wait()
    qw = qup.shape[0] // sizes[3]
    kw_lat = lup.shape[0] // sizes[3]
    tile = 128
    lane = lax.broadcasted_iota(jnp.int32, (rows, tile), 1)
    half_turn = ROPE // 2
    step = (lane % half_turn).astype(F32)
    row = lax.broadcasted_iota(jnp.int32, (rows, tile), 0)
    pos = (z * BLOCK + row % BLOCK).astype(F32)
    angle = pos * jnp.exp(step * (-2.0 * math.log(ROPE_THETA) / ROPE))
    cos, sin_t = jnp.cos(angle), jnp.sin(angle)

    def normed_parts(lo, w, g):
        parts = [lat[i, :, lo : lo + w].astype(F32) for i in range(sizes[3])]
        squares = sum(jnp.sum(p * p, axis=-1, keepdims=True) for p in parts)
        scale = lax.rsqrt(squares / (w * sizes[3]) + NORM_EPS)
        return [
            (p * scale * g[:, i * w : (i + 1) * w]).astype(BF16) for i, p in enumerate(parts)
        ]

    kparts = normed_parts(qw, kw_lat, kgain)
    krank = kw_lat * sizes[3]
    for i, p in enumerate(kparts):
        kvr[:, i * kw_lat : (i + 1) * kw_lat] = p
    allheads = heads * C
    src = lax.broadcasted_iota(jnp.int32, (tile, tile), 0)
    dst = lax.broadcasted_iota(jnp.int32, (tile, tile), 1)
    rope_raw = sm_all.astype(BF16)
    base = 2 * allheads + dst % half_turn

    def pick(cond, kind):
        return jnp.where(cond, 1.0, 0.0).astype(kind)

    rlo = dot(rope_raw, pick(src == base, BF16))
    rhi = dot(rope_raw, pick(src == base + half_turn, BF16))
    left = lane < tile // 2
    kvr[:, krank : krank + tile] = jnp.where(
        left, rlo * cos - rhi * sin_t, rhi * cos + rlo * sin_t
    ).astype(BF16)

    def kv_copy(k):
        return pltpu.make_async_remote_copy(
            src_ref=kvr,
            dst_ref=kbuf.at[z],
            send_sem=ksem.at[0, k],
            recv_sem=ksem.at[1, z],
            device_id={"sp": z + k},
            device_id_type=MESH,
        )

    for k in range(1, Z):
        when(z + k < Z, lambda k=k: kv_copy(k).start())
    ri = lax.broadcasted_iota(jnp.int32, (rows, rows), 0)
    ci = lax.broadcasted_iota(jnp.int32, (rows, rows), 1)
    tri = jnp.where((ri >= ci) & (ri // BLOCK == ci // BLOCK), 1.0, 0.0).astype(F32)
    rate[...] = jnp.zeros(rate.shape, F32)
    rate[:, allheads : 2 * allheads] = rate_in[...]
    first_head = c * heads
    own_beta = pick((dst < heads) & (src == first_head + dst), F32)
    own_rate = pick(
        (dst >= heads) & (dst < 2 * heads) & (src == allheads + first_head + dst - heads), F32
    )
    pre = dot(sm_all, own_beta + own_rate, HIGHEST)
    rates = dot(jnp.broadcast_to(rate[...], (8, tile)), own_rate, HIGHEST)[:1]
    beta_all = jax.nn.sigmoid(pre)
    log_a = -rates * (jnp.maximum(pre, 0.0) + jnp.log1p(jnp.exp(-jnp.abs(pre))))
    gates = dot(tri, log_a, HIGHEST)
    gates_t = gates.T
    r = lax.broadcasted_iota(jnp.int32, (BLOCK, BLOCK), 0)
    cc = lax.broadcasted_iota(jnp.int32, (BLOCK, BLOCK), 1)
    strict = r > cc
    causal = r >= cc
    eye = jnp.where(r == cc, 1.0, 0.0).astype(F32)
    lanes = [(b, h) for b in range(seqs) for h in range(heads)]
    width = heads * HEAD
    terms = []
    for b, h in lanes:
        t = slice(b * BLOCK, (b + 1) * BLOCK)

        def act(i):
            v = raw[t, i * width + h * HEAD : i * width + (h + 1) * HEAD].astype(F32)
            return v * jax.nn.sigmoid(v)

        def unit(u):
            return u * lax.rsqrt(jnp.sum(u * u, axis=-1, keepdims=True) + NORM_EPS)

        q = unit(act(0)) * HEAD ** (-0.5)
        k = unit(act(1))
        v = act(2)
        beta = beta_all[t, h : h + 1]
        gcol = gates[t, heads + h : heads + h + 1]
        grow = gates_t[heads + h : heads + h + 1, t]
        glast = gates[(b + 1) * BLOCK - 1 : (b + 1) * BLOCK, heads + h : heads + h + 1]
        gap = gcol - grow
        decay = jnp.where(causal, jnp.exp(jnp.where(causal, gap, 0.0)), 0.0)
        ks = k * beta
        low = jnp.where(strict, dot_t(ks, k, HIGHEST) * decay, 0.0)
        scores = dot_t(q.astype(BF16), k.astype(BF16)) * decay
        eg = jnp.exp(gcol)
        terms.append([low, scores, v * beta, ks * eg, q * eg, k * jnp.exp(glast - gcol),
                      jnp.exp(glast)])
    every = range(len(lanes))
    inv = [eye - jnp.where((r // 2 == cc // 2), terms[i][0], 0.0) for i in every]
    size = 2
    while size < BLOCK:
        joint = (r // (2 * size) == cc // (2 * size)) & (r // size != cc // size)
        mids = [dot(jnp.where(joint, terms[i][0], 0.0), inv[i], HIGHEST) for i in every]
        inv = [inv[i] - dot(inv[i], mids[i], HIGHEST) for i in every]
        size *= 2
    inv = [m.astype(BF16) for m in inv]
    nv = [dot(inv[i], terms[i][2].astype(BF16)) for i in every]
    kw = [dot(inv[i], terms[i][3].astype(BF16)) for i in every]

    def state_copy(i):
        return pltpu.make_async_remote_copy(
            src_ref=sout.at[i],
            dst_ref=sin.at[i],
            send_sem=ssem.at[0, i],
            recv_sem=ssem.at[1, i],
            device_id={"sp": z + 1},
            device_id_type=MESH,
        )

    g.cross_step(0)
    if Z > 2:
        g.step(2)
    for i, (b, h) in enumerate(lanes):
        low, scores, vb, ke, qd, kd, factor = terms[i]

        def clear(i=i):
            sin[i] = jnp.zeros((HEAD, HEAD), BF16)

        when(z == 0, clear)
        when(z > 0, lambda i=i: state_copy(i).wait_recv())
        s_in = sin[i]
        corrected = nv[i] - dot(kw[i].astype(BF16), s_in)
        sout[i] = (
            s_in.astype(F32) * factor + t_dot(kd.astype(BF16), corrected.astype(BF16))
        ).astype(BF16)
        when(z + 1 < Z, lambda i=i: state_copy(i).start())
        o = dot(qd.astype(BF16), s_in) + dot(scores.astype(BF16), corrected.astype(BF16))
        o = o * lax.rsqrt(jnp.mean(o * o, axis=-1, keepdims=True) + NORM_EPS) * gain[...]
        hbuf[b * BLOCK : (b + 1) * BLOCK, h * HEAD : (h + 1) * HEAD] = o.astype(BF16)
    g.cross_step(1)
    for k in range(3, Z):
        g.step(k)
        if k < Z - 1:
            g.cross_step(k - 1)

    for k in range(1, Z):
        def take(k=k):
            pltpu.make_async_remote_copy(
                src_ref=kvr, dst_ref=kbuf.at[z - k], send_sem=ksem.at[0, k],
                recv_sem=ksem.at[1, z - k], device_id={"sp": z}, device_id_type=MESH,
            ).wait_recv()

        when(z - k >= 0, take)
    for s in range(Z):
        def fill(s=s):
            kbuf[s] = kvr[...]

        def none(s=s):
            kbuf[s] = jnp.zeros(kbuf.shape[1:], BF16)

        when(z == s, fill)
        when(z < s, none)
    qparts = normed_parts(0, qw, qgain)
    qa = sum(dot(p, qup[i * qw : (i + 1) * qw, :]) for i, p in enumerate(qparts)).astype(BF16)
    plain_width = qa.shape[1] - 2 * tile
    qlo_raw = qa[:, plain_width : plain_width + tile].astype(F32)
    qhi_raw = qa[:, plain_width + tile :].astype(F32)
    qlo = (qlo_raw * cos - qhi_raw * sin_t).astype(BF16)
    qhi = (qhi_raw * cos + qlo_raw * sin_t).astype(BF16)
    lane1 = lax.broadcasted_iota(jnp.int32, (1, tile), 1)

    def keep(cond):
        return jnp.where(cond, 1.0, 0.0).astype(BF16)

    keys = Z * BLOCK
    allowed = lax.broadcasted_iota(jnp.int32, (2 * BLOCK, keys), 1) // BLOCK <= z
    left_half = lax.broadcasted_iota(jnp.int32, (BLOCK, tile), 1) < tile // 2
    for b in range(seqs):
        t = slice(b * BLOCK, (b + 1) * BLOCK)
        kv = jnp.concatenate([kbuf[s, t, :] for s in range(Z)], axis=0)
        up = dot(kv[:, :krank], lup[...]).astype(BF16)
        turn = kv[:, krank : krank + tile].astype(F32)
        rolled = pltpu.roll(turn, tile // 2, 1)
        sel = lax.broadcasted_iota(jnp.int32, (keys, tile), 1) < tile // 2
        klo = jnp.where(sel, turn, rolled).astype(BF16)
        khi = jnp.where(sel, rolled, turn).astype(BF16)
        for j in range(plain_width // tile):
            at = slice(j * tile, (j + 1) * tile)
            qp = qa[t, at]
            first, second = keep(lane1 < tile // 2), keep(lane1 >= tile // 2)
            m0, m1 = keep(lane1 // half_turn == 2 * j), keep(lane1 // half_turn == 2 * j + 1)
            s = (
                dot_t(jnp.concatenate([qp * first, qp * second], axis=0), up[:, at])
                + dot_t(jnp.concatenate([qlo[t] * m0, qlo[t] * m1], axis=0), klo)
                + dot_t(jnp.concatenate([qhi[t] * m0, qhi[t] * m1], axis=0), khi)
            ) * (NOPE + ROPE) ** (-0.5)
            s = jnp.where(allowed, s, -jnp.inf)
            w = jnp.exp(s - jnp.max(s, axis=-1, keepdims=True))
            o = dot(w.astype(BF16), up[:, plain_width + j * tile : plain_width + (j + 1) * tile])
            o = o / jnp.sum(w, axis=-1, keepdims=True)
            hbuf[t, width + j * tile : width + (j + 1) * tile] = jnp.where(
                left_half, o[:BLOCK], o[BLOCK:]
            ).astype(BF16)
    if Z > 3:
        g.cross_step(Z - 2)
    g.finish()
    n = buf.shape[0]
    half = n // 2
    hv = hbuf[...]

    def part(s, carry):
        pbuf[s] = dot(hv, buf[s]).astype(BF16)
        return carry

    lax.fori_loop(0, n, part, 0)
    peer = 1 - c
    copy = pltpu.make_async_remote_copy(
        src_ref=pbuf.at[pl.ds(peer * half, half)],
        dst_ref=rbuf,
        send_sem=tsem.at[0],
        recv_sem=tsem.at[1],
        device_id={"tp": peer},
        device_id_type=MESH,
    )
    copy.start()
    g1.drain()
    g.drain()
    for k in range(1, Z):
        when(z + k < Z, lambda k=k: kv_copy(k).wait_send())
    for i in every:
        when(z + 1 < Z, lambda i=i: state_copy(i).wait_send())
    copy.wait()
    total = jnp.zeros((rows, 1), F32)
    mixed = []
    for s in range(half):
        m = pbuf[c * half + s].astype(F32) + rbuf[s].astype(F32)
        mixed.append(m)
        total = total + jnp.sum(m * m, axis=-1, keepdims=True)
    sq[0] = jnp.broadcast_to(total, sq.shape[1:])
    squares = pltpu.make_async_remote_copy(
        src_ref=sq.at[0],
        dst_ref=sq.at[1],
        send_sem=tsem.at[2],
        recv_sem=tsem.at[3],
        device_id={"tp": peer},
        device_id_type=MESH,
    )
    squares.start()
    squares.wait()
    total = total + sq[1][:, :1]
    cb = buf.shape[2]
    scale = lax.rsqrt(total / (n * cb) + NORM_EPS)
    for s in range(half):
        out[:, s * cb : (s + 1) * cb] = (mixed[s] * scale * post[s]).astype(BF16)


def vmem():
    return pl.BlockSpec(memory_space=pltpu.VMEM)


def anywhere():
    return pl.BlockSpec(memory_space=pl.ANY)


def local(
    sizes,
    tokens, pre_gain, query_weight, key_weight, value_weight, beta_weight, decay_weight,
    decay_rate, delta_gain, query_down, latent_down, rope_weight, query_gain, latent_gain,
    query_up, latent_up, delta_out, latent_out, post_gain,
):
    Y, Z, X, C = sizes
    n = Z * X
    seqs, count, width = tokens.shape
    if splits_by_heads(sizes, seqs, count, query_weight.shape, query_down.shape,
                       latent_down.shape, query_up.shape, latent_up.shape, delta_out.shape,
                       latent_out.shape):
        return by_heads(
            sizes, tokens, pre_gain, query_weight, key_weight, value_weight, beta_weight,
            decay_weight, decay_rate, delta_gain, query_down, latent_down, rope_weight,
            query_gain, latent_gain, query_up, latent_up, delta_out, latent_out, post_gain,
        )
    rows = seqs * count
    qw = query_down.shape[1] // C
    kw = latent_down.shape[1] // C
    heads = query_weight.shape[1] // HEAD
    shard = query_weight.shape[0]
    third = (3 * query_weight.shape[1] + qw + kw) // 3
    small = [beta_weight.T, decay_weight.T, rope_weight.T]
    used = sum(w.shape[0] for w in small)
    small = jnp.concatenate(small + [jnp.zeros((128 - used, width), BF16)], axis=0)
    lanes = seqs * heads
    cb = delta_out.shape[1]
    depth = delta_out.shape[0] + latent_out.shape[0]
    cuts = (0, depth * 3 // 8, depth * 6 // 8, depth)
    half = n // 2
    kv_width = latent_down.shape[1] + 128
    args = (
        tokens.reshape(rows, width), pre_gain.reshape(1, width), small,
        query_weight, key_weight, value_weight, query_down, latent_down, delta_out, latent_out,
        query_gain.reshape(1, -1), latent_gain.reshape(1, -1), query_up, latent_up,
        decay_rate.reshape(1, -1), delta_gain.reshape(1, HEAD), post_gain.reshape(half, 1, cb),
    )
    result = pl.pallas_call(
        functools.partial(back_kernel, sizes, seqs, heads, cuts),
        name="layer",
        out_shape=jax.ShapeDtypeStruct((rows, half * cb), BF16),
        in_specs=[anywhere() if 3 <= i < 10 else vmem() for i in range(len(args))],
        out_specs=vmem(),
        scratch_shapes=[
            pltpu.VMEM(query_up.shape, BF16),
            pltpu.VMEM(latent_up.shape, BF16),
            pltpu.VMEM((rows, 3 * third), BF16),
            pltpu.VMEM((C, rows, qw + kw), BF16),
            pltpu.VMEM((1, 128), F32),
            pltpu.VMEM((3, shard, third), BF16),
            pltpu.VMEM((depth, cb), BF16),
            pltpu.VMEM((3, n, shard, third), BF16),
            pltpu.VMEM((rows, kv_width), BF16),
            pltpu.VMEM((Z, rows, kv_width), BF16),
            pltpu.VMEM((lanes, HEAD, HEAD), BF16),
            pltpu.VMEM((lanes, HEAD, HEAD), BF16),
            pltpu.VMEM((rows, depth), BF16),
            pltpu.VMEM((n, depth, cb), BF16),
            pltpu.VMEM((n, rows, cb), BF16),
            pltpu.VMEM((half, rows, cb), BF16),
            pltpu.VMEM((2, rows, 128), F32),
            pltpu.SemaphoreType.DMA((16,)),
            pltpu.SemaphoreType.DMA((2, Z)),
            pltpu.SemaphoreType.DMA((2, lanes)),
        ]
        + Gather.scratch(Z, X) + Gather.scratch(Z, X) + [pltpu.SemaphoreType.DMA((6,))],
        compiler_params=pltpu.CompilerParams(
            collective_id=0, has_side_effects=True, vmem_limit_bytes=60 * 1024 * 1024
        ),
    )(*args)
    return result.reshape(seqs, count, half * cb)


class Puts:
    def __init__(self, sems):
        self.sems, self.sent = sems, []

    def put(self, cond, src, dst, recv, dev):
        index = len(self.sent)

        def make():
            return pltpu.make_async_remote_copy(
                src_ref=src, dst_ref=dst, send_sem=self.sems.at[index], recv_sem=recv,
                device_id=dev, device_id_type=MESH,
            )

        when(cond, lambda: make().start())
        self.sent.append((cond, make))

    def drain(self):
        for cond, make in self.sent:
            when(cond, lambda make=make: make().wait_send())


def landed(cond, ref, dummy, recv, c):
    def wait():
        pltpu.make_async_remote_copy(
            src_ref=ref, dst_ref=ref, send_sem=dummy, recv_sem=recv,
            device_id={"tp": c}, device_id_type=MESH,
        ).wait_recv()

    when(cond, wait)


def heads_kernel(
    sizes, seqs, tokens, pre_gain, w_beta, w_decay, w_rope, w_query, w_key, w_value,
    w_qdown, w_kdown, w_delta, w_latent, qgain, kgain, w_qup, w_lup, rate_in, gain, post,
    out, tok, beta_v, decay_v, rope_v, qup_v, lup_v, wown, wbuf, nbuf, ssel, qsel, turn_a, turn_b,
    raw, sm, lat, hsrc, hbuf, obuf, pbuf, rbuf, sq,
    asem, wsend, wrecv, nsend, nrecv, lsend, lrecv, hsend, hrecv, osend, orecv, psend, precv,
    ksem, dummy, tsem,
):
    place = Place(sizes)
    Z, X = place.Z, place.X
    y, z, x, c = place.y, place.z, place.x, place.c
    tile = 128
    shard = wown.shape[1]
    part = shard // 2
    me = z * X + x
    nk = w_kdown.shape[1] // tile
    kblock = lax.rem(z, nk)
    length = Z * BLOCK
    count = seqs * length
    width = nbuf.shape[3]
    ncol = wown.shape[2]
    barrier = pltpu.get_barrier_semaphore()
    peers = [{"sp": lax.rem(z + k, Z)} for k in range(1, Z)]
    peers += [{"fs": 1 - x}, {"grp": 1 - y}, {"fs": 1 - x, "grp": 1 - y}, {"tp": 1 - c},
              {"fs": 1 - x, "tp": 1 - c}]
    for dev in peers:
        pl.semaphore_signal(barrier, inc=1, device_id=dev, device_id_type=MESH)
    loads = []

    def load(src, dst, cond=True):
        index = len(loads)

        def make():
            return pltpu.make_async_copy(src, dst, asem.at[index])

        when(cond, lambda: make().start())
        loads.append(make)
        return index

    first = []
    for d in range(Z):
        for i, w in enumerate((w_query, w_key, w_value)):
            at = wown.at[d, :, pl.ds(i * tile, tile)]
            first.append(load(w.at[:, pl.ds(d * tile, tile)], at))
        at = wown.at[d, :, pl.ds(3 * tile, tile)]
        index = load(w_qdown.at[:, pl.ds(d * tile, tile)], at, c == 0)
        first.append(index)
        kd = d % nk

        def other(kd=kd, at=at, index=index):
            pltpu.make_async_copy(
                w_kdown.at[:, pl.ds(kd * tile, tile)], at, asem.at[index]
            ).start()

        when(c == 1, other)
    tok_at = load(tokens, tok)
    rest = [load(a, b) for a, b in (
        (w_beta, beta_v), (w_decay, decay_v), (w_rope, rope_v), (w_qup, qup_v), (w_lup, lup_v),
    )]
    upper = w_delta.shape[0]
    outs = [load(w_delta, obuf.at[z, pl.ds(0, upper)]),
            load(w_latent, obuf.at[z, pl.ds(upper, w_latent.shape[0])])]

    pl.semaphore_wait(barrier, len(peers))

    for index in first:
        loads[index]().wait()
    W, N, L, H = Puts(wsend), Puts(nsend), Puts(lsend), Puts(hsend)
    O, R = Puts(osend), Puts(psend)
    mine = pl.ds(pl.multiple_of(y * part, part), part)
    yours = pl.ds(pl.multiple_of((1 - y) * part, part), part)
    for k in range(1, Z):
        to = lax.rem(z + k, Z)
        W.put(True, wown.at[to, mine], wbuf.at[me, mine], wrecv.at[me, y], {"sp": to})
    W.put(True, wown.at[z], wbuf.at[me], wrecv.at[me, 0], {"fs": 1 - x})
    keep_own = pltpu.make_async_copy(wown.at[z], wbuf.at[me], ksem.at[0])
    keep_own.start()
    loads[tok_at]().wait()
    for b in range(seqs):
        t = tok[b * BLOCK : (b + 1) * BLOCK].astype(F32)
        scale = lax.rsqrt(jnp.mean(t * t, axis=-1, keepdims=True) + NORM_EPS)
        nbuf[b, z] = (t * scale * pre_gain[...]).astype(BF16)
    chunks = nrecv.shape[2]
    span = BLOCK // chunks

    def chunk(seq, zz, i):
        return nbuf.at[seq, zz, pl.ds(i * span, span)]

    for i in range(chunks):
        for sign in (1, -1):
            nxt = z + sign
            ref = chunk(c, z, i)
            N.put(jnp.logical_and(nxt >= 0, nxt < Z), ref, ref, nrecv.at[c, z, i], {"sp": nxt})

    for index in rest:
        loads[index]().wait()
    lane = lax.broadcasted_iota(jnp.int32, (length, tile), 1)
    row = lax.broadcasted_iota(jnp.int32, (length, tile), 0)
    half_turn = ROPE // 2
    step = (lane % half_turn).astype(F32)
    angle = row.astype(F32) * jnp.exp(step * (-2.0 * math.log(ROPE_THETA) / ROPE))
    turning = (lane >= NOPE) & (lane < NOPE + ROPE)
    turn_a[...] = jnp.where(lane < NOPE, 1.0, jnp.where(turning, jnp.cos(angle), 0.0))
    sin_t = jnp.sin(angle)
    turn_b[...] = jnp.where(turning, jnp.where(lane < NOPE + half_turn, -sin_t, sin_t), 0.0)

    def pick(cond):
        return jnp.where(cond, 1.0, 0.0).astype(BF16)

    head = c * w_query.shape[1] // HEAD + z
    nb = w_beta.shape[0]
    r8 = lax.broadcasted_iota(jnp.int32, (2 * tile, nb), 1)
    l8 = lax.broadcasted_iota(jnp.int32, (2 * tile, nb), 0)
    r32 = lax.broadcasted_iota(jnp.int32, (2 * tile, ROPE), 1)
    l32 = lax.broadcasted_iota(jnp.int32, (2 * tile, ROPE), 0)
    turned_lane = jnp.where(l32 < tile, r32 + NOPE, (r32 + half_turn) % ROPE + NOPE + tile)
    ssel[...] = (
        dot(pick((r8 == head) & (l8 == 0)), beta_v[...])
        + dot(pick((r8 == head) & (l8 == 1)), decay_v[...])
        + dot(pick(l32 == turned_lane), rope_v[...])
    ).astype(BF16)
    per = NOPE + ROPE
    lh = w_qup.shape[1] // per // Z
    qd = lax.broadcasted_iota(jnp.int32, (w_qup.shape[1], tile), 1)
    qs = lax.broadcasted_iota(jnp.int32, (w_qup.shape[1], tile), 0)
    swapped = jnp.where(qd < NOPE, qd, NOPE + (qd - NOPE + half_turn) % ROPE)
    for j in range(lh):
        base = (z * lh + j) * per
        qsel[:, j * tile : (j + 1) * tile] = dot(
            qup_v[...], pick((qd < per) & (qs == base + qd))
        ).astype(BF16)
        qsel[:, (lh + j) * tile : (lh + j + 1) * tile] = dot(
            qup_v[...], pick((qd >= NOPE) & (qd < per) & (qs == base + swapped))
        ).astype(BF16)

    for index in outs:
        loads[index]().wait()
    obl = upper
    omine = pl.ds(pl.multiple_of(y * obl, obl), obl)
    oyours = pl.ds(pl.multiple_of((1 - y) * obl, obl), obl)

    def out_send():
        for sign in (1, -1):
            to = z + sign
            ref = obuf.at[z, omine]
            O.put(jnp.logical_and(to >= 0, to < Z), ref, ref, orecv.at[z, y], {"sp": to})

    def out_pass(dist):
        for sign in (1, -1):
            zz = z - sign * dist
            ok = jnp.logical_and(zz >= 0, zz < Z)
            nxt = z + sign
            ref = obuf.at[zz, omine]
            landed(ok, ref, dummy.at[0], orecv.at[zz, y], c)
            O.put(both(ok, jnp.logical_and(nxt >= 0, nxt < Z)), ref, ref, orecv.at[zz, y],
                  {"sp": nxt})
            O.put(ok, ref, ref, orecv.at[zz, y], {"grp": 1 - y})

    def wait_w(zz, xx, yy, rows):
        slot = zz * X + xx
        landed(True, wbuf.at[slot, rows], dummy.at[0], wrecv.at[slot, yy], c)

    for k in range(1, Z):
        zz = lax.rem(z - k + Z, Z)
        slot = zz * X + x
        wait_w(zz, x, y, mine)
        for dev in ({"fs": 1 - x}, {"grp": 1 - y}, {"fs": 1 - x, "grp": 1 - y}):
            ref = wbuf.at[slot, mine]
            W.put(True, ref, ref, wrecv.at[slot, y], dev)
        for i in range(chunks):
            for sign in (1, -1):
                zz = z - sign * k
                ok = jnp.logical_and(zz >= 0, zz < Z)
                nxt = z + sign
                ref = chunk(c, zz, i)
                landed(ok, ref, dummy.at[1], nrecv.at[c, zz, i], c)
                N.put(both(ok, jnp.logical_and(nxt >= 0, nxt < Z)), ref, ref,
                      nrecv.at[c, zz, i], {"sp": nxt})
                N.put(ok, ref, ref, nrecv.at[c, zz, i], {"tp": 1 - c})
        if k == max(1, Z - 2):
            out_send()
    for k in range(1, Z):
        zz = lax.rem(z - k + Z, Z)
        wait_w(zz, x, 1 - y, yours)
        wait_w(zz, 1 - x, y, mine)
        wait_w(zz, 1 - x, 1 - y, yours)
    slot = z * X + 1 - x
    landed(True, wbuf.at[slot], dummy.at[0], wrecv.at[slot, 0], c)
    keep_own.wait()
    for k in range(1, Z):
        zz = lax.rem(z - k + Z, Z)
        for i in range(chunks):
            landed(True, chunk(1 - c, zz, i), dummy.at[1], nrecv.at[1 - c, zz, i], c)

    lslot = (1 - c) * z + c * (Z + kblock)
    for b in range(seqs):
        at = slice(b * length, (b + 1) * length)
        normed = nbuf[b].reshape(length, width)
        lat[lslot, at] = dot(normed, wbuf[:, :, 3 * tile :].reshape(width, tile)).astype(BF16)

    def latput(cond, slot, dev):
        L.put(cond, lat.at[slot], lat.at[slot], lrecv.at[slot], dev)

    for k in range(1, Z):
        latput(c == 0, z, {"sp": lax.rem(z + k, Z)})
    pair = z - kblock
    for k in range(1, nk):
        latput(c == 1, Z + kblock, {"sp": pair + lax.rem(kblock + k, nk)})
    latput(True, lslot, {"tp": 1 - c})
    for b in range(seqs):
        at = slice(b * length, (b + 1) * length)
        normed = nbuf[b].reshape(length, width)
        raw[at] = dot(normed, wbuf[:, :, : 3 * tile].reshape(width, 3 * tile)).astype(BF16)
        sm[at] = dot_t(normed, ssel[...])

    ri = lax.broadcasted_iota(jnp.int32, (BLOCK, BLOCK), 0)
    ci = lax.broadcasted_iota(jnp.int32, (BLOCK, BLOCK), 1)
    strict = ri > ci
    causal = ri >= ci
    eye = jnp.where(ri == ci, 1.0, 0.0).astype(F32)
    tri = jnp.where(causal, 1.0, 0.0).astype(F32)
    units = [(b, n) for b in range(seqs) for n in range(Z)]
    lane1 = lax.broadcasted_iota(jnp.int32, (1, nb), 1)
    rate = jnp.sum(jnp.where(lane1 == head, rate_in[...], 0.0), axis=-1, keepdims=True)
    pre_b = sm[:, 0:1]
    pre_d = sm[:, 1:2]
    beta_all = jax.nn.sigmoid(pre_b)
    log_a = -rate * (jnp.maximum(pre_d, 0.0) + jnp.log1p(jnp.exp(-jnp.abs(pre_d))))
    blane = lax.broadcasted_iota(jnp.int32, (BLOCK, tile), 1)
    spread_a = jnp.zeros((BLOCK, tile), F32)
    for u in range(len(units)):
        spread_a = jnp.where(blane == u, log_a[u * BLOCK : (u + 1) * BLOCK], spread_a)
    gates = dot(tri, spread_a, HIGHEST)
    gates_t = gates.T
    terms = []
    for u in range(len(units)):
        at = slice(u * BLOCK, (u + 1) * BLOCK)

        def act(i):
            v = raw[at, i * tile : (i + 1) * tile].astype(F32)
            return v * jax.nn.sigmoid(v)

        def unit(v):
            return v * lax.rsqrt(jnp.sum(v * v, axis=-1, keepdims=True) + NORM_EPS)

        q = unit(act(0)) * HEAD ** (-0.5)
        k = unit(act(1))
        v = act(2)
        beta = beta_all[at]
        gcol = gates[:, u : u + 1]
        grow = gates_t[u : u + 1, :]
        glast = gates[BLOCK - 1 : BLOCK, u : u + 1]
        gap = gcol - grow
        decay = jnp.where(causal, jnp.exp(jnp.where(causal, gap, 0.0)), 0.0)
        ks = k * beta
        low = jnp.where(strict, dot_t(ks, k, HIGHEST) * decay, 0.0)
        scores = dot_t(q.astype(BF16), k.astype(BF16)) * decay
        eg = jnp.exp(gcol)
        terms.append([low, scores, v * beta, ks * eg, q * eg, k * jnp.exp(glast - gcol),
                      jnp.exp(glast)])
    every = range(len(units))
    inv = [eye - jnp.where((ri // 2 == ci // 2), terms[i][0], 0.0) for i in every]
    size = 2
    while size < BLOCK:
        joint = (ri // (2 * size) == ci // (2 * size)) & (ri // size != ci // size)
        mids = [dot(jnp.where(joint, terms[i][0], 0.0), inv[i], HIGHEST) for i in every]
        inv = [inv[i] - dot(inv[i], mids[i], HIGHEST) for i in every]
        size *= 2
    inv = [m.astype(BF16) for m in inv]
    nv = [dot(inv[i], terms[i][2].astype(BF16)) for i in every]
    kw = [dot(inv[i], terms[i][3].astype(BF16)).astype(BF16) for i in every]
    out_pass(1)
    state = [None] * seqs
    for n in range(Z):
        for b in range(seqs):
            i = b * Z + n
            _, scores, _, _, qd_, kd_, factor = terms[i]
            corrected = nv[i]
            if n:
                s_in = state[b].astype(BF16)
                corrected = corrected - dot(kw[i], s_in)
            o = dot(scores.astype(BF16), corrected.astype(BF16))
            if n:
                o = o + dot(qd_.astype(BF16), s_in)
            grown = t_dot(kd_.astype(BF16), corrected.astype(BF16))
            state[b] = state[b] * factor + grown if n else grown
            o = o * lax.rsqrt(jnp.mean(o * o, axis=-1, keepdims=True) + NORM_EPS) * gain[...]
            hsrc[0, n, b * BLOCK : (b + 1) * BLOCK] = o.astype(BF16)

    def give(kind):
        for k in range(1, Z):
            to = lax.rem(z + k, Z)
            H.put(True, hsrc.at[kind, to], hbuf.at[x, kind, z], hrecv.at[x, kind, z], {"sp": to})
        hbuf[x, kind, z] = hsrc[kind, z]
        H.put(True, hsrc.at[kind, z], hbuf.at[x, kind, z], hrecv.at[x, kind, z], {"fs": 1 - x})

    def pass_heads(kind):
        for k in range(1, Z):
            zz = lax.rem(z - k + Z, Z)
            ref = hbuf.at[x, kind, zz]
            landed(True, ref, dummy.at[2], hrecv.at[x, kind, zz], c)
            H.put(True, ref, ref, hrecv.at[x, kind, zz], {"fs": 1 - x})

    give(0)
    for k in range(1, Z):
        zz = lax.rem(z - k + Z, Z)
        landed(c == 0, lat.at[zz], dummy.at[2], lrecv.at[zz], c)
        latput(c == 0, zz, {"tp": 1 - c})
    for k in range(1, nk):
        slot = Z + lax.rem(kblock + k, nk)
        landed(c == 1, lat.at[slot], dummy.at[2], lrecv.at[slot], c)
        latput(c == 1, slot, {"tp": 1 - c})
    for s in range(Z):
        landed(c == 1, lat.at[s], dummy.at[2], lrecv.at[s], c)
    for s in range(Z, Z + nk):
        landed(c == 0, lat.at[s], dummy.at[2], lrecv.at[s], c)

    scale = per ** (-0.5)
    la = lax.broadcasted_iota(jnp.int32, (length, length), 1) // BLOCK
    lb = lax.broadcasted_iota(jnp.int32, (length, length), 0) // BLOCK
    allowed = la <= lb
    lcol = pl.ds(pl.multiple_of(z * lh * tile, lh * tile), lh * tile)

    def normed_parts(slots, at, g_):
        parts = [lat[s, at].astype(F32) for s in slots]
        squares = sum(jnp.sum(p * p, axis=-1, keepdims=True) for p in parts)
        factor = lax.rsqrt(squares / (len(parts) * tile) + NORM_EPS)
        return jnp.concatenate(
            [(p * factor * g_[:, i * tile : (i + 1) * tile]).astype(BF16)
             for i, p in enumerate(parts)], axis=1
        )

    for b in range(seqs):
        at = slice(b * length, (b + 1) * length)
        ta, tb = turn_a[...], turn_b[...]
        qn = normed_parts(range(Z), at, qgain)
        kn = normed_parts(range(Z, Z + nk), at, kgain)
        qa = dot(qn, qsel[...]).astype(BF16).astype(F32)
        ka = dot(kn, lup_v[:, lcol]).astype(BF16)
        rope = sm[at].astype(BF16).astype(F32)
        turned = (rope[:, :tile] * ta + rope[:, tile:] * tb).astype(BF16)
        outs_ = []
        for j in range(lh):
            qf = (qa[:, j * tile : (j + 1) * tile] * ta
                  + qa[:, (lh + j) * tile : (lh + j + 1) * tile] * tb).astype(BF16)
            kj = ka[:, j * tile : (j + 1) * tile]
            kf = jnp.where(lane < NOPE, kj, turned)
            s = jnp.where(allowed, dot_t(qf, kf) * scale, -jnp.inf)
            w = jnp.exp(s - jnp.max(s, axis=-1, keepdims=True))
            o = dot(w.astype(BF16), kj) / jnp.sum(w, axis=-1, keepdims=True)
            outs_.append(o)
        both_ = jnp.where(lane < VDIM, pltpu.roll(outs_[0], VDIM, 1), outs_[1]).astype(BF16)
        for n in range(Z):
            hsrc[1, n, b * BLOCK : (b + 1) * BLOCK] = both_[n * BLOCK : (n + 1) * BLOCK]
    give(1)
    pass_heads(0)
    out_pass(2)
    pass_heads(1)
    for dist in range(3, Z):
        out_pass(dist)
    for kind in range(2):
        for zz in range(Z):
            landed(True, hbuf.at[1 - x, kind, zz], dummy.at[2], hrecv.at[1 - x, kind, zz], c)
    hv = jnp.concatenate(
        [jnp.concatenate([hbuf[xx, kind, s] for kind in range(2) for s in range(Z)], axis=1)
         for xx in range(X)], axis=0
    )
    rows = hbuf.shape[3]
    cb = obuf.shape[2]
    zh = Z // 2
    way = 1 - 2 * (z // zh)
    for i in range(Z):
        zz = lax.rem(z + way * i + Z, Z)
        if i:
            landed(True, obuf.at[zz, oyours], dummy.at[0], orecv.at[zz, 1 - y], c)
        res = dot(hv, obuf[zz]).astype(BF16)
        owner, at = zz // zh, lax.rem(zz, zh)
        for xx in range(X):
            pbuf[zz, xx] = res[xx * rows : (xx + 1) * rows]
        for to in range(2):
            R.put(owner == to, pbuf.at[zz, 1 - x], rbuf.at[c, 1, at], precv.at[c, 1, at],
                  {"fs": 1 - x, "tp": to})
        R.put(owner != c, pbuf.at[zz, x], rbuf.at[1 - c, 0, at], precv.at[1 - c, 0, at],
              {"tp": 1 - c})
    for p in (W, N, L, H, O):
        p.drain()
    total = jnp.zeros((rows, 1), F32)
    mixed = []
    for at in range(zh):
        landed(True, rbuf.at[c, 0, at], dummy.at[2], precv.at[c, 0, at], c)
        m = pbuf[c * zh + at, x].astype(F32) + rbuf[c, 0, at].astype(F32)
        mixed.append((at * X + x, m))
        total = total + jnp.sum(m * m, axis=-1, keepdims=True)
    for at in range(zh):
        for cc in range(2):
            landed(True, rbuf.at[cc, 1, at], dummy.at[2], precv.at[cc, 1, at], c)
        m = rbuf[0, 1, at].astype(F32) + rbuf[1, 1, at].astype(F32)
        mixed.append((at * X + 1 - x, m))
        total = total + jnp.sum(m * m, axis=-1, keepdims=True)
    sq[0] = jnp.broadcast_to(total, sq.shape[1:])
    squares = pltpu.make_async_remote_copy(
        src_ref=sq.at[0], dst_ref=sq.at[1], send_sem=tsem.at[0], recv_sem=tsem.at[1],
        device_id={"tp": 1 - c}, device_id_type=MESH,
    )
    squares.start()
    R.drain()
    squares.wait()
    total = total + sq[1][:, :1]
    norm = lax.rsqrt(total / (Z * X * cb) + NORM_EPS)
    for s, m in mixed:
        at = pl.ds(pl.multiple_of(s * cb, cb), cb)
        out[:, at] = (m * norm * post[s]).astype(BF16)


def splits_by_heads(sizes, seqs, count, qw, qd, kd, qup, lup, do, lo):
    Y, Z, X, C = sizes
    nk = kd[1] // 128
    return (
        Y == 2 and X == 2 and C == 2 and seqs == C and count == BLOCK and qw[1] == Z * HEAD
        and qd[1] == Z * 128 and kd[1] == nk * 128 and Z % nk == 0 and Z % 2 == 0
        and do[0] == lo[0]
        and qup[1] == Z * 2 * (NOPE + ROPE) and lup[1] == Z * 2 * (NOPE + VDIM)
    )


def by_heads(sizes, *arrays):
    (tokens, pre_gain, query_weight, key_weight, value_weight, beta_weight, decay_weight,
     decay_rate, delta_gain, query_down, latent_down, rope_weight, query_gain, latent_gain,
     query_up, latent_up, delta_out, latent_out, post_gain) = arrays
    Y, Z, X, C = sizes
    n = Z * X
    seqs, count, width = tokens.shape
    rows = seqs * count
    shard = query_weight.shape[0]
    nk = latent_down.shape[1] // 128
    cb = delta_out.shape[1]
    depth = delta_out.shape[0] + latent_out.shape[0]
    half = n // 2
    lh = query_up.shape[1] // (NOPE + ROPE) // Z
    total = rows * Z
    ncol = 4 * 128
    chunks = 4
    small = [w.T for w in (beta_weight, decay_weight, rope_weight)]
    args = (
        tokens.reshape(rows, width), pre_gain.reshape(1, width),
        small[0], small[1], small[2],
        query_weight, key_weight, value_weight, query_down, latent_down, delta_out, latent_out,
        query_gain.reshape(1, -1), latent_gain.reshape(1, -1), query_up, latent_up,
        decay_rate.reshape(1, -1), delta_gain.reshape(1, HEAD), post_gain.reshape(half, 1, cb),
    )
    hbm = (0, 2, 3, 4, 5, 6, 7, 8, 9, 10, 11, 14, 15)
    DMA = pltpu.SemaphoreType.DMA
    result = pl.pallas_call(
        functools.partial(heads_kernel, sizes, seqs),
        name="layer",
        out_shape=jax.ShapeDtypeStruct((rows, half * cb), BF16),
        in_specs=[anywhere() if i in hbm else vmem() for i in range(len(args))],
        out_specs=vmem(),
        scratch_shapes=[
            pltpu.VMEM((rows, width), BF16),
            pltpu.VMEM(small[0].shape, BF16),
            pltpu.VMEM(small[1].shape, BF16),
            pltpu.VMEM(small[2].shape, BF16),
            pltpu.VMEM(query_up.shape, BF16),
            pltpu.VMEM(latent_up.shape, BF16),
            pltpu.VMEM((Z, shard, ncol), BF16),
            pltpu.VMEM((n, shard, ncol), BF16),
            pltpu.VMEM((seqs, Z, BLOCK, width), BF16),
            pltpu.VMEM((256, width), BF16),
            pltpu.VMEM((query_up.shape[0], 2 * lh * 128), BF16),
            pltpu.VMEM((Z * BLOCK, 128), F32),
            pltpu.VMEM((Z * BLOCK, 128), F32),
            pltpu.VMEM((total, 384), BF16),
            pltpu.VMEM((total, 256), F32),
            pltpu.VMEM((Z + nk, total, 128), BF16),
            pltpu.VMEM((2, Z, rows, 128), BF16),
            pltpu.VMEM((X, 2, Z, rows, 128), BF16),
            pltpu.VMEM((Z, depth, cb), BF16),
            pltpu.VMEM((Z, X, rows, cb), BF16),
            pltpu.VMEM((2, 2, Z // 2, rows, cb), BF16),
            pltpu.VMEM((2, rows, 128), F32),
            DMA((4 * Z + 8,)),
            DMA((4 * Z,)),
            DMA((n, 2)),
            DMA((2 * chunks + 4 * Z * chunks,)),
            DMA((seqs, Z, chunks)),
            DMA((2 * Z + 2 * nk,)),
            DMA((Z + nk,)),
            DMA((4 * Z,)),
            DMA((X, 2, Z)),
            DMA((4 + 6 * Z,)),
            DMA((Z, 2)),
            DMA((3 * Z,)),
            DMA((2, 2, Z // 2)),
            DMA((1,)),
            DMA((3,)),
            DMA((2,)),
        ],
        compiler_params=pltpu.CompilerParams(
            collective_id=0, has_side_effects=True, vmem_limit_bytes=60 * 1024 * 1024
        ),
    )(*args)
    return result.reshape(seqs, count, half * cb)


def solution(mesh):
    sizes = tuple(mesh.shape[a] for a in ("grp", "sp", "fs", "tp"))
    return jax.shard_map(
        functools.partial(local, sizes),
        mesh=mesh,
        in_specs=(
            P(("grp", "fs"), "sp", None),
            P(),
            P(("sp", "fs"), "tp"),
            P(("sp", "fs"), "tp"),
            P(("sp", "fs"), "tp"),
            P(),
            P(),
            P(),
            P(),
            P(("sp", "fs"), None),
            P(("sp", "fs"), None),
            P(),
            P(),
            P(),
            P(None, "tp"),
            P(None, "tp"),
            P("tp", ("sp", "fs")),
            P("tp", ("sp", "fs")),
            P("tp"),
        ),
        out_specs=P(("grp", "fs"), "sp", "tp"),
        check_vma=False,
    )
```

```python
import functools
import math

import jax
import jax.numpy as jnp
from jax import lax
from jax.experimental import pallas as pl
from jax.experimental.pallas import tpu as pltpu
from jax.sharding import PartitionSpec as P

HEAD = 128
NOPE = 64
ROPE = 32
VDIM = 64
BLOCK = 64
NORM_EPS = 1e-06
ROPE_THETA = 10000.0
HIGHEST = lax.Precision.HIGHEST
MESH = pl.DeviceIdType.MESH
F32 = jnp.float32
BF16 = jnp.bfloat16


def dot(a, b, precision=None):
    return jnp.dot(a, b, preferred_element_type=F32, precision=precision)


def dot_t(a, b, precision=None):
    return lax.dot_general(
        a, b, (((1,), (1,)), ((), ())), preferred_element_type=F32, precision=precision
    )


def t_dot(a, b, precision=None):
    return lax.dot_general(
        a, b, (((0,), (0,)), ((), ())), preferred_element_type=F32, precision=precision
    )


def when(cond, fn):
    if cond is True:
        fn()
    elif cond is not False:
        pl.when(cond)(fn)


def both(a, b):
    if a is True:
        return b
    if b is True:
        return a
    return jnp.logical_and(a, b)


class Place:
    def __init__(self, sizes):
        self.Y, self.Z, self.X, self.C = sizes
        self.y = lax.axis_index("grp")
        self.z = lax.axis_index("sp")
        self.x = lax.axis_index("fs")
        self.c = lax.axis_index("tp")


def greet(place, plane=True, later=False):
    barrier = pltpu.get_barrier_semaphore()

    def signal(cond, dev):
        when(
            cond,
            lambda: pl.semaphore_signal(barrier, inc=1, device_id=dev, device_id_type=MESH),
        )

    count = jnp.int32(0)
    if later:
        for k in range(1, place.Z):
            signal(place.z + k < place.Z, {"sp": place.z + k})
            signal(place.z - k >= 0, {"sp": place.z - k})
        count += place.Z - 1
    else:
        signal(place.z + 1 < place.Z, {"sp": place.z + 1})
        signal(place.z > 0, {"sp": place.z - 1})
        count += (place.z + 1 < place.Z).astype(jnp.int32) + (place.z > 0).astype(jnp.int32)
    if plane:
        for d in range(1, place.X):
            signal(True, {"fs": lax.rem(place.x + d, place.X)})
        count += place.X - 1
        if place.Y == 2:
            signal(True, {"grp": 1 - place.y})
            count += 1
    signal(True, {"tp": 1 - place.c})
    count += 1
    pl.semaphore_wait(barrier, count)


class Gather:
    def __init__(self, place, own, buf, send, recv, lsem):
        self.pl, self.own, self.buf = place, own, buf
        self.send, self.recv, self.lsem = send, recv, lsem
        self.sends = []
        self.ev = 0

    def active(self, p):
        return True if p == 2 else self.pl.y == p

    def push(self, cond, src, p, slot, dev, ev, way):
        index = len(self.sends)

        def make():
            return pltpu.make_async_remote_copy(
                src_ref=src,
                dst_ref=self.buf(p, slot),
                send_sem=self.send.at[index],
                recv_sem=self.recv.at[slot, p],
                device_id=dev,
                device_id_type=MESH,
            )

        when(cond, lambda: make().start())
        self.sends.append((cond, make))

    def arrived(self, cond, p, slot):
        def wait():
            ref = self.buf(p, slot)
            pltpu.make_async_remote_copy(
                src_ref=ref,
                dst_ref=ref,
                send_sem=self.lsem.at[p],
                recv_sem=self.recv.at[slot, p],
                device_id={"tp": self.pl.c},
                device_id_type=MESH,
            ).wait_recv()

        when(cond, wait)

    def across(self, cond, src, p, slot, ev):
        q = self.pl
        for d in range(1, q.X):
            self.push(cond, src, p, slot, {"fs": lax.rem(q.x + d, q.X)}, ev, 1 + d)

    def to_y(self, cond, src, p, slot, ev):
        if p < 2:
            self.push(cond, src, p, slot, {"grp": 1 - self.pl.y}, ev, 0)

    def kinds(self):
        return (0, 1, 2)

    def start_along(self):
        q = self.pl
        me = q.z * q.X + q.x
        for p in self.kinds():
            a = self.active(p)
            src = self.own(p)
            self.push(both(a, q.z + 1 < q.Z), src, p, me, {"sp": q.z + 1}, 0, 0)
            self.push(both(a, q.z > 0), src, p, me, {"sp": q.z - 1}, 0, 1)

    def start_across(self):
        q = self.pl
        me = q.z * q.X + q.x
        for p in self.kinds():
            self.across(self.active(p), self.own(p), p, me, 0)
        for p in self.kinds():
            pltpu.make_async_copy(self.own(p), self.buf(p, me), self.lsem.at[p]).start()

    def step(self, k):
        q = self.pl
        for p in self.kinds():
            a = self.active(p)
            for sign in (1, -1):
                zz = q.z - sign * k
                ok = both(a, jnp.logical_and(zz >= 0, zz < q.Z))
                slot = zz * q.X + q.x
                nxt = q.z + sign
                ev = 2 * k - (sign == 1)
                self.arrived(ok, p, slot)
                ref = self.buf(p, slot)
                self.push(
                    both(ok, jnp.logical_and(nxt >= 0, nxt < q.Z)),
                    ref, p, slot, {"sp": nxt}, ev, 1,
                )
                self.across(ok, ref, p, slot, ev)
                self.to_y(ok, ref, p, slot, ev)

    def cross_step(self, k):
        q = self.pl
        base = 2 * q.Z
        for p in self.kinds():
            a = self.active(p)
            for sign in (1, -1) if k else (1,):
                zz = q.z - sign * k
                ok = both(a, jnp.logical_and(zz >= 0, zz < q.Z))
                for d in range(1, q.X):
                    slot = zz * q.X + lax.rem(q.x + d, q.X)
                    ev = base + (2 * k - (sign == 1) + 1) * (q.X - 1) + d - 1
                    self.arrived(ok, p, slot)
                    self.to_y(ok, self.buf(p, slot), p, slot, ev)

    def finish(self):
        q = self.pl
        self.cross_step(q.Z - 1)
        me = q.z * q.X + q.x
        for p in (0, 1):
            for s in range(q.Z * q.X):
                self.arrived(jnp.logical_and(q.y != p, me != s), p, s)
        for p in self.kinds():
            pltpu.make_async_copy(self.own(p), self.buf(p, me), self.lsem.at[p]).wait()

    def drain(self):
        for cond, make in self.sends:
            when(cond, lambda make=make: make().wait_send())

    @staticmethod
    def scratch(Z, X):
        n = Z * X
        sends = 3 * (X + 1) + 2 * (Z - 1) * (3 * X + 2) + (2 * Z - 1) * (X - 1) * 2
        return [
            pltpu.SemaphoreType.DMA((sends,)),
            pltpu.SemaphoreType.DMA((n, 3)),
            pltpu.SemaphoreType.DMA((3,)),
        ]


def spread(copies, parts, target, bounds):
    at = 0
    for ref, offset, width in parts:
        done = 0
        while done < width:
            p, col = divmod(at + done, bounds)
            size = min(width - done, bounds - col)
            start = offset + done
            if not isinstance(start, int):
                start = pl.multiple_of(start, 128)
            copies.append((ref.at[:, pl.ds(start, size)], target.at[p, :, pl.ds(col, size)]))
            done += size
        at += width


def back_kernel(
    sizes, seqs, heads, cuts, tokens, pre_gain, small, w_query, w_key, w_value, w_qdown, w_kdown,
    w_delta, w_latent, qgain, kgain, w_qup, w_lup, rate_in, gain, post,
    out, qup, lup, raw, lat, rate, own1, own, buf1, kvr, kbuf, sin, sout, hbuf, buf, pbuf, rbuf, sq,
    asem, ksem, ssem, send1, recv1, lsem1, send, recv, lsem, tsem,
):
    place = Place(sizes)
    Z, z, c = place.Z, place.z, place.c
    C = sizes[3]
    rows = tokens.shape[0]
    third = own1.shape[2]
    qcols, kcols = w_qdown.shape[1] // C, w_kdown.shape[1] // C
    pairs = []
    spread(
        pairs,
        [(w, 0, w.shape[1]) for w in (w_query, w_key, w_value)]
        + [(w_qdown, c * qcols, qcols), (w_kdown, c * kcols, kcols)],
        own1, third,
    )
    upper = w_delta.shape[0]
    pairs.append((w_delta, own.at[pl.ds(0, upper)]))
    pairs.append((w_latent, own.at[pl.ds(upper, w_latent.shape[0])]))
    loads = [pltpu.make_async_copy(a, b, asem.at[i]) for i, (a, b) in enumerate(pairs)]
    for load in loads:
        load.start()
    greet(place, later=True)
    for load in loads:
        load.wait()
    g1 = Gather(
        place, lambda p: own1.at[p], lambda p, s: buf1.at[p, s], send1, recv1, lsem1
    )
    g = Gather(
        place,
        lambda p: own.at[pl.ds(cuts[p], cuts[p + 1] - cuts[p])],
        lambda p, s: buf.at[s, pl.ds(cuts[p], cuts[p + 1] - cuts[p])],
        send, recv, lsem,
    )
    g1.start_along()
    g1.start_across()
    x = tokens[...].astype(F32)
    xscale = lax.rsqrt(jnp.mean(x * x, axis=-1, keepdims=True) + NORM_EPS)
    normed = (x * xscale * pre_gain[...]).astype(BF16)
    sm_all = dot_t(normed, small[...])
    qcol = w_qup.shape[1]
    lh = qcol // (NOPE + ROPE)
    turn_w = ROPE // 2
    kinds = ((NOPE, 0, qup, w_qup, NOPE + ROPE), (turn_w, NOPE, qup, w_qup, NOPE + ROPE),
             (turn_w, NOPE + turn_w, qup, w_qup, NOPE + ROPE),
             (NOPE, 0, lup, w_lup, NOPE + VDIM), (VDIM, NOPE, lup, w_lup, NOPE + VDIM))
    fill_at = {}
    for w, off, to, frm, per in kinds:
        size = lh * w
        dst_i = lax.broadcasted_iota(jnp.int32, (frm.shape[1], size), 1)
        src_i = lax.broadcasted_iota(jnp.int32, (frm.shape[1], size), 0)
        perm = jnp.where(src_i == dst_i // w * per + off + dst_i % w, 1.0, 0.0).astype(BF16)
        lo = fill_at.get(per, 0)
        to[:, lo : lo + size] = dot(frm[...], perm).astype(BF16)
        fill_at[per] = lo + size
    for k in range(1, Z):
        g1.step(k)
        g1.cross_step(k - 1)
        if k == max(1, Z - 2):
            g.start_along()
    g.start_across()
    if Z > 1:
        g.step(1)
    g1.finish()
    depth1 = buf1.shape[1] * buf1.shape[2]
    part2 = dot(normed, buf1[2].reshape(depth1, third)).astype(BF16)
    lat[c] = part2[:, third - qcols - kcols :]
    trade = pltpu.make_async_remote_copy(
        src_ref=lat.at[c], dst_ref=lat.at[c], send_sem=tsem.at[4], recv_sem=tsem.at[5],
        device_id={"tp": 1 - c}, device_id_type=MESH,
    )
    trade.start()
    raw[:, 2 * third : 3 * third] = part2
    for p in range(2):
        raw[:, p * third : (p + 1) * third] = dot(
            normed, buf1[p].reshape(depth1, third)
        ).astype(BF16)
    trade.wait()
    qw = qup.shape[0] // sizes[3]
    kw_lat = lup.shape[0] // sizes[3]
    tile = 128
    lane = lax.broadcasted_iota(jnp.int32, (rows, tile), 1)
    half_turn = ROPE // 2
    step = (lane % half_turn).astype(F32)
    row = lax.broadcasted_iota(jnp.int32, (rows, tile), 0)
    pos = (z * BLOCK + row % BLOCK).astype(F32)
    angle = pos * jnp.exp(step * (-2.0 * math.log(ROPE_THETA) / ROPE))
    cos, sin_t = jnp.cos(angle), jnp.sin(angle)

    def normed_parts(lo, w, g):
        parts = [lat[i, :, lo : lo + w].astype(F32) for i in range(sizes[3])]
        squares = sum(jnp.sum(p * p, axis=-1, keepdims=True) for p in parts)
        scale = lax.rsqrt(squares / (w * sizes[3]) + NORM_EPS)
        return [
            (p * scale * g[:, i * w : (i + 1) * w]).astype(BF16) for i, p in enumerate(parts)
        ]

    kparts = normed_parts(qw, kw_lat, kgain)
    krank = kw_lat * sizes[3]
    for i, p in enumerate(kparts):
        kvr[:, i * kw_lat : (i + 1) * kw_lat] = p
    allheads = heads * C
    src = lax.broadcasted_iota(jnp.int32, (tile, tile), 0)
    dst = lax.broadcasted_iota(jnp.int32, (tile, tile), 1)
    rope_raw = sm_all.astype(BF16)
    base = 2 * allheads + dst % half_turn

    def pick(cond, kind):
        return jnp.where(cond, 1.0, 0.0).astype(kind)

    rlo = dot(rope_raw, pick(src == base, BF16))
    rhi = dot(rope_raw, pick(src == base + half_turn, BF16))
    left = lane < tile // 2
    kvr[:, krank : krank + tile] = jnp.where(
        left, rlo * cos - rhi * sin_t, rhi * cos + rlo * sin_t
    ).astype(BF16)

    def kv_copy(k):
        return pltpu.make_async_remote_copy(
            src_ref=kvr,
            dst_ref=kbuf.at[z],
            send_sem=ksem.at[0, k],
            recv_sem=ksem.at[1, z],
            device_id={"sp": z + k},
            device_id_type=MESH,
        )

    for k in range(1, Z):
        when(z + k < Z, lambda k=k: kv_copy(k).start())
    ri = lax.broadcasted_iota(jnp.int32, (rows, rows), 0)
    ci = lax.broadcasted_iota(jnp.int32, (rows, rows), 1)
    tri = jnp.where((ri >= ci) & (ri // BLOCK == ci // BLOCK), 1.0, 0.0).astype(F32)
    rate[...] = jnp.zeros(rate.shape, F32)
    rate[:, allheads : 2 * allheads] = rate_in[...]
    first_head = c * heads
    own_beta = pick((dst < heads) & (src == first_head + dst), F32)
    own_rate = pick(
        (dst >= heads) & (dst < 2 * heads) & (src == allheads + first_head + dst - heads), F32
    )
    pre = dot(sm_all, own_beta + own_rate, HIGHEST)
    rates = dot(jnp.broadcast_to(rate[...], (8, tile)), own_rate, HIGHEST)[:1]
    beta_all = jax.nn.sigmoid(pre)
    log_a = -rates * (jnp.maximum(pre, 0.0) + jnp.log1p(jnp.exp(-jnp.abs(pre))))
    gates = dot(tri, log_a, HIGHEST)
    gates_t = gates.T
    r = lax.broadcasted_iota(jnp.int32, (BLOCK, BLOCK), 0)
    cc = lax.broadcasted_iota(jnp.int32, (BLOCK, BLOCK), 1)
    strict = r > cc
    causal = r >= cc
    eye = jnp.where(r == cc, 1.0, 0.0).astype(F32)
    lanes = [(b, h) for b in range(seqs) for h in range(heads)]
    width = heads * HEAD
    terms = []
    for b, h in lanes:
        t = slice(b * BLOCK, (b + 1) * BLOCK)

        def act(i):
            v = raw[t, i * width + h * HEAD : i * width + (h + 1) * HEAD].astype(F32)
            return v * jax.nn.sigmoid(v)

        def unit(u):
            return u * lax.rsqrt(jnp.sum(u * u, axis=-1, keepdims=True) + NORM_EPS)

        q = unit(act(0)) * HEAD ** (-0.5)
        k = unit(act(1))
        v = act(2)
        beta = beta_all[t, h : h + 1]
        gcol = gates[t, heads + h : heads + h + 1]
        grow = gates_t[heads + h : heads + h + 1, t]
        glast = gates[(b + 1) * BLOCK - 1 : (b + 1) * BLOCK, heads + h : heads + h + 1]
        gap = gcol - grow
        decay = jnp.where(causal, jnp.exp(jnp.where(causal, gap, 0.0)), 0.0)
        ks = k * beta
        low = jnp.where(strict, dot_t(ks, k, HIGHEST) * decay, 0.0)
        scores = dot_t(q.astype(BF16), k.astype(BF16)) * decay
        eg = jnp.exp(gcol)
        terms.append([low, scores, v * beta, ks * eg, q * eg, k * jnp.exp(glast - gcol),
                      jnp.exp(glast)])
    every = range(len(lanes))
    inv = [eye - jnp.where((r // 2 == cc // 2), terms[i][0], 0.0) for i in every]
    size = 2
    while size < BLOCK:
        joint = (r // (2 * size) == cc // (2 * size)) & (r // size != cc // size)
        mids = [dot(jnp.where(joint, terms[i][0], 0.0), inv[i], HIGHEST) for i in every]
        inv = [inv[i] - dot(inv[i], mids[i], HIGHEST) for i in every]
        size *= 2
    inv = [m.astype(BF16) for m in inv]
    nv = [dot(inv[i], terms[i][2].astype(BF16)) for i in every]
    kw = [dot(inv[i], terms[i][3].astype(BF16)) for i in every]

    def state_copy(i):
        return pltpu.make_async_remote_copy(
            src_ref=sout.at[i],
            dst_ref=sin.at[i],
            send_sem=ssem.at[0, i],
            recv_sem=ssem.at[1, i],
            device_id={"sp": z + 1},
            device_id_type=MESH,
        )

    g.cross_step(0)
    if Z > 2:
        g.step(2)
    for i, (b, h) in enumerate(lanes):
        low, scores, vb, ke, qd, kd, factor = terms[i]

        def clear(i=i):
            sin[i] = jnp.zeros((HEAD, HEAD), BF16)

        when(z == 0, clear)
        when(z > 0, lambda i=i: state_copy(i).wait_recv())
        s_in = sin[i]
        corrected = nv[i] - dot(kw[i].astype(BF16), s_in)
        sout[i] = (
            s_in.astype(F32) * factor + t_dot(kd.astype(BF16), corrected.astype(BF16))
        ).astype(BF16)
        when(z + 1 < Z, lambda i=i: state_copy(i).start())
        o = dot(qd.astype(BF16), s_in) + dot(scores.astype(BF16), corrected.astype(BF16))
        o = o * lax.rsqrt(jnp.mean(o * o, axis=-1, keepdims=True) + NORM_EPS) * gain[...]
        hbuf[b * BLOCK : (b + 1) * BLOCK, h * HEAD : (h + 1) * HEAD] = o.astype(BF16)
    g.cross_step(1)
    for k in range(3, Z):
        g.step(k)
        if k < Z - 1:
            g.cross_step(k - 1)

    for k in range(1, Z):
        def take(k=k):
            pltpu.make_async_remote_copy(
                src_ref=kvr, dst_ref=kbuf.at[z - k], send_sem=ksem.at[0, k],
                recv_sem=ksem.at[1, z - k], device_id={"sp": z}, device_id_type=MESH,
            ).wait_recv()

        when(z - k >= 0, take)
    for s in range(Z):
        def fill(s=s):
            kbuf[s] = kvr[...]

        def none(s=s):
            kbuf[s] = jnp.zeros(kbuf.shape[1:], BF16)

        when(z == s, fill)
        when(z < s, none)
    qparts = normed_parts(0, qw, qgain)
    qa = sum(dot(p, qup[i * qw : (i + 1) * qw, :]) for i, p in enumerate(qparts)).astype(BF16)
    plain_width = qa.shape[1] - 2 * tile
    qlo_raw = qa[:, plain_width : plain_width + tile].astype(F32)
    qhi_raw = qa[:, plain_width + tile :].astype(F32)
    qlo = (qlo_raw * cos - qhi_raw * sin_t).astype(BF16)
    qhi = (qhi_raw * cos + qlo_raw * sin_t).astype(BF16)
    lane1 = lax.broadcasted_iota(jnp.int32, (1, tile), 1)

    def keep(cond):
        return jnp.where(cond, 1.0, 0.0).astype(BF16)

    keys = Z * BLOCK
    allowed = lax.broadcasted_iota(jnp.int32, (2 * BLOCK, keys), 1) // BLOCK <= z
    left_half = lax.broadcasted_iota(jnp.int32, (BLOCK, tile), 1) < tile // 2
    for b in range(seqs):
        t = slice(b * BLOCK, (b + 1) * BLOCK)
        kv = jnp.concatenate([kbuf[s, t, :] for s in range(Z)], axis=0)
        up = dot(kv[:, :krank], lup[...]).astype(BF16)
        turn = kv[:, krank : krank + tile].astype(F32)
        rolled = pltpu.roll(turn, tile // 2, 1)
        sel = lax.broadcasted_iota(jnp.int32, (keys, tile), 1) < tile // 2
        klo = jnp.where(sel, turn, rolled).astype(BF16)
        khi = jnp.where(sel, rolled, turn).astype(BF16)
        for j in range(plain_width // tile):
            at = slice(j * tile, (j + 1) * tile)
            qp = qa[t, at]
            first, second = keep(lane1 < tile // 2), keep(lane1 >= tile // 2)
            m0, m1 = keep(lane1 // half_turn == 2 * j), keep(lane1 // half_turn == 2 * j + 1)
            s = (
                dot_t(jnp.concatenate([qp * first, qp * second], axis=0), up[:, at])
                + dot_t(jnp.concatenate([qlo[t] * m0, qlo[t] * m1], axis=0), klo)
                + dot_t(jnp.concatenate([qhi[t] * m0, qhi[t] * m1], axis=0), khi)
            ) * (NOPE + ROPE) ** (-0.5)
            s = jnp.where(allowed, s, -jnp.inf)
            w = jnp.exp(s - jnp.max(s, axis=-1, keepdims=True))
            o = dot(w.astype(BF16), up[:, plain_width + j * tile : plain_width + (j + 1) * tile])
            o = o / jnp.sum(w, axis=-1, keepdims=True)
            hbuf[t, width + j * tile : width + (j + 1) * tile] = jnp.where(
                left_half, o[:BLOCK], o[BLOCK:]
            ).astype(BF16)
    if Z > 3:
        g.cross_step(Z - 2)
    g.finish()
    n = buf.shape[0]
    half = n // 2
    hv = hbuf[...]

    def part(s, carry):
        pbuf[s] = dot(hv, buf[s]).astype(BF16)
        return carry

    lax.fori_loop(0, n, part, 0)
    peer = 1 - c
    copy = pltpu.make_async_remote_copy(
        src_ref=pbuf.at[pl.ds(peer * half, half)],
        dst_ref=rbuf,
        send_sem=tsem.at[0],
        recv_sem=tsem.at[1],
        device_id={"tp": peer},
        device_id_type=MESH,
    )
    copy.start()
    g1.drain()
    g.drain()
    for k in range(1, Z):
        when(z + k < Z, lambda k=k: kv_copy(k).wait_send())
    for i in every:
        when(z + 1 < Z, lambda i=i: state_copy(i).wait_send())
    copy.wait()
    total = jnp.zeros((rows, 1), F32)
    mixed = []
    for s in range(half):
        m = pbuf[c * half + s].astype(F32) + rbuf[s].astype(F32)
        mixed.append(m)
        total = total + jnp.sum(m * m, axis=-1, keepdims=True)
    sq[0] = jnp.broadcast_to(total, sq.shape[1:])
    squares = pltpu.make_async_remote_copy(
        src_ref=sq.at[0],
        dst_ref=sq.at[1],
        send_sem=tsem.at[2],
        recv_sem=tsem.at[3],
        device_id={"tp": peer},
        device_id_type=MESH,
    )
    squares.start()
    squares.wait()
    total = total + sq[1][:, :1]
    cb = buf.shape[2]
    scale = lax.rsqrt(total / (n * cb) + NORM_EPS)
    for s in range(half):
        out[:, s * cb : (s + 1) * cb] = (mixed[s] * scale * post[s]).astype(BF16)


def vmem():
    return pl.BlockSpec(memory_space=pltpu.VMEM)


def anywhere():
    return pl.BlockSpec(memory_space=pl.ANY)


def local(
    sizes,
    tokens, pre_gain, query_weight, key_weight, value_weight, beta_weight, decay_weight,
    decay_rate, delta_gain, query_down, latent_down, rope_weight, query_gain, latent_gain,
    query_up, latent_up, delta_out, latent_out, post_gain,
):
    Y, Z, X, C = sizes
    n = Z * X
    seqs, count, width = tokens.shape
    if splits_by_heads(sizes, seqs, count, query_weight.shape, query_down.shape,
                       latent_down.shape, query_up.shape, latent_up.shape, delta_out.shape,
                       latent_out.shape):
        return by_heads(
            sizes, tokens, pre_gain, query_weight, key_weight, value_weight, beta_weight,
            decay_weight, decay_rate, delta_gain, query_down, latent_down, rope_weight,
            query_gain, latent_gain, query_up, latent_up, delta_out, latent_out, post_gain,
        )
    rows = seqs * count
    qw = query_down.shape[1] // C
    kw = latent_down.shape[1] // C
    heads = query_weight.shape[1] // HEAD
    shard = query_weight.shape[0]
    third = (3 * query_weight.shape[1] + qw + kw) // 3
    small = [beta_weight.T, decay_weight.T, rope_weight.T]
    used = sum(w.shape[0] for w in small)
    small = jnp.concatenate(small + [jnp.zeros((128 - used, width), BF16)], axis=0)
    lanes = seqs * heads
    cb = delta_out.shape[1]
    depth = delta_out.shape[0] + latent_out.shape[0]
    cuts = (0, depth * 3 // 8, depth * 6 // 8, depth)
    half = n // 2
    kv_width = latent_down.shape[1] + 128
    args = (
        tokens.reshape(rows, width), pre_gain.reshape(1, width), small,
        query_weight, key_weight, value_weight, query_down, latent_down, delta_out, latent_out,
        query_gain.reshape(1, -1), latent_gain.reshape(1, -1), query_up, latent_up,
        decay_rate.reshape(1, -1), delta_gain.reshape(1, HEAD), post_gain.reshape(half, 1, cb),
    )
    result = pl.pallas_call(
        functools.partial(back_kernel, sizes, seqs, heads, cuts),
        name="layer",
        out_shape=jax.ShapeDtypeStruct((rows, half * cb), BF16),
        in_specs=[anywhere() if 3 <= i < 10 else vmem() for i in range(len(args))],
        out_specs=vmem(),
        scratch_shapes=[
            pltpu.VMEM(query_up.shape, BF16),
            pltpu.VMEM(latent_up.shape, BF16),
            pltpu.VMEM((rows, 3 * third), BF16),
            pltpu.VMEM((C, rows, qw + kw), BF16),
            pltpu.VMEM((1, 128), F32),
            pltpu.VMEM((3, shard, third), BF16),
            pltpu.VMEM((depth, cb), BF16),
            pltpu.VMEM((3, n, shard, third), BF16),
            pltpu.VMEM((rows, kv_width), BF16),
            pltpu.VMEM((Z, rows, kv_width), BF16),
            pltpu.VMEM((lanes, HEAD, HEAD), BF16),
            pltpu.VMEM((lanes, HEAD, HEAD), BF16),
            pltpu.VMEM((rows, depth), BF16),
            pltpu.VMEM((n, depth, cb), BF16),
            pltpu.VMEM((n, rows, cb), BF16),
            pltpu.VMEM((half, rows, cb), BF16),
            pltpu.VMEM((2, rows, 128), F32),
            pltpu.SemaphoreType.DMA((16,)),
            pltpu.SemaphoreType.DMA((2, Z)),
            pltpu.SemaphoreType.DMA((2, lanes)),
        ]
        + Gather.scratch(Z, X) + Gather.scratch(Z, X) + [pltpu.SemaphoreType.DMA((6,))],
        compiler_params=pltpu.CompilerParams(
            collective_id=0, has_side_effects=True, vmem_limit_bytes=60 * 1024 * 1024
        ),
    )(*args)
    return result.reshape(seqs, count, half * cb)


def cut(a):
    high = a.astype(BF16)
    return high, (a - high.astype(F32)).astype(BF16)


def dot3(a, b, f=dot):
    (ah, al), (bh, bl) = cut(a), cut(b)
    return f(ah, bh) + (f(ah, bl) + f(al, bh))


class Puts:
    def __init__(self, sems):
        self.sems, self.sent = sems, []

    def put(self, cond, src, dst, recv, dev):
        index = len(self.sent)

        def make():
            return pltpu.make_async_remote_copy(
                src_ref=src, dst_ref=dst, send_sem=self.sems.at[index], recv_sem=recv,
                device_id=dev, device_id_type=MESH,
            )

        when(cond, lambda: make().start())
        self.sent.append((cond, make))

    def drain(self):
        for cond, make in self.sent:
            when(cond, lambda make=make: make().wait_send())


def landed(cond, ref, dummy, recv, c):
    def wait():
        pltpu.make_async_remote_copy(
            src_ref=ref, dst_ref=ref, send_sem=dummy, recv_sem=recv,
            device_id={"tp": c}, device_id_type=MESH,
        ).wait_recv()

    when(cond, wait)


def heads_kernel(
    sizes, seqs, tokens, pre_gain, w_beta, w_decay, w_rope, w_query, w_key, w_value,
    w_qdown, w_kdown, w_delta, w_latent, qgain, kgain, w_qup, w_lup, rate_in, gain, post,
    out, tok, beta_v, decay_v, rope_v, qup_v, lup_v, wown, wbuf, nbuf, ssel, qsel, turn_a, turn_b,
    raw, sm, lat, hsrc, hbuf, obuf, pbuf, rbuf, sq,
    asem, wsend, wrecv, nsend, nrecv, lsend, lrecv, hsend, hrecv, osend, orecv, psend, precv,
    ksem, dummy, tsem,
):
    place = Place(sizes)
    Z, X = place.Z, place.X
    y, z, x, c = place.y, place.z, place.x, place.c
    tile = 128
    shard = wown.shape[1]
    part = shard // 2
    me = z * X + x
    nk = w_kdown.shape[1] // tile
    kblock = lax.rem(z, nk)
    length = Z * BLOCK
    count = seqs * length
    width = nbuf.shape[3]
    ncol = wown.shape[2]
    barrier = pltpu.get_barrier_semaphore()
    peers = [{"sp": lax.rem(z + k, Z)} for k in range(1, Z)]
    peers += [{"fs": 1 - x}, {"grp": 1 - y}, {"fs": 1 - x, "grp": 1 - y}, {"tp": 1 - c},
              {"fs": 1 - x, "tp": 1 - c}]
    for dev in peers:
        pl.semaphore_signal(barrier, inc=1, device_id=dev, device_id_type=MESH)
    loads = []

    def load(src, dst, cond=True):
        index = len(loads)

        def make():
            return pltpu.make_async_copy(src, dst, asem.at[index])

        when(cond, lambda: make().start())
        loads.append(make)
        return index

    first = []
    for d in range(Z):
        for i, w in enumerate((w_query, w_key, w_value)):
            at = wown.at[d, :, pl.ds(i * tile, tile)]
            first.append(load(w.at[:, pl.ds(d * tile, tile)], at))
        at = wown.at[d, :, pl.ds(3 * tile, tile)]
        index = load(w_qdown.at[:, pl.ds(d * tile, tile)], at, c == 0)
        first.append(index)
        kd = d % nk

        def other(kd=kd, at=at, index=index):
            pltpu.make_async_copy(
                w_kdown.at[:, pl.ds(kd * tile, tile)], at, asem.at[index]
            ).start()

        when(c == 1, other)
    tok_at = load(tokens, tok)
    rest = [load(a, b) for a, b in (
        (w_beta, beta_v), (w_decay, decay_v), (w_rope, rope_v), (w_qup, qup_v), (w_lup, lup_v),
    )]
    upper = w_delta.shape[0]
    outs = [load(w_delta, obuf.at[z, pl.ds(0, upper)]),
            load(w_latent, obuf.at[z, pl.ds(upper, w_latent.shape[0])])]

    pl.semaphore_wait(barrier, len(peers))

    for index in first:
        loads[index]().wait()
    W, N, L, H = Puts(wsend), Puts(nsend), Puts(lsend), Puts(hsend)
    O, R = Puts(osend), Puts(psend)
    mine = pl.ds(pl.multiple_of(y * part, part), part)
    yours = pl.ds(pl.multiple_of((1 - y) * part, part), part)
    for k in range(1, Z):
        to = lax.rem(z + k, Z)
        W.put(True, wown.at[to, mine], wbuf.at[me, mine], wrecv.at[me, y], {"sp": to})
    W.put(True, wown.at[z], wbuf.at[me], wrecv.at[me, 0], {"fs": 1 - x})
    keep_own = pltpu.make_async_copy(wown.at[z], wbuf.at[me], ksem.at[0])
    keep_own.start()
    loads[tok_at]().wait()
    for b in range(seqs):
        t = tok[b * BLOCK : (b + 1) * BLOCK].astype(F32)
        scale = lax.rsqrt(jnp.mean(t * t, axis=-1, keepdims=True) + NORM_EPS)
        nbuf[b, z] = (t * scale * pre_gain[...]).astype(BF16)
    chunks = nrecv.shape[2]
    span = BLOCK // chunks

    def chunk(seq, zz, i):
        return nbuf.at[seq, zz, pl.ds(i * span, span)]

    for i in range(chunks):
        for sign in (1, -1):
            nxt = z + sign
            ref = chunk(c, z, i)
            N.put(jnp.logical_and(nxt >= 0, nxt < Z), ref, ref, nrecv.at[c, z, i], {"sp": nxt})

    for index in rest:
        loads[index]().wait()
    lane = lax.broadcasted_iota(jnp.int32, (length, tile), 1)
    row = lax.broadcasted_iota(jnp.int32, (length, tile), 0)
    half_turn = ROPE // 2
    step = (lane % half_turn).astype(F32)
    angle = row.astype(F32) * jnp.exp(step * (-2.0 * math.log(ROPE_THETA) / ROPE))
    turning = (lane >= NOPE) & (lane < NOPE + ROPE)
    turn_a[...] = jnp.where(lane < NOPE, 1.0, jnp.where(turning, jnp.cos(angle), 0.0))
    sin_t = jnp.sin(angle)
    turn_b[...] = jnp.where(turning, jnp.where(lane < NOPE + half_turn, -sin_t, sin_t), 0.0)

    def pick(cond):
        return jnp.where(cond, 1.0, 0.0).astype(BF16)

    head = c * w_query.shape[1] // HEAD + z
    nb = w_beta.shape[0]
    r8 = lax.broadcasted_iota(jnp.int32, (2 * tile, nb), 1)
    l8 = lax.broadcasted_iota(jnp.int32, (2 * tile, nb), 0)
    r32 = lax.broadcasted_iota(jnp.int32, (2 * tile, ROPE), 1)
    l32 = lax.broadcasted_iota(jnp.int32, (2 * tile, ROPE), 0)
    turned_lane = jnp.where(l32 < tile, r32 + NOPE, (r32 + half_turn) % ROPE + NOPE + tile)
    ssel[...] = (
        dot(pick((r8 == head) & (l8 == 0)), beta_v[...])
        + dot(pick((r8 == head) & (l8 == 1)), decay_v[...])
        + dot(pick(l32 == turned_lane), rope_v[...])
    ).astype(BF16)
    per = NOPE + ROPE
    lh = w_qup.shape[1] // per // Z
    qd = lax.broadcasted_iota(jnp.int32, (w_qup.shape[1], tile), 1)
    qs = lax.broadcasted_iota(jnp.int32, (w_qup.shape[1], tile), 0)
    swapped = jnp.where(qd < NOPE, qd, NOPE + (qd - NOPE + half_turn) % ROPE)
    for j in range(lh):
        base = (z * lh + j) * per
        qsel[:, j * tile : (j + 1) * tile] = dot(
            qup_v[...], pick((qd < per) & (qs == base + qd))
        ).astype(BF16)
        qsel[:, (lh + j) * tile : (lh + j + 1) * tile] = dot(
            qup_v[...], pick((qd >= NOPE) & (qd < per) & (qs == base + swapped))
        ).astype(BF16)

    for index in outs:
        loads[index]().wait()
    obl = upper
    omine = pl.ds(pl.multiple_of(y * obl, obl), obl)
    oyours = pl.ds(pl.multiple_of((1 - y) * obl, obl), obl)

    def out_send():
        for sign in (1, -1):
            to = z + sign
            ref = obuf.at[z, omine]
            O.put(jnp.logical_and(to >= 0, to < Z), ref, ref, orecv.at[z, y], {"sp": to})

    def out_pass(dist):
        for sign in (1, -1):
            zz = z - sign * dist
            ok = jnp.logical_and(zz >= 0, zz < Z)
            nxt = z + sign
            ref = obuf.at[zz, omine]
            landed(ok, ref, dummy.at[0], orecv.at[zz, y], c)
            O.put(both(ok, jnp.logical_and(nxt >= 0, nxt < Z)), ref, ref, orecv.at[zz, y],
                  {"sp": nxt})
            O.put(ok, ref, ref, orecv.at[zz, y], {"grp": 1 - y})

    def wait_w(zz, xx, yy, rows):
        slot = zz * X + xx
        landed(True, wbuf.at[slot, rows], dummy.at[0], wrecv.at[slot, yy], c)

    for k in range(1, Z):
        zz = lax.rem(z - k + Z, Z)
        slot = zz * X + x
        wait_w(zz, x, y, mine)
        for dev in ({"fs": 1 - x}, {"grp": 1 - y}, {"fs": 1 - x, "grp": 1 - y}):
            ref = wbuf.at[slot, mine]
            W.put(True, ref, ref, wrecv.at[slot, y], dev)
        for i in range(chunks):
            for sign in (1, -1):
                zz = z - sign * k
                ok = jnp.logical_and(zz >= 0, zz < Z)
                nxt = z + sign
                ref = chunk(c, zz, i)
                landed(ok, ref, dummy.at[1], nrecv.at[c, zz, i], c)
                N.put(both(ok, jnp.logical_and(nxt >= 0, nxt < Z)), ref, ref,
                      nrecv.at[c, zz, i], {"sp": nxt})
                N.put(ok, ref, ref, nrecv.at[c, zz, i], {"tp": 1 - c})
        if k == max(1, Z - 2):
            out_send()
    for k in range(1, Z):
        zz = lax.rem(z - k + Z, Z)
        wait_w(zz, x, 1 - y, yours)
        wait_w(zz, 1 - x, y, mine)
        wait_w(zz, 1 - x, 1 - y, yours)
    slot = z * X + 1 - x
    landed(True, wbuf.at[slot], dummy.at[0], wrecv.at[slot, 0], c)
    keep_own.wait()
    for k in range(1, Z):
        zz = lax.rem(z - k + Z, Z)
        for i in range(chunks):
            landed(True, chunk(1 - c, zz, i), dummy.at[1], nrecv.at[1 - c, zz, i], c)

    lslot = (1 - c) * z + c * (Z + kblock)
    for b in range(seqs):
        at = slice(b * length, (b + 1) * length)
        normed = nbuf[b].reshape(length, width)
        lat[lslot, at] = dot(normed, wbuf[:, :, 3 * tile :].reshape(width, tile)).astype(BF16)

    def latput(cond, slot, dev):
        L.put(cond, lat.at[slot], lat.at[slot], lrecv.at[slot], dev)

    for k in range(1, Z):
        latput(c == 0, z, {"sp": lax.rem(z + k, Z)})
    pair = z - kblock
    for k in range(1, nk):
        latput(c == 1, Z + kblock, {"sp": pair + lax.rem(kblock + k, nk)})
    latput(True, lslot, {"tp": 1 - c})
    for b in range(seqs):
        at = slice(b * length, (b + 1) * length)
        normed = nbuf[b].reshape(length, width)
        raw[at] = dot(normed, wbuf[:, :, : 3 * tile].reshape(width, 3 * tile)).astype(BF16)
        sm[at] = dot_t(normed, ssel[...])

    ri = lax.broadcasted_iota(jnp.int32, (BLOCK, BLOCK), 0)
    ci = lax.broadcasted_iota(jnp.int32, (BLOCK, BLOCK), 1)
    strict = ri > ci
    causal = ri >= ci
    eye = jnp.where(ri == ci, 1.0, 0.0).astype(F32)
    tri = jnp.where(causal, 1.0, 0.0).astype(F32)
    units = [(b, n) for b in range(seqs) for n in range(Z)]
    lane1 = lax.broadcasted_iota(jnp.int32, (1, nb), 1)
    rate = jnp.sum(jnp.where(lane1 == head, rate_in[...], 0.0), axis=-1, keepdims=True)
    pre_b = sm[:, 0:1]
    pre_d = sm[:, 1:2]
    beta_all = jax.nn.sigmoid(pre_b)
    log_a = -rate * (jnp.maximum(pre_d, 0.0) + jnp.log1p(jnp.exp(-jnp.abs(pre_d))))
    blane = lax.broadcasted_iota(jnp.int32, (BLOCK, tile), 1)
    spread_a = jnp.zeros((BLOCK, tile), F32)
    for u in range(len(units)):
        spread_a = jnp.where(blane == u, log_a[u * BLOCK : (u + 1) * BLOCK], spread_a)
    gates = dot(tri, spread_a, HIGHEST)
    gates_t = gates.T
    terms = []
    for u in range(len(units)):
        at = slice(u * BLOCK, (u + 1) * BLOCK)

        def act(i):
            v = raw[at, i * tile : (i + 1) * tile].astype(F32)
            return v * jax.nn.sigmoid(v)

        def unit(v):
            return v * lax.rsqrt(jnp.sum(v * v, axis=-1, keepdims=True) + NORM_EPS)

        q = unit(act(0)) * HEAD ** (-0.5)
        k = unit(act(1))
        v = act(2)
        beta = beta_all[at]
        gcol = gates[:, u : u + 1]
        grow = gates_t[u : u + 1, :]
        glast = gates[BLOCK - 1 : BLOCK, u : u + 1]
        gap = gcol - grow
        decay = jnp.where(causal, jnp.exp(jnp.where(causal, gap, 0.0)), 0.0)
        ks = k * beta
        low = jnp.where(strict, dot3(ks, k, dot_t) * decay, 0.0)
        scores = dot_t(q.astype(BF16), k.astype(BF16)) * decay
        eg = jnp.exp(gcol)
        terms.append([low, scores, v * beta, ks * eg, q * eg, k * jnp.exp(glast - gcol),
                      jnp.exp(glast)])
    every = range(len(units))
    inv = [eye - jnp.where((ri // 2 == ci // 2), terms[i][0], 0.0) for i in every]
    size = 2
    while size < BLOCK:
        joint = (ri // (2 * size) == ci // (2 * size)) & (ri // size != ci // size)
        mids = [dot3(jnp.where(joint, terms[i][0], 0.0), inv[i]) for i in every]
        inv = [inv[i] - dot3(inv[i], mids[i]) for i in every]
        size *= 2
    inv = [m.astype(BF16) for m in inv]
    nv = [dot(inv[i], terms[i][2].astype(BF16)) for i in every]
    kw = [dot(inv[i], terms[i][3].astype(BF16)).astype(BF16) for i in every]
    out_pass(1)
    state = [None] * seqs
    for n in range(Z):
        for b in range(seqs):
            i = b * Z + n
            _, scores, _, _, qd_, kd_, factor = terms[i]
            corrected = nv[i]
            if n:
                s_in = state[b].astype(BF16)
                corrected = corrected - dot(kw[i], s_in)
            o = dot(scores.astype(BF16), corrected.astype(BF16))
            if n:
                o = o + dot(qd_.astype(BF16), s_in)
            grown = t_dot(kd_.astype(BF16), corrected.astype(BF16))
            state[b] = state[b] * factor + grown if n else grown
            o = o * lax.rsqrt(jnp.mean(o * o, axis=-1, keepdims=True) + NORM_EPS) * gain[...]
            hsrc[0, n, b * BLOCK : (b + 1) * BLOCK] = o.astype(BF16)

    def give(kind):
        for k in range(1, Z):
            to = lax.rem(z + k, Z)
            H.put(True, hsrc.at[kind, to], hbuf.at[x, kind, z], hrecv.at[x, kind, z], {"sp": to})
        hbuf[x, kind, z] = hsrc[kind, z]
        H.put(True, hsrc.at[kind, z], hbuf.at[x, kind, z], hrecv.at[x, kind, z], {"fs": 1 - x})

    def pass_heads(kind):
        for k in range(1, Z):
            zz = lax.rem(z - k + Z, Z)
            ref = hbuf.at[x, kind, zz]
            landed(True, ref, dummy.at[2], hrecv.at[x, kind, zz], c)
            H.put(True, ref, ref, hrecv.at[x, kind, zz], {"fs": 1 - x})

    give(0)
    for k in range(1, Z):
        zz = lax.rem(z - k + Z, Z)
        landed(c == 0, lat.at[zz], dummy.at[2], lrecv.at[zz], c)
        latput(c == 0, zz, {"tp": 1 - c})
    for k in range(1, nk):
        slot = Z + lax.rem(kblock + k, nk)
        landed(c == 1, lat.at[slot], dummy.at[2], lrecv.at[slot], c)
        latput(c == 1, slot, {"tp": 1 - c})
    for s in range(Z):
        landed(c == 1, lat.at[s], dummy.at[2], lrecv.at[s], c)
    for s in range(Z, Z + nk):
        landed(c == 0, lat.at[s], dummy.at[2], lrecv.at[s], c)

    scale = per ** (-0.5)
    la = lax.broadcasted_iota(jnp.int32, (length, length), 1) // BLOCK
    lb = lax.broadcasted_iota(jnp.int32, (length, length), 0) // BLOCK
    allowed = la <= lb
    lcol = pl.ds(pl.multiple_of(z * lh * tile, lh * tile), lh * tile)

    def normed_parts(slots, at, g_):
        parts = [lat[s, at].astype(F32) for s in slots]
        squares = sum(jnp.sum(p * p, axis=-1, keepdims=True) for p in parts)
        factor = lax.rsqrt(squares / (len(parts) * tile) + NORM_EPS)
        return jnp.concatenate(
            [(p * factor * g_[:, i * tile : (i + 1) * tile]).astype(BF16)
             for i, p in enumerate(parts)], axis=1
        )

    for b in range(seqs):
        at = slice(b * length, (b + 1) * length)
        ta, tb = turn_a[...], turn_b[...]
        qn = normed_parts(range(Z), at, qgain)
        kn = normed_parts(range(Z, Z + nk), at, kgain)
        qa = dot(qn, qsel[...]).astype(BF16).astype(F32)
        ka = dot(kn, lup_v[:, lcol]).astype(BF16)
        rope = sm[at].astype(BF16).astype(F32)
        turned = (rope[:, :tile] * ta + rope[:, tile:] * tb).astype(BF16)
        outs_ = []
        for j in range(lh):
            qf = (qa[:, j * tile : (j + 1) * tile] * ta
                  + qa[:, (lh + j) * tile : (lh + j + 1) * tile] * tb).astype(BF16)
            kj = ka[:, j * tile : (j + 1) * tile]
            kf = jnp.where(lane < NOPE, kj, turned)
            s = jnp.where(allowed, dot_t(qf, kf) * scale, -jnp.inf)
            w = jnp.exp(s - jnp.max(s, axis=-1, keepdims=True))
            o = dot(w.astype(BF16), kj) / jnp.sum(w, axis=-1, keepdims=True)
            outs_.append(o)
        both_ = jnp.where(lane < VDIM, pltpu.roll(outs_[0], VDIM, 1), outs_[1]).astype(BF16)
        for n in range(Z):
            hsrc[1, n, b * BLOCK : (b + 1) * BLOCK] = both_[n * BLOCK : (n + 1) * BLOCK]
    give(1)
    pass_heads(0)
    out_pass(2)
    pass_heads(1)
    for dist in range(3, Z):
        out_pass(dist)
    for kind in range(2):
        for zz in range(Z):
            landed(True, hbuf.at[1 - x, kind, zz], dummy.at[2], hrecv.at[1 - x, kind, zz], c)
    hv = jnp.concatenate(
        [jnp.concatenate([hbuf[xx, kind, s] for kind in range(2) for s in range(Z)], axis=1)
         for xx in range(X)], axis=0
    )
    rows = hbuf.shape[3]
    cb = obuf.shape[2]
    zh = Z // 2
    way = 1 - 2 * (z // zh)
    for i in range(Z):
        zz = lax.rem(z + way * i + Z, Z)
        if i:
            landed(True, obuf.at[zz, oyours], dummy.at[0], orecv.at[zz, 1 - y], c)
        res = dot(hv, obuf[zz]).astype(BF16)
        owner, at = zz // zh, lax.rem(zz, zh)
        for xx in range(X):
            pbuf[zz, xx] = res[xx * rows : (xx + 1) * rows]
        for to in range(2):
            R.put(owner == to, pbuf.at[zz, 1 - x], rbuf.at[c, 1, at], precv.at[c, 1, at],
                  {"fs": 1 - x, "tp": to})
        R.put(owner != c, pbuf.at[zz, x], rbuf.at[1 - c, 0, at], precv.at[1 - c, 0, at],
              {"tp": 1 - c})
    for p in (W, N, L, H, O):
        p.drain()
    total = jnp.zeros((rows, 1), F32)
    mixed = []
    for at in range(zh):
        landed(True, rbuf.at[c, 0, at], dummy.at[2], precv.at[c, 0, at], c)
        m = pbuf[c * zh + at, x].astype(F32) + rbuf[c, 0, at].astype(F32)
        mixed.append((at * X + x, m))
        total = total + jnp.sum(m * m, axis=-1, keepdims=True)
    for at in range(zh):
        for cc in range(2):
            landed(True, rbuf.at[cc, 1, at], dummy.at[2], precv.at[cc, 1, at], c)
        m = rbuf[0, 1, at].astype(F32) + rbuf[1, 1, at].astype(F32)
        mixed.append((at * X + 1 - x, m))
        total = total + jnp.sum(m * m, axis=-1, keepdims=True)
    sq[0] = jnp.broadcast_to(total, sq.shape[1:])
    squares = pltpu.make_async_remote_copy(
        src_ref=sq.at[0], dst_ref=sq.at[1], send_sem=tsem.at[0], recv_sem=tsem.at[1],
        device_id={"tp": 1 - c}, device_id_type=MESH,
    )
    squares.start()
    R.drain()
    squares.wait()
    total = total + sq[1][:, :1]
    norm = lax.rsqrt(total / (Z * X * cb) + NORM_EPS)
    for s, m in mixed:
        at = pl.ds(pl.multiple_of(s * cb, cb), cb)
        out[:, at] = (m * norm * post[s]).astype(BF16)


def splits_by_heads(sizes, seqs, count, qw, qd, kd, qup, lup, do, lo):
    Y, Z, X, C = sizes
    nk = kd[1] // 128
    return (
        Y == 2 and X == 2 and C == 2 and seqs == C and count == BLOCK and qw[1] == Z * HEAD
        and qd[1] == Z * 128 and kd[1] == nk * 128 and Z % nk == 0 and Z % 2 == 0
        and do[0] == lo[0]
        and qup[1] == Z * 2 * (NOPE + ROPE) and lup[1] == Z * 2 * (NOPE + VDIM)
    )


def by_heads(sizes, *arrays):
    (tokens, pre_gain, query_weight, key_weight, value_weight, beta_weight, decay_weight,
     decay_rate, delta_gain, query_down, latent_down, rope_weight, query_gain, latent_gain,
     query_up, latent_up, delta_out, latent_out, post_gain) = arrays
    Y, Z, X, C = sizes
    n = Z * X
    seqs, count, width = tokens.shape
    rows = seqs * count
    shard = query_weight.shape[0]
    nk = latent_down.shape[1] // 128
    cb = delta_out.shape[1]
    depth = delta_out.shape[0] + latent_out.shape[0]
    half = n // 2
    lh = query_up.shape[1] // (NOPE + ROPE) // Z
    total = rows * Z
    ncol = 4 * 128
    chunks = 4
    small = [w.T for w in (beta_weight, decay_weight, rope_weight)]
    args = (
        tokens.reshape(rows, width), pre_gain.reshape(1, width),
        small[0], small[1], small[2],
        query_weight, key_weight, value_weight, query_down, latent_down, delta_out, latent_out,
        query_gain.reshape(1, -1), latent_gain.reshape(1, -1), query_up, latent_up,
        decay_rate.reshape(1, -1), delta_gain.reshape(1, HEAD), post_gain.reshape(half, 1, cb),
    )
    hbm = (0, 2, 3, 4, 5, 6, 7, 8, 9, 10, 11, 14, 15)
    DMA = pltpu.SemaphoreType.DMA
    result = pl.pallas_call(
        functools.partial(heads_kernel, sizes, seqs),
        name="layer",
        out_shape=jax.ShapeDtypeStruct((rows, half * cb), BF16),
        in_specs=[anywhere() if i in hbm else vmem() for i in range(len(args))],
        out_specs=vmem(),
        scratch_shapes=[
            pltpu.VMEM((rows, width), BF16),
            pltpu.VMEM(small[0].shape, BF16),
            pltpu.VMEM(small[1].shape, BF16),
            pltpu.VMEM(small[2].shape, BF16),
            pltpu.VMEM(query_up.shape, BF16),
            pltpu.VMEM(latent_up.shape, BF16),
            pltpu.VMEM((Z, shard, ncol), BF16),
            pltpu.VMEM((n, shard, ncol), BF16),
            pltpu.VMEM((seqs, Z, BLOCK, width), BF16),
            pltpu.VMEM((256, width), BF16),
            pltpu.VMEM((query_up.shape[0], 2 * lh * 128), BF16),
            pltpu.VMEM((Z * BLOCK, 128), F32),
            pltpu.VMEM((Z * BLOCK, 128), F32),
            pltpu.VMEM((total, 384), BF16),
            pltpu.VMEM((total, 256), F32),
            pltpu.VMEM((Z + nk, total, 128), BF16),
            pltpu.VMEM((2, Z, rows, 128), BF16),
            pltpu.VMEM((X, 2, Z, rows, 128), BF16),
            pltpu.VMEM((Z, depth, cb), BF16),
            pltpu.VMEM((Z, X, rows, cb), BF16),
            pltpu.VMEM((2, 2, Z // 2, rows, cb), BF16),
            pltpu.VMEM((2, rows, 128), F32),
            DMA((4 * Z + 8,)),
            DMA((4 * Z,)),
            DMA((n, 2)),
            DMA((2 * chunks + 4 * Z * chunks,)),
            DMA((seqs, Z, chunks)),
            DMA((2 * Z + 2 * nk,)),
            DMA((Z + nk,)),
            DMA((4 * Z,)),
            DMA((X, 2, Z)),
            DMA((4 + 6 * Z,)),
            DMA((Z, 2)),
            DMA((3 * Z,)),
            DMA((2, 2, Z // 2)),
            DMA((1,)),
            DMA((3,)),
            DMA((2,)),
        ],
        compiler_params=pltpu.CompilerParams(
            collective_id=0, has_side_effects=True, vmem_limit_bytes=60 * 1024 * 1024
        ),
    )(*args)
    return result.reshape(seqs, count, half * cb)


def solution(mesh):
    sizes = tuple(mesh.shape[a] for a in ("grp", "sp", "fs", "tp"))
    return jax.shard_map(
        functools.partial(local, sizes),
        mesh=mesh,
        in_specs=(
            P(("grp", "fs"), "sp", None),
            P(),
            P(("sp", "fs"), "tp"),
            P(("sp", "fs"), "tp"),
            P(("sp", "fs"), "tp"),
            P(),
            P(),
            P(),
            P(),
            P(("sp", "fs"), None),
            P(("sp", "fs"), None),
            P(),
            P(),
            P(),
            P(None, "tp"),
            P(None, "tp"),
            P("tp", ("sp", "fs")),
            P("tp", ("sp", "fs")),
            P("tp"),
        ),
        out_specs=P(("grp", "fs"), "sp", "tp"),
        check_vma=False,
    )
```
